256 devices in a mesh: ep: 16 (over y, x), tp: 16 (over z, core).
Axes of the slice: x: 4, y: 4, z: 8, core: 2. Of those that a mesh axis runs over, the one named last changes fastest.
Arguments:
- tokens: bfloat16 [1024, 4096], P('ep'), may hold values from -6 to 6
- norm_gain: float32 [4096], replicated, may hold values from 0.1 to 1.9
- ffn_gain: float32 [4096], replicated, may hold values from 0.1 to 1.9
- w_in: bfloat16 [4096, 2048], P(None, 'tp'), may hold values from -0.09375 to 0.09375
- decay_rate: float32 [8192], P('tp'), may hold values from 0.02 to 2
- frequency: float32 [8192], P('tp'), may hold values from -3.140625 to 3.140625
- log_step: float32 [128], P('tp'), may hold values from -2.3 to 0
- input_real: float32 [16, 8192], P(None, 'tp'), may hold values from -1 to 1
- input_imag: float32 [16, 8192], P(None, 'tp'), may hold values from -1 to 1
- readout_real: float32 [16, 8192], P(None, 'tp'), may hold values from -0.5 to 0.5
- readout_imag: float32 [16, 8192], P(None, 'tp'), may hold values from -0.5 to 0.5
- skip_gain: float32 [2048], P('tp'), may hold values from -4 to 4
- state_real: float32 [1024, 8192], P('ep', 'tp'), may hold values from -6 to 6
- state_imag: float32 [1024, 8192], P('ep', 'tp'), may hold values from -6 to 6
- w_out: bfloat16 [2048, 4096], P('tp'), may hold values from -0.125 to 0.125
- shared_gate: bfloat16 [4096, 1024], P(None, 'tp'), may hold values from -0.09375 to 0.09375
- shared_up: bfloat16 [4096, 1024], P(None, 'tp'), may hold values from -0.09375 to 0.09375
- shared_down: bfloat16 [1024, 4096], P('tp'), may hold values from -0.1875 to 0.1875
- expert_gate: bfloat16 [64, 4096, 1024], P('ep', 'tp'), may hold values from -0.09375 to 0.09375
- expert_up: bfloat16 [64, 4096, 1024], P('ep', 'tp'), may hold values from -0.09375 to 0.09375
- expert_down: bfloat16 [64, 1024, 4096], P('ep', None, 'tp'), may hold values from -0.1875 to 0.1875
- routing: int32 [1024, 4], P('ep'), may hold values from 0 to 63, all different within a row; in each aligned block of 64 rows (0 to 63, 64 to 127, ...) at most 8 rows name the same one
- route_weight: float32 [1024, 4], P('ep'), may hold values from 0.1 to 1
Outputs:
- mixed: bfloat16 [1024, 4096], P('ep', 'tp')
- new_state_real: float32 [1024, 8192], P('ep', 'tp')
- new_state_imag: float32 [1024, 8192], P('ep', 'tp')
The draws below stay inside these ranges and needn't reach their ends.
Inputs may be any that keep to these rules, and one draw needn't show every extreme that they name: `routing`: each row names 4 different experts. In the rows of one index of ep (aligned blocks of 64 rows) no expert is named more than 8 times, and in every draw some expert is named exactly 8 times in some block.
All inputs are finite; a program needn't handle non-finite values.
Results may differ from the reference program's by a relative error of at most 0.02.
Values may be sent and summed in bfloat16 or wider, within the bound.
No kernel may reach another device: no remote copies, remote signals or barrier semaphores. Data moves between devices by JAX's collectives and lax.ppermute only.
A program may use at most 64 MiB of HBM per device.

```python
import math
import jax
import jax.numpy as jnp
import numpy as np
from jax import lax

D = 4096
GROUPS = 128
CHAN = 16
STATE = 64
FE = 1024
FS = 1024
TOP_K = 4
SEQ_DEV = 64
SEQS = 1024
EXPERTS = 64
CAP = 8


def steps_of(rng, dims, pieces, low, high):
    loudness, own = 1.0, jax.random.fold_in(rng, 6)
    for axis_at, shards_of in pieces:
        heights = jnp.exp(jax.random.uniform(jax.random.fold_in(own, axis_at), (shards_of,), jnp.float32, low / len(pieces), high / len(pieces)))
        loudness = loudness * jnp.repeat(heights, dims[axis_at] // shards_of).reshape([-1 if axis == axis_at else 1 for axis in range(len(dims))])
    return loudness


def routed_block(key, own, number, rows, amount, top, most, skew):
    sequence = jax.random.permutation(key, amount)
    heavy_load, usual = load_shares(amount, rows * top, most, skew, True), load_shares(amount, rows * top, most, skew, False)
    places = jnp.arange(amount)

    def named(tallies, rotation):
        used = int((tallies > 0).sum())
        fixed = max(1, used // 4)
        shifted = fixed + (places - fixed + rotation * (used - fixed)) % max(1, amount - fixed)
        return jnp.zeros((amount,), jnp.int32).at[sequence[jnp.where(places < fixed, places, shifted)]].set(jnp.asarray(tallies, jnp.int32))

    tallies = jnp.where(number % 4 == 0, named(heavy_load, number // 4), named(usual, number - number // 4 - 1))
    mixed = jax.random.permutation(jax.random.fold_in(own, 3), amount)
    source_of, taker = mixed[0:amount // 2 * 2:2], mixed[1:amount // 2 * 2:2]
    margin = jnp.minimum(tallies[source_of] - 1, most - tallies[taker]) // 2
    margin = jnp.where((source_of == sequence[0]) | (taker == sequence[0]) | (tallies[taker] == 0), 0, jnp.maximum(margin, 0))
    shifted = jax.random.randint(jax.random.fold_in(own, 4), (amount // 2,), 0, 1 << 20) % (margin + 1)
    tallies = tallies.at[source_of].add(-shifted).at[taker].add(shifted)
    members = jnp.searchsorted(jnp.cumsum(tallies), jnp.arange(rows * top), side="right").astype(jnp.int32)
    table = members.reshape(top, rows).T
    table = table[jax.random.permutation(jax.random.fold_in(own, 1), rows)]
    rotation = jax.random.randint(jax.random.fold_in(own, 2), (rows, 1), 0, top)
    return jnp.take_along_axis(table, (jnp.arange(top)[None, :] + rotation) % top, axis=1)


def load_shares(count, total, bound, skew, full):
    loads = [(1 << 20) // math.isqrt(standing ** skew) + 1 for standing in range(1, count + 1)]
    largest = bound if full else min(bound, max(-(-total // count), total * loads[0] // sum(loads)))
    least = 1 if total - largest >= count - 1 else 0
    holding, spare = [largest] + [least] * (count - 1), total - largest - least * (count - 1)
    while spare > 0:
        free = [i for i in range(1, count) if holding[i] < largest] or [i for i in range(1, count) if holding[i] < bound]
        mass, budget = sum([loads[i] for i in free]), spare
        for i in free:
            more = min(bound - holding[i], max(1, budget * loads[i] // mass), spare)
            holding[i] = holding[i] + more
            spare = spare - more
    return np.array(holding)


def noise(own_key, dims, scale, reach, pieces=(), kind=jnp.bfloat16):
    entries = jax.random.normal(own_key, dims, jnp.float32) * scale
    if len(pieces) > 0:
        entries = steps_of(own_key, dims, pieces, -0.22, 0.18) * entries
    return jnp.clip(entries, min=-reach, max=reach).astype(kind)


def setup_inputs(seed: int = 0) -> dict:
    streams_of = jax.random.split(jax.random.key(seed), 24)
    tokens = noise(streams_of[0], (SEQS, D), 1.0, 6.0, ((0, 16),))
    norm_gain = jnp.clip(1.0 + 0.18 * jax.random.normal(streams_of[1], (D,), jnp.float32), 0.1, 1.9)
    ffn_gain = jnp.clip(1.0 + 0.18 * jax.random.normal(streams_of[2], (D,), jnp.float32), 0.1, 1.9)
    w_in = noise(streams_of[3], (D, GROUPS * CHAN), D ** -0.5, 0.09375, ((1, 16),))
    decay_rate = jnp.clip(jnp.exp(math.log(2.0) - 4.6051702 * jax.random.uniform(streams_of[4], (GROUPS * STATE,), jnp.float32) ** steps_of(streams_of[4], (GROUPS * STATE,), ((0, 16),), -0.2, 0.2)), 0.02, 2.0)
    frequency = jnp.clip(jax.random.uniform(streams_of[5], (GROUPS * STATE,), jnp.float32, -3.140625, 3.140625), -3.140625, 3.140625)
    log_step = jnp.clip(-2.3 + 2.3 * jax.random.uniform(streams_of[6], (GROUPS,), jnp.float32) ** steps_of(streams_of[6], (GROUPS,), ((0, 16),), -0.2, 0.2), -2.3, 0.0)
    input_real = noise(streams_of[7], (CHAN, GROUPS * STATE), (2 * CHAN) ** -0.5, 1.0, ((1, 16),), jnp.float32)
    input_imag = noise(streams_of[8], (CHAN, GROUPS * STATE), (2 * CHAN) ** -0.5, 1.0, ((1, 16),), jnp.float32)
    readout_real = noise(streams_of[9], (CHAN, GROUPS * STATE), (2 * STATE) ** -0.5, 0.5, ((1, 16),), jnp.float32)
    readout_imag = noise(streams_of[10], (CHAN, GROUPS * STATE), (2 * STATE) ** -0.5, 0.5, ((1, 16),), jnp.float32)
    skip_gain = noise(streams_of[11], (GROUPS * CHAN,), 1.0, 4.0, ((0, 16),), jnp.float32)
    state_real = noise(streams_of[12], (SEQS, GROUPS * STATE), 1.0, 6.0, ((0, 16), (1, 16)), jnp.float32)
    state_imag = noise(streams_of[13], (SEQS, GROUPS * STATE), 1.0, 6.0, ((0, 16), (1, 16)), jnp.float32)
    w_out = noise(streams_of[14], (GROUPS * CHAN, D), (GROUPS * CHAN) ** -0.5, 0.125, ((0, 16),))
    shared_gate = noise(streams_of[15], (D, FS), D ** -0.5, 0.09375, ((1, 16),))
    shared_up = noise(streams_of[16], (D, FS), D ** -0.5, 0.09375, ((1, 16),))
    shared_down = noise(streams_of[17], (FS, D), FS ** -0.5, 0.1875, ((0, 16),))
    expert_gate = noise(streams_of[18], (EXPERTS, D, FE), D ** -0.5, 0.09375, ((0, 16), (1, 16)))
    expert_up = noise(streams_of[19], (EXPERTS, D, FE), D ** -0.5, 0.09375, ((0, 16), (1, 16)))
    expert_down = noise(streams_of[20], (EXPERTS, FE, D), FE ** -0.5, 0.1875, ((0, 16), (2, 16)))
    routing_keys = jax.random.split(jax.random.fold_in(streams_of[21], 1), SEQS // SEQ_DEV)
    routing_turns = jax.random.permutation(jax.random.fold_in(streams_of[21], 3), SEQS // SEQ_DEV)
    routing = jax.vmap(lambda own, number: routed_block(jax.random.fold_in(streams_of[21], 2), own, number, SEQ_DEV, EXPERTS, TOP_K, CAP, 2))(routing_keys, routing_turns).reshape((SEQS, TOP_K))
    route_weight = jnp.clip(jnp.exp(math.log(1.0) - 2.3025851 * jax.random.uniform(streams_of[22], (SEQS, TOP_K), jnp.float32) ** steps_of(streams_of[22], (SEQS, TOP_K), ((0, 16),), -0.2, 0.2)), 0.1, 1.0)
    return {"tokens": tokens, "norm_gain": norm_gain, "ffn_gain": ffn_gain, "w_in": w_in, "decay_rate": decay_rate, "frequency": frequency, "log_step": log_step, "input_real": input_real, "input_imag": input_imag, "readout_real": readout_real, "readout_imag": readout_imag, "skip_gain": skip_gain, "state_real": state_real, "state_imag": state_imag, "w_out": w_out, "shared_gate": shared_gate, "shared_up": shared_up, "shared_down": shared_down, "expert_gate": expert_gate, "expert_up": expert_up, "expert_down": expert_down, "routing": routing, "route_weight": route_weight}


EPS = 1e-06
ROUTED_SCALE = 2.5
HIGH = lax.Precision.HIGHEST

def rms_scale(values_in, gains):
    values = values_in.astype(jnp.float32)
    factor = lax.rsqrt(lax.optimization_barrier(jnp.mean(values * values, axis=-1, keepdims=True)) + EPS)
    return (values * factor * gains).astype(jnp.bfloat16)

def state_update(normed, w_in, decay_rate, frequency, log_step, input_real, input_imag, readout_real, readout_imag, skip_gain, state_real, state_imag):
    seq_count = normed.shape[0]
    groups = log_step.shape[0]
    chan_count = skip_gain.shape[0] // groups
    state_width = decay_rate.shape[0] // groups
    drive_rows = jnp.dot(normed, w_in, preferred_element_type=jnp.float32).astype(jnp.bfloat16)
    drive_f = drive_rows.astype(jnp.float32).reshape(seq_count, groups, chan_count)
    decays = decay_rate.reshape(groups, state_width)
    omegas = frequency.reshape(groups, state_width)
    step_size = jnp.exp(log_step)[:, None]
    pole_mag = jnp.exp(-decays * step_size)
    pole_angle = omegas * step_size
    pole_re = pole_mag * jnp.cos(pole_angle)
    pole_im = pole_mag * jnp.sin(pole_angle)
    pole_norm = decays * decays + omegas * omegas
    diff_re = pole_re - 1.0
    lift_re = (-decays * diff_re + omegas * pole_im) / pole_norm
    lift_im = (-decays * pole_im - omegas * diff_re) / pole_norm
    in_re = input_real.reshape(chan_count, groups, state_width)
    in_im = input_imag.reshape(chan_count, groups, state_width)
    push_re = jnp.einsum('sgh,hgp->sgp', drive_f, in_re, precision=HIGH)
    push_im = jnp.einsum('sgh,hgp->sgp', drive_f, in_im, precision=HIGH)
    old_re = state_real.reshape(seq_count, groups, state_width)
    old_im = state_imag.reshape(seq_count, groups, state_width)
    new_re = pole_re * old_re - pole_im * old_im + lift_re * push_re - lift_im * push_im
    new_im = pole_re * old_im + pole_im * old_re + lift_re * push_im + lift_im * push_re
    out_re = readout_real.reshape(chan_count, groups, state_width)
    out_im = readout_imag.reshape(chan_count, groups, state_width)
    read_rows = jnp.einsum('sgp,hgp->sgh', new_re, out_re, precision=HIGH) - jnp.einsum('sgp,hgp->sgh', new_im, out_im, precision=HIGH)
    read_rows = read_rows + skip_gain.reshape(groups, chan_count) * drive_f
    activated = jax.nn.gelu(read_rows).reshape(seq_count, groups * chan_count).astype(jnp.bfloat16)
    return (activated, new_re.reshape(seq_count, groups * state_width), new_im.reshape(seq_count, groups * state_width))

def reference(tokens, norm_gain, ffn_gain, w_in, decay_rate, frequency, log_step, input_real, input_imag, readout_real, readout_imag, skip_gain, state_real, state_imag, w_out, shared_gate, shared_up, shared_down, expert_gate, expert_up, expert_down, routing, route_weight):
    normed = rms_scale(tokens, norm_gain)
    activated, new_real, new_imag = state_update(normed, w_in, decay_rate, frequency, log_step, input_real, input_imag, readout_real, readout_imag, skip_gain, state_real, state_imag)
    mixer_terms = jnp.dot(activated, w_out, preferred_element_type=jnp.float32)
    resid = (tokens.astype(jnp.float32) + mixer_terms).astype(jnp.bfloat16)
    ffn_rows = rms_scale(resid, ffn_gain)
    shared_gate_rows = jnp.dot(ffn_rows, shared_gate, preferred_element_type=jnp.float32)
    shared_up_rows = jnp.dot(ffn_rows, shared_up, preferred_element_type=jnp.float32)
    shared_inner = (jax.nn.silu(shared_gate_rows) * shared_up_rows).astype(jnp.bfloat16)
    shared = jnp.dot(shared_inner, shared_down, preferred_element_type=jnp.float32)
    seq_total = tokens.shape[0]
    expert_count = expert_gate.shape[0]
    block_count = seq_total // SEQ_DEV
    per_block = SEQ_DEV * TOP_K
    flat_ids = routing.reshape(-1).astype(jnp.int32)
    one_hot = (flat_ids[:, None] == jnp.arange(expert_count, dtype=jnp.int32)[None, :]).astype(jnp.int32)
    blocked = one_hot.reshape(block_count, per_block, expert_count)
    earlier = (jnp.cumsum(blocked, axis=1) - blocked).reshape(seq_total * TOP_K, expert_count)
    slot_rank = lax.optimization_barrier(jnp.sum(earlier * one_hot, axis=1)).astype(jnp.int32)
    block_ids = (jnp.arange(seq_total * TOP_K, dtype=jnp.int32) // per_block).astype(jnp.int32)
    buffer_rows = block_count * CAP
    column = (block_ids * CAP + slot_rank).astype(jnp.int32)
    token_ids = (jnp.arange(seq_total * TOP_K, dtype=jnp.int32) // TOP_K).astype(jnp.int32)
    table = jnp.full((expert_count, buffer_rows), seq_total, jnp.int32).at[flat_ids, column].set(token_ids)
    padded = jnp.concatenate([ffn_rows, jnp.zeros((1, ffn_rows.shape[1]), jnp.bfloat16)], axis=0)

    def one_expert(args):
        index_rows, gate_w, up_w, down_w = args
        picked = padded[index_rows].astype(jnp.float32)
        gate_rows = jnp.dot(picked, gate_w.astype(jnp.float32), preferred_element_type=jnp.float32)
        up_rows = jnp.dot(picked, up_w.astype(jnp.float32), preferred_element_type=jnp.float32)
        inner_rows = (jax.nn.silu(gate_rows) * up_rows).astype(jnp.bfloat16)
        return jnp.dot(inner_rows.astype(jnp.float32), down_w.astype(jnp.float32), preferred_element_type=jnp.float32)
    outputs = lax.map(one_expert, (table, expert_gate, expert_up, expert_down))
    flat_out = outputs.reshape(expert_count * buffer_rows, outputs.shape[2])
    picked_rows = flat_out[(flat_ids * buffer_rows + column).astype(jnp.int32)].reshape(seq_total, TOP_K, outputs.shape[2])
    weights = route_weight / lax.optimization_barrier(jnp.sum(route_weight, axis=1, keepdims=True)) * ROUTED_SCALE
    routed = lax.optimization_barrier(jnp.sum(weights[:, :, None] * picked_rows, axis=1))
    mixed = (resid.astype(jnp.float32) + shared + routed).astype(jnp.bfloat16)
    return (mixed, new_real, new_imag)
```

```python
import jax
import jax.numpy as jnp
from jax import lax
from jax.sharding import Mesh
from jax.sharding import PartitionSpec as P

EPS = 1e-06
ROUTED_SCALE = 2.5
HIGH = lax.Precision.HIGHEST
TP = ("z", "c")


def swapped(x):
    return lax.ppermute(x, "c", [(0, 1), (1, 0)])


def sent_to_all(x, axis):
    copies = jnp.broadcast_to(x, (lax.axis_size(axis), *x.shape))
    return lax.all_to_all(copies, axis, split_axis=0, concat_axis=0, tiled=True)


def of_pair(x, which, dim):
    width = x.shape[dim] // 2
    return lax.dynamic_slice_in_dim(x, which * width, width, dim)


def summed_over_tp(parts, c):
    halves = parts.astype(jnp.bfloat16)
    kept = lax.dynamic_index_in_dim(halves, c, 1, keepdims=False)
    given = lax.dynamic_index_in_dim(halves, 1 - c, 1, keepdims=False)
    got = swapped(given)
    both = (kept.astype(jnp.float32) + got.astype(jnp.float32)).astype(jnp.bfloat16)
    arrived = lax.all_to_all(both, "z", split_axis=0, concat_axis=0, tiled=True)
    return arrived.astype(jnp.float32).sum(axis=0)


def rms_scale(values_in, gains):
    values = values_in.astype(jnp.float32)
    factor = lax.rsqrt(jnp.mean(values * values, axis=-1, keepdims=True) + EPS)
    return (values * factor * gains).astype(jnp.bfloat16)


def state_update(
    normed,
    w_in,
    decay_rate,
    frequency,
    log_step,
    input_real,
    input_imag,
    readout_real,
    readout_imag,
    skip_gain,
    state_real,
    state_imag,
):
    seq_count = normed.shape[0]
    groups = log_step.shape[0]
    chan_count = skip_gain.shape[0] // groups
    state_width = decay_rate.shape[0] // groups
    drive_rows = jnp.dot(normed, w_in, preferred_element_type=jnp.float32).astype(jnp.bfloat16)
    drive_f = drive_rows.astype(jnp.float32).reshape(seq_count, groups, chan_count)
    decays = decay_rate.reshape(groups, state_width)
    omegas = frequency.reshape(groups, state_width)
    step_size = jnp.exp(log_step)[:, None]
    pole_mag = jnp.exp(-decays * step_size)
    pole_angle = omegas * step_size
    pole_re = pole_mag * jnp.cos(pole_angle)
    pole_im = pole_mag * jnp.sin(pole_angle)
    pole_norm = decays * decays + omegas * omegas
    diff_re = pole_re - 1.0
    lift_re = (-decays * diff_re + omegas * pole_im) / pole_norm
    lift_im = (-decays * pole_im - omegas * diff_re) / pole_norm
    in_re = input_real.reshape(chan_count, groups, state_width)
    in_im = input_imag.reshape(chan_count, groups, state_width)
    push_re = jnp.einsum("sgh,hgp->sgp", drive_f, in_re, precision=HIGH)
    push_im = jnp.einsum("sgh,hgp->sgp", drive_f, in_im, precision=HIGH)
    old_re = state_real.reshape(seq_count, groups, state_width)
    old_im = state_imag.reshape(seq_count, groups, state_width)
    new_re = pole_re * old_re - pole_im * old_im + lift_re * push_re - lift_im * push_im
    new_im = pole_re * old_im + pole_im * old_re + lift_re * push_im + lift_im * push_re
    out_re = readout_real.reshape(chan_count, groups, state_width)
    out_im = readout_imag.reshape(chan_count, groups, state_width)
    read_rows = jnp.einsum("sgp,hgp->sgh", new_re, out_re, precision=HIGH) - jnp.einsum(
        "sgp,hgp->sgh", new_im, out_im, precision=HIGH
    )
    read_rows = read_rows + skip_gain.reshape(groups, chan_count) * drive_f
    activated = jax.nn.gelu(read_rows).reshape(seq_count, groups * chan_count).astype(jnp.bfloat16)
    return (
        activated,
        new_re.reshape(seq_count, groups * state_width),
        new_im.reshape(seq_count, groups * state_width),
    )


def local(
    tokens,
    norm_gain,
    ffn_gain,
    w_in,
    decay_rate,
    frequency,
    log_step,
    input_real,
    input_imag,
    readout_real,
    readout_imag,
    skip_gain,
    state_real,
    state_imag,
    w_out,
    shared_gate,
    shared_up,
    shared_down,
    expert_gate,
    expert_up,
    expert_down,
    routing,
    route_weight,
):
    bf16, f32 = jnp.bfloat16, jnp.float32
    seq_count, model_width = tokens.shape
    ep_count, z_count = lax.axis_size("ep"), lax.axis_size("z")
    z, c = lax.axis_index("z"), lax.axis_index("c")
    slice_width = model_width // (2 * z_count)
    offset = (2 * z + c) * slice_width
    other_offset = (2 * z + 1 - c) * slice_width

    gate_own, up_own, down_own = (of_pair(w, c, 0) for w in (expert_gate, expert_up, expert_down))
    gate_par, up_par, down_par = (
        swapped(of_pair(w, 1 - c, 0)) for w in (expert_gate, expert_up, expert_down)
    )

    normed = rms_scale(tokens, norm_gain)
    activated, new_real, new_imag = state_update(
        normed,
        w_in,
        decay_rate,
        frequency,
        log_step,
        input_real,
        input_imag,
        readout_real,
        readout_imag,
        skip_gain,
        state_real,
        state_imag,
    )
    mixer_parts = jnp.einsum(
        "sk,kzcd->zcsd",
        activated,
        w_out.reshape(-1, z_count, 2, slice_width),
        preferred_element_type=f32,
    )
    mixer_own = summed_over_tp(mixer_parts, c)
    own_tokens = lax.dynamic_slice_in_dim(tokens, offset, slice_width, 1)
    resid_own = (own_tokens.astype(f32) + mixer_own).astype(bf16)

    expert_dev = expert_gate.shape[0]
    expert_count = expert_dev * ep_count
    top_count = routing.shape[1]
    capacity = 2 * seq_count * top_count // expert_count
    slot_count = expert_count * capacity
    flat_ids = routing.reshape(-1)
    one_hot = (flat_ids[:, None] == jnp.arange(expert_count, dtype=jnp.int32)[None, :]).astype(
        jnp.int32
    )
    earlier = jnp.cumsum(one_hot, axis=0) - one_hot
    slot_rank = jnp.sum(earlier * one_hot, axis=1)
    target = jnp.bitwise_xor(flat_ids, c * (expert_dev // 2)) * capacity + slot_rank
    slot_ids = jnp.arange(slot_count, dtype=jnp.int32)
    placed = (target[None, :] == slot_ids[:, None]).reshape(slot_count, seq_count, top_count)
    dispatch_map = jnp.sum(placed.astype(f32), axis=2).astype(bf16)
    outgoing = jnp.dot(dispatch_map, resid_own, preferred_element_type=f32).astype(bf16)
    outgoing = outgoing.reshape(ep_count, expert_dev * capacity, slice_width)
    incoming = lax.all_to_all(outgoing, "ep", split_axis=0, concat_axis=0, tiled=True)

    along_z = sent_to_all(resid_own, "z")
    across = swapped(along_z)
    first = jnp.where(c == 0, along_z, across)
    second = jnp.where(c == 0, across, along_z)
    resid_rows = jnp.stack([first, second], axis=1)
    resid_rows = resid_rows.transpose(2, 0, 1, 3).reshape(seq_count, model_width)
    ffn_rows = rms_scale(resid_rows, ffn_gain)
    shared_gate_rows = jnp.dot(ffn_rows, shared_gate, preferred_element_type=f32)
    shared_up_rows = jnp.dot(ffn_rows, shared_up, preferred_element_type=f32)
    shared_inner = (jax.nn.silu(shared_gate_rows) * shared_up_rows).astype(bf16)
    shared_parts = jnp.einsum(
        "sf,fzcd->zcsd",
        shared_inner,
        shared_down.reshape(-1, z_count, 2, slice_width),
        preferred_element_type=f32,
    )
    shared_own = summed_over_tp(shared_parts, c)

    half = expert_dev // 2
    pair_rows = half * ep_count * capacity
    arrived = incoming.reshape(ep_count, 2, half, capacity, slice_width)
    rows_own, rows_given = arrived[:, 0], arrived[:, 1]
    rows_par = swapped(rows_given)
    gain_own = lax.dynamic_slice_in_dim(ffn_gain, offset, slice_width, 0)
    gain_par = lax.dynamic_slice_in_dim(ffn_gain, other_offset, slice_width, 0)
    own_f, par_f = rows_own.astype(f32), rows_par.astype(f32)
    squares = jnp.sum(own_f * own_f, axis=-1) + jnp.sum(par_f * par_f, axis=-1)
    squares = squares.transpose(1, 0, 2).reshape(-1)
    squares_high = squares.astype(bf16)
    squares_low = (squares - squares_high.astype(f32)).astype(bf16)
    scaled_own = (own_f * gain_own).astype(bf16)
    scaled_par = (par_f * gain_par).astype(bf16)

    def sums(w_own, w_par):
        def one(rows, w):
            return jnp.einsum("secd,edf->escf", rows, w, preferred_element_type=f32)

        whole = one(scaled_own, w_own) + one(scaled_par, w_par)
        return whole.astype(bf16).reshape(pair_rows, z_count, -1).transpose(1, 0, 2)

    gate_parts, up_parts = sums(gate_own, gate_par), sums(up_own, up_par)
    lanes = gate_parts.shape[2]
    extra = jnp.concatenate([squares_high, squares_low]).reshape(1, -1, lanes)
    extra = jnp.broadcast_to(extra, (z_count, *extra.shape[1:]))
    parcel = jnp.concatenate([gate_parts, up_parts, extra], axis=1)
    parcels = lax.all_to_all(parcel, "z", split_axis=0, concat_axis=0, tiled=True)
    totals = parcels.astype(f32).sum(axis=0)
    squares_all = totals[2 * pair_rows :].reshape(2, pair_rows).sum(axis=0)
    factor = lax.rsqrt(squares_all / model_width + EPS)[:, None]
    gate_rows, up_rows = totals[:pair_rows] * factor, totals[pair_rows : 2 * pair_rows] * factor
    inner = (jax.nn.silu(gate_rows) * up_rows).astype(bf16)
    inner_all = sent_to_all(inner, "z").reshape(z_count, half, -1, lanes)

    def down(w):
        w_f = w.reshape(half, z_count, lanes, slice_width)
        out = jnp.einsum("zerf,ezfd->erd", inner_all, w_f, preferred_element_type=f32)
        out = out.astype(bf16).reshape(half, ep_count, capacity, slice_width)
        return out.transpose(1, 0, 2, 3).reshape(ep_count, half * capacity, slice_width)

    out_own, out_given = down(down_own), down(down_par)
    results = jnp.concatenate([out_own, swapped(out_given)], axis=1)
    returned = lax.all_to_all(results, "ep", split_axis=0, concat_axis=0, tiled=True).astype(f32)

    weights = route_weight / jnp.sum(route_weight, axis=1, keepdims=True) * ROUTED_SCALE
    chosen = target.reshape(seq_count, top_count)[:, :, None] == slot_ids[None, None, :]
    combine = jnp.sum(jnp.where(chosen, weights[:, :, None], 0.0), axis=1)
    routed = jnp.dot(combine, returned.reshape(slot_count, slice_width), precision=HIGH)
    mixed = (resid_own.astype(f32) + shared_own + routed).astype(bf16)
    return (mixed, new_real, new_imag)


def solution(mesh):
    ep_count, tp_count = mesh.devices.shape
    cores = Mesh(mesh.devices.reshape(ep_count, tp_count // 2, 2), ("ep", "z", "c"))
    placed = (
        P("ep", None),
        P(),
        P(),
        P(None, TP),
        P(TP),
        P(TP),
        P(TP),
        P(None, TP),
        P(None, TP),
        P(None, TP),
        P(None, TP),
        P(TP),
        P("ep", TP),
        P("ep", TP),
        P(TP, None),
        P(None, TP),
        P(None, TP),
        P(TP, None),
        P("ep", TP, None),
        P("ep", TP, None),
        P("ep", None, TP),
        P("ep", None),
        P("ep", None),
    )
    return jax.shard_map(
        local,
        mesh=cores,
        in_specs=placed,
        out_specs=(P("ep", TP), P("ep", TP), P("ep", TP)),
        check_vma=False,
    )
```

```python
import functools

import jax
import jax.numpy as jnp
from jax import lax
from jax.experimental import pallas as pl
from jax.experimental.pallas import tpu as pltpu
from jax.sharding import Mesh
from jax.sharding import PartitionSpec as P

EPS = 1e-06
ROUTED_SCALE = 2.5
HIGH = lax.Precision.HIGHEST
TP = ("z", "c")
F32, BF16 = jnp.float32, jnp.bfloat16


def swapped(x):
    return lax.ppermute(x, "c", [(0, 1), (1, 0)])


def exchanged(x, axis, bit):
    return lax.ppermute(x, axis, [(i, i ^ bit) for i in range(lax.axis_size(axis))])


def of_pair(x, which, dim):
    width = x.shape[dim] // 2
    return lax.dynamic_slice_in_dim(x, which * width, width, dim)


def of_bit(x, bit):
    return jnp.where(bit == 0, x[0], x[1])


def rms_scale(values_in, gains):
    values = values_in.astype(F32)
    factor = lax.rsqrt(jnp.mean(values * values, axis=-1, keepdims=True) + EPS)
    return (values * factor * gains).astype(BF16)


def dot32(a, b):
    return jnp.dot(a, b, preferred_element_type=F32)


def dot_nt(a, b):
    return lax.dot_general(a, b, (((1,), (1,)), ((), ())), preferred_element_type=F32)


def two_parts(x):
    high = x.astype(BF16)
    return high, (x - high.astype(F32)).astype(BF16)


def cost(flops, moved):
    return pl.CostEstimate(flops=flops, bytes_accessed=moved, transcendentals=0)


def front_kernel(
    core,
    log_step,
    tokens,
    norm_gain,
    w_in,
    decay_rate,
    frequency,
    input_real,
    input_imag,
    readout_real,
    readout_imag,
    skip_gain,
    state_real,
    state_imag,
    w_out,
    new_real,
    new_imag,
    kept,
    given,
):
    groups = log_step.shape[0]
    chan_count, entries = input_real.shape
    channels = skip_gain.shape[1]
    width = entries // groups
    normed = rms_scale(tokens[...], norm_gain[...])
    drive = dot32(normed, w_in[...]).astype(BF16)
    group_of = lax.broadcasted_iota(jnp.int32, (1, entries), 1) // width
    step_size = jnp.zeros((1, entries), F32)
    for g in range(groups):
        step_size = jnp.where(group_of == g, log_step[g], step_size)
    step_size = jnp.exp(step_size)
    decays, omegas = decay_rate[...], frequency[...]
    pole_mag = jnp.exp(-decays * step_size)
    pole_angle = omegas * step_size
    pole_re = pole_mag * jnp.cos(pole_angle)
    pole_im = pole_mag * jnp.sin(pole_angle)
    pole_norm = decays * decays + omegas * omegas
    diff_re = pole_re - 1.0
    lift_re = (-decays * diff_re + omegas * pole_im) / pole_norm
    lift_im = (-decays * pole_im - omegas * diff_re) / pole_norm
    row_group = lax.broadcasted_iota(jnp.int32, (channels, entries), 0) // chan_count
    col_group = lax.broadcasted_iota(jnp.int32, (channels, entries), 1) // width
    same = row_group == col_group

    def spread(block):
        return two_parts(jnp.where(same, jnp.concatenate([block[...]] * groups, axis=0), 0.0))

    def push_of(block):
        high, low = spread(block)
        return dot32(drive, high) + dot32(drive, low)

    push_re, push_im = push_of(input_real), push_of(input_imag)
    old_re, old_im = state_real[...], state_imag[...]
    new_re = pole_re * old_re - pole_im * old_im + lift_re * push_re - lift_im * push_im
    new_im = pole_re * old_im + pole_im * old_re + lift_re * push_im + lift_im * push_re
    new_real[...] = new_re
    new_imag[...] = new_im

    def read_of(state, block):
        (high, low), (block_high, block_low) = two_parts(state), spread(block)
        return dot_nt(high, block_high) + dot_nt(high, block_low) + dot_nt(low, block_high)

    read = read_of(new_re, readout_real) - read_of(new_im, readout_imag)
    read = read + skip_gain[...] * drive.astype(F32)
    bent = jnp.tanh(0.7978845608028654 * (read + 0.044715 * (read * read * read)))
    activated = (0.5 * read * (1.0 + bent)).astype(BF16)
    wide = kept.shape[2]
    for z in range(kept.shape[0]):
        for out, c in ((kept, core[0]), (given, 1 - core[0])):
            at = pl.multiple_of((2 * z + c) * wide, wide)
            out[z] = dot32(activated, w_out[:, pl.ds(at, wide)]).astype(out.dtype)


def front(core, log_step, *arrays):
    tokens, w_out, state = arrays[0], arrays[-1], arrays[-2]
    seqs, model_width = tokens.shape
    z_count = lax.axis_size("z")
    part = (z_count, seqs, model_width // (2 * z_count))
    smem, vmem = pl.BlockSpec(memory_space=pltpu.SMEM), pl.BlockSpec(memory_space=pltpu.VMEM)
    return pl.pallas_call(
        front_kernel,
        out_shape=(
            jax.ShapeDtypeStruct(state.shape, F32),
            jax.ShapeDtypeStruct(state.shape, F32),
            jax.ShapeDtypeStruct(part, F32),
            jax.ShapeDtypeStruct(part, BF16),
        ),
        in_specs=[smem, smem] + [vmem] * len(arrays),
        out_specs=(vmem,) * 4,
        cost_estimate=cost(4 * seqs * model_width * w_out.shape[0], 2 * w_out.size * 2),
        name="front",
    )(core, log_step, *arrays)


def gate_up_kernel(core, own, par, gain_own, gain_par, gate_own, gate_par, up_own, up_par, parcel):
    e = pl.program_id(0)
    seq_devs, _, _, capacity, width = own.shape
    rows = seq_devs * capacity
    z_count, _, lanes = parcel.shape
    ones = jnp.ones((8, width), BF16)
    squares = jnp.zeros((8, rows), F32)
    scaled = []
    for part, gain in ((own, gain_own), (par, gain_par)):
        values = part[...].reshape(rows, width).astype(F32)
        scaled.append((values * gain[...]).astype(BF16))
        high, low = two_parts(values * values)
        squares = squares + dot_nt(ones, high) + dot_nt(ones, low)
    for at, w_own, w_par in ((0, gate_own, gate_par), (2 * rows, up_own, up_par)):
        sums = dot32(scaled[0], w_own[0]) + dot32(scaled[1], w_par[0])
        sums = sums.astype(BF16)
        for z in range(z_count):
            parcel[z, pl.ds(at + e * rows, rows), :] = sums[:, z * lanes : (z + 1) * lanes]
    high, low = two_parts(squares)
    line = lax.broadcasted_iota(jnp.int32, squares.shape, 0)
    both = jnp.where(line == 0, high.astype(F32), jnp.where(line == 1, low.astype(F32), 0.0))
    for z in range(z_count):
        parcel[z, pl.ds(4 * rows + e * 8, 8), :] = both.astype(BF16)


def gate_up(core, incoming, par, gain_own, gain_par, gate, gate_par, up, up_par):
    seq_devs, _, half, capacity, width = incoming.shape
    z_count = lax.axis_size("z")
    rows, units = seq_devs * capacity, gate.shape[2]
    lanes = units // z_count
    mine = pl.BlockSpec((1, width, units), lambda e, c: (half * c[0] + e, 0, 0))
    theirs = pl.BlockSpec((1, width, units), lambda e, c: (e, 0, 0))
    block = (seq_devs, 1, 1, capacity, width)
    gain = pl.BlockSpec((1, width), lambda e, c: (0, 0))
    depth = 2 * half * rows + half * 8
    return pl.pallas_call(
        gate_up_kernel,
        grid_spec=pltpu.PrefetchScalarGridSpec(
            num_scalar_prefetch=1,
            grid=(half,),
            in_specs=[
                pl.BlockSpec(block, lambda e, c: (0, 0, e, 0, 0)),
                pl.BlockSpec(block, lambda e, c: (0, 0, e, 0, 0)),
                gain,
                gain,
                mine,
                theirs,
                mine,
                theirs,
            ],
            out_specs=pl.BlockSpec((z_count, depth, lanes), lambda e, c: (0, 0, 0)),
        ),
        out_shape=jax.ShapeDtypeStruct((z_count, depth, lanes), BF16),
        cost_estimate=cost(8 * half * rows * width * units, 8 * half * width * units),
        name="gate_up",
    )(core, incoming, par, gain_own, gain_par, gate, gate_par, up, up_par)


def inner_kernel(model_width, half, parcels, inner):
    totals = parcels[0].astype(F32)
    z_count = parcels.shape[0]
    for z in range(1, z_count):
        totals = totals + parcels[z].astype(F32)
    lanes = totals.shape[1]
    pair_rows = inner.shape[1]
    rows = pair_rows // half
    for e in range(half):
        line = 2 * pair_rows + 8 * e
        squares = totals[line : line + 1] + totals[line + 1 : line + 2]
        factor = lax.rsqrt(squares / model_width + EPS)
        factor = jnp.broadcast_to(factor, (lanes, rows)).T
        gate = totals[e * rows : (e + 1) * rows] * factor
        up = totals[pair_rows + e * rows : pair_rows + (e + 1) * rows] * factor
        done = (gate / (1.0 + jnp.exp(-gate)) * up).astype(BF16)
        for z in range(z_count):
            inner[z, e * rows : (e + 1) * rows, :] = done


def inner_copies(parcels, model_width, half):
    z_count, depth, lanes = parcels.shape
    pair_rows = (depth - half * 8) // 2
    return pl.pallas_call(
        functools.partial(inner_kernel, model_width, half),
        out_shape=jax.ShapeDtypeStruct((z_count, pair_rows, lanes), BF16),
        in_specs=[pl.BlockSpec(memory_space=pltpu.VMEM)],
        out_specs=pl.BlockSpec(memory_space=pltpu.VMEM),
        cost_estimate=cost(parcels.size * 4, parcels.size * 4),
        name="inner",
    )(parcels)


def down_kernel(core, inner, down_own, down_par, own, given):
    z_count = inner.shape[0]
    row = jnp.concatenate([inner[z] for z in range(z_count)], axis=1)
    for out, w in ((own, down_own), (given, down_par)):
        out[...] = dot32(row, w[0]).astype(BF16).reshape(out.shape)


def down(core, inner, w_down, w_par, seq_devs, capacity):
    half = w_par.shape[0]
    z_count, pair_rows, lanes = inner.shape
    units, width = w_par.shape[1:]
    rows = pair_rows // half
    out = pl.BlockSpec((seq_devs, capacity, width), lambda e, c: (0, e, 0))
    shape = jax.ShapeDtypeStruct((seq_devs, half * capacity, width), BF16)
    return pl.pallas_call(
        down_kernel,
        grid_spec=pltpu.PrefetchScalarGridSpec(
            num_scalar_prefetch=1,
            grid=(half,),
            in_specs=[
                pl.BlockSpec((z_count, rows, lanes), lambda e, c: (0, e, 0)),
                pl.BlockSpec((1, units, width), lambda e, c: (half * c[0] + e, 0, 0)),
                pl.BlockSpec((1, units, width), lambda e, c: (e, 0, 0)),
            ],
            out_specs=(out, out),
        ),
        out_shape=(shape, shape),
        cost_estimate=cost(4 * half * rows * units * width, 4 * half * units * width),
        name="down",
    )(core, inner, w_down, w_par)


def local(
    tokens,
    norm_gain,
    ffn_gain,
    w_in,
    decay_rate,
    frequency,
    log_step,
    input_real,
    input_imag,
    readout_real,
    readout_imag,
    skip_gain,
    state_real,
    state_imag,
    w_out,
    shared_gate,
    shared_up,
    shared_down,
    expert_gate,
    expert_up,
    expert_down,
    routing,
    route_weight,
):
    seq_count, model_width = tokens.shape
    ep_count, z_count = lax.axis_size("ep"), lax.axis_size("z")
    z, c = lax.axis_index("z"), lax.axis_index("c")
    core = c.reshape(1)
    slice_width = model_width // (2 * z_count)
    offset = (2 * z + c) * slice_width
    other_offset = (2 * z + 1 - c) * slice_width

    gate_par, up_par, down_par = (
        swapped(of_pair(w, 1 - c, 0)) for w in (expert_gate, expert_up, expert_down)
    )

    new_real, new_imag, kept, given = front(
        core,
        log_step,
        tokens,
        norm_gain.reshape(1, -1),
        w_in,
        decay_rate.reshape(1, -1),
        frequency.reshape(1, -1),
        input_real,
        input_imag,
        readout_real,
        readout_imag,
        skip_gain.reshape(1, -1),
        state_real,
        state_imag,
        w_out,
    )
    both = (kept + swapped(given).astype(F32)).astype(BF16)
    mixer_own = lax.all_to_all(both, "z", split_axis=0, concat_axis=0, tiled=True)
    mixer_own = mixer_own.astype(F32).sum(axis=0)
    own_tokens = lax.dynamic_slice_in_dim(tokens, offset, slice_width, 1)
    resid_own = (own_tokens.astype(F32) + mixer_own).astype(BF16)

    expert_dev = expert_gate.shape[0]
    expert_count = expert_dev * ep_count
    top_count = routing.shape[1]
    capacity = 2 * seq_count * top_count // expert_count
    slot_count = expert_count * capacity
    flat_ids = routing.reshape(-1)
    one_hot = (flat_ids[:, None] == jnp.arange(expert_count, dtype=jnp.int32)[None, :]).astype(
        jnp.int32
    )
    earlier = jnp.cumsum(one_hot, axis=0) - one_hot
    slot_rank = jnp.sum(earlier * one_hot, axis=1)
    target = jnp.bitwise_xor(flat_ids, c * (expert_dev // 2)) * capacity + slot_rank
    slot_ids = jnp.arange(slot_count, dtype=jnp.int32)
    placed = (target[None, :] == slot_ids[:, None]).reshape(slot_count, seq_count, top_count)
    dispatch_map = jnp.sum(placed.astype(F32), axis=2).astype(BF16)
    outgoing = jnp.dot(dispatch_map, resid_own, preferred_element_type=F32).astype(BF16)
    outgoing = outgoing.reshape(ep_count, expert_dev * capacity, slice_width)
    incoming = lax.all_to_all(outgoing, "ep", split_axis=0, concat_axis=0, tiled=True)

    half = expert_dev // 2
    arrived = incoming.reshape(ep_count, 2, half, capacity, slice_width)
    parcel = gate_up(
        core,
        arrived,
        swapped(arrived[:, 1:]),
        lax.dynamic_slice_in_dim(ffn_gain, offset, slice_width, 0).reshape(1, -1),
        lax.dynamic_slice_in_dim(ffn_gain, other_offset, slice_width, 0).reshape(1, -1),
        expert_gate,
        gate_par,
        expert_up,
        up_par,
    )
    parcels = lax.all_to_all(parcel, "z", split_axis=0, concat_axis=0, tiled=True)
    copies = inner_copies(parcels, model_width, half)
    inner_all = lax.all_to_all(copies, "z", split_axis=0, concat_axis=0, tiled=True)
    out_own, out_given = down(core, inner_all, expert_down, down_par, ep_count, capacity)
    results = jnp.concatenate([out_own, swapped(out_given)], axis=1)
    returned = lax.all_to_all(results, "ep", split_axis=0, concat_axis=0, tiled=True).astype(F32)

    grown = resid_own[None]
    bit = 1
    while bit < z_count:
        theirs = exchanged(grown, "z", bit)
        low = (z & bit) == 0
        grown = jnp.stack([jnp.where(low, grown, theirs), jnp.where(low, theirs, grown)])
        grown = grown.reshape(-1, seq_count, slice_width)
        bit *= 2
    across = swapped(grown)
    first, second = jnp.where(c == 0, grown, across), jnp.where(c == 0, across, grown)
    resid_rows = jnp.stack([first, second], axis=1)
    resid_rows = resid_rows.transpose(2, 0, 1, 3).reshape(seq_count, model_width)
    ffn_rows = rms_scale(resid_rows, ffn_gain)
    shared_gate_rows, shared_up_rows = dot32(ffn_rows, shared_gate), dot32(ffn_rows, shared_up)
    shared_inner = (jax.nn.silu(shared_gate_rows) * shared_up_rows).astype(BF16)
    shared_parts = jnp.einsum(
        "sf,fzcd->czsd",
        shared_inner,
        shared_down.reshape(-1, z_count, 2, slice_width),
        preferred_element_type=F32,
    )
    shared_own = of_bit(shared_parts, c)
    shared_own = shared_own + swapped(of_bit(shared_parts, 1 - c).astype(BF16)).astype(F32)
    bit = z_count // 2
    while bit > 0:
        halves = shared_own.reshape(2, -1, seq_count, slice_width)
        high = (z & bit) // bit
        theirs = exchanged(of_bit(halves, 1 - high).astype(BF16), "z", bit)
        shared_own = of_bit(halves, high) + theirs.astype(F32)
        bit //= 2
    shared_own = shared_own[0]

    weights = route_weight / jnp.sum(route_weight, axis=1, keepdims=True) * ROUTED_SCALE
    chosen = target.reshape(seq_count, top_count)[:, :, None] == slot_ids[None, None, :]
    combine = jnp.sum(jnp.where(chosen, weights[:, :, None], 0.0), axis=1)
    routed = jnp.dot(combine, returned.reshape(slot_count, slice_width), precision=HIGH)
    mixed = (resid_own.astype(F32) + shared_own + routed).astype(BF16)
    return (mixed, new_real, new_imag)


def solution(mesh):
    ep_count, tp_count = mesh.devices.shape
    cores = Mesh(mesh.devices.reshape(ep_count, tp_count // 2, 2), ("ep", "z", "c"))
    placed = (
        P("ep", None),
        P(),
        P(),
        P(None, TP),
        P(TP),
        P(TP),
        P(TP),
        P(None, TP),
        P(None, TP),
        P(None, TP),
        P(None, TP),
        P(TP),
        P("ep", TP),
        P("ep", TP),
        P(TP, None),
        P(None, TP),
        P(None, TP),
        P(TP, None),
        P("ep", TP, None),
        P("ep", TP, None),
        P("ep", None, TP),
        P("ep", None),
        P("ep", None),
    )
    return jax.shard_map(
        local,
        mesh=cores,
        in_specs=placed,
        out_specs=(P("ep", TP), P("ep", TP), P("ep", TP)),
        check_vma=False,
    )
```

```python
import functools

import jax
import jax.numpy as jnp
from jax import lax
from jax.experimental import pallas as pl
from jax.experimental.pallas import tpu as pltpu
from jax.sharding import Mesh
from jax.sharding import PartitionSpec as P


EPS = 1e-06
ROUTED_SCALE = 2.5
TP = ("z", "c")
F32, BF16 = jnp.float32, jnp.bfloat16
ROOM = pltpu.CompilerParams(vmem_limit_bytes=20 * 2**20)


def swapped(x):
    return lax.ppermute(x, "c", [(0, 1), (1, 0)])


def exchanged(x, axis, bit):
    return lax.ppermute(x, axis, [(i, i ^ bit) for i in range(lax.axis_size(axis))])


def of_pair(x, which, dim):
    width = x.shape[dim] // 2
    return lax.dynamic_slice_in_dim(x, which * width, width, dim)


def rms_scale(values_in, gains):
    values = values_in.astype(F32)
    factor = lax.rsqrt(jnp.mean(values * values, axis=-1, keepdims=True) + EPS)
    return (values * factor * gains).astype(BF16)


def dot32(a, b):
    return jnp.dot(a, b, preferred_element_type=F32)


def dot_nt(a, b):
    return lax.dot_general(a, b, (((1,), (1,)), ((), ())), preferred_element_type=F32)


def two_parts(x):
    high = x.astype(BF16)
    return high, (x - high.astype(F32)).astype(BF16)


def cost(flops, moved):
    return pl.CostEstimate(flops=flops, bytes_accessed=moved, transcendentals=0)


def fetch(source, target, arrival):
    copy = pltpu.make_async_copy(source, target, arrival)
    copy.start()
    copy.wait()


def front_kernel(
    core,
    log_step,
    tokens,
    norm_gain,
    w_in,
    decay_rate,
    frequency,
    input_real,
    input_imag,
    readout_real,
    readout_imag,
    skip_gain,
    state_real,
    state_imag,
    w_out,
    new_real,
    new_imag,
    kept,
    given,
):
    groups = log_step.shape[0]
    chan_count, entries = input_real.shape
    channels = skip_gain.shape[1]
    width = entries // groups
    normed = rms_scale(tokens[...], norm_gain[...])
    drive = dot32(normed, w_in[...]).astype(BF16)
    group_of = lax.broadcasted_iota(jnp.int32, (1, entries), 1) // width
    step_size = jnp.zeros((1, entries), F32)
    for g in range(groups):
        step_size = jnp.where(group_of == g, log_step[g], step_size)
    step_size = jnp.exp(step_size)
    decays, omegas = decay_rate[...], frequency[...]
    pole_mag = jnp.exp(-decays * step_size)
    pole_angle = omegas * step_size
    pole_re = pole_mag * jnp.cos(pole_angle)
    pole_im = pole_mag * jnp.sin(pole_angle)
    pole_norm = decays * decays + omegas * omegas
    diff_re = pole_re - 1.0
    lift_re = (-decays * diff_re + omegas * pole_im) / pole_norm
    lift_im = (-decays * pole_im - omegas * diff_re) / pole_norm
    row_group = lax.broadcasted_iota(jnp.int32, (channels, entries), 0) // chan_count
    col_group = lax.broadcasted_iota(jnp.int32, (channels, entries), 1) // width
    same = row_group == col_group

    def spread(block):
        return two_parts(jnp.where(same, jnp.concatenate([block[...]] * groups, axis=0), 0.0))

    def push_of(block):
        high, low = spread(block)
        return dot32(drive, high) + dot32(drive, low)

    push_re, push_im = push_of(input_real), push_of(input_imag)
    old_re, old_im = state_real[...], state_imag[...]
    new_re = pole_re * old_re - pole_im * old_im + lift_re * push_re - lift_im * push_im
    new_im = pole_re * old_im + pole_im * old_re + lift_re * push_im + lift_im * push_re
    new_real[...] = new_re
    new_imag[...] = new_im

    def read_of(state, block):
        (high, low), (block_high, block_low) = two_parts(state), spread(block)
        return dot_nt(high, block_high) + dot_nt(high, block_low) + dot_nt(low, block_high)

    read = read_of(new_re, readout_real) - read_of(new_im, readout_imag)
    read = read + skip_gain[...] * drive.astype(F32)
    bent = jnp.tanh(0.7978845608028654 * (read + 0.044715 * (read * read * read)))
    activated = (0.5 * read * (1.0 + bent)).astype(BF16)
    wide = kept.shape[2]
    for z in range(kept.shape[0]):
        for out, c in ((kept, core[0]), (given, 1 - core[0])):
            at = pl.multiple_of((2 * z + c) * wide, wide)
            out[z] = dot32(activated, w_out[:, pl.ds(at, wide)]).astype(out.dtype)


def front(core, log_step, *arrays):
    tokens, w_out, state = arrays[0], arrays[-1], arrays[-2]
    seqs, model_width = tokens.shape
    z_count = lax.axis_size("z")
    part = (z_count, seqs, model_width // (2 * z_count))
    smem, vmem = pl.BlockSpec(memory_space=pltpu.SMEM), pl.BlockSpec(memory_space=pltpu.VMEM)
    return pl.pallas_call(
        front_kernel,
        out_shape=(
            jax.ShapeDtypeStruct(state.shape, F32),
            jax.ShapeDtypeStruct(state.shape, F32),
            jax.ShapeDtypeStruct(part, F32),
            jax.ShapeDtypeStruct(part, BF16),
        ),
        in_specs=[smem, smem] + [vmem] * len(arrays),
        out_specs=(vmem,) * 4,
        cost_estimate=cost(4 * seqs * model_width * w_out.shape[0], 2 * w_out.size * 2),
        name="front",
    )(core, log_step, *arrays)


def gate_up_kernel(
    at, arrived, gain, gate, gate_par, up, up_par, sent, incoming, weights, parcel, ins, outs
):
    half, _, _, width, _ = weights.shape
    seq_devs, _, pair_slots, _ = incoming.shape
    z_count, _, lanes = parcel.shape
    capacity = pair_slots // half
    rows = seq_devs * capacity
    first = pltpu.make_async_copy(arrived, incoming, ins.at[0])
    first.start()
    loads = {}
    for e in range(half):
        for m, (own, par) in enumerate(((gate, gate_par), (up, up_par))):
            for part, source in enumerate((own.at[half * at[0] + e], par.at[e])):
                arrival = ins.at[1 + 4 * e + 2 * m + part]
                copy = pltpu.make_async_copy(source, weights.at[e, m, part], arrival)
                copy.start()
                loads[e, m, part] = copy
    ones = jnp.ones((8, width), BF16)
    features = [pl.ds(pl.multiple_of(at[1 + part] * width, width), width) for part in range(2)]
    first.wait()
    stores = []

    def store(depth, size):
        place = pl.ds(depth, size)
        copy = pltpu.make_async_copy(
            parcel.at[:, place, :], sent.at[:, place, :], outs.at[len(stores)]
        )
        copy.start()
        stores.append(copy)

    scaled = {}
    for e in range(half):
        squares = jnp.zeros((8, rows), F32)
        for part in range(2):
            values = incoming[:, part, e * capacity : (e + 1) * capacity, :]
            values = values.reshape(rows, width).astype(F32)
            scaled[e, part] = (values * gain[:, features[part]]).astype(BF16)
            high, low = two_parts(values * values)
            squares = squares + dot_nt(ones, high) + dot_nt(ones, low)
        high, low = two_parts(squares)
        line = lax.broadcasted_iota(jnp.int32, squares.shape, 0)
        both = jnp.where(line == 0, high.astype(F32), jnp.where(line == 1, low.astype(F32), 0.0))
        depth = 2 * half * rows + e * 8
        for z in range(z_count):
            parcel[z, depth : depth + 8, :] = both.astype(BF16)
    store(2 * half * rows, half * 8)
    for e in range(half):
        for m in range(2):
            for part in range(2):
                loads[e, m, part].wait()
            sums = dot32(scaled[e, 0], weights[e, m, 0]) + dot32(scaled[e, 1], weights[e, m, 1])
            sums = sums.astype(BF16)
            depth = (half * m + e) * rows
            for z in range(z_count):
                parcel[z, depth : depth + rows, :] = sums[:, z * lanes : (z + 1) * lanes]
            store(depth, rows)
    for copy in stores:
        copy.wait()


def gate_up(at, incoming, gain, gate, gate_par, up, up_par):
    seq_devs, _, pair_slots, width = incoming.shape
    half, _, units = gate_par.shape
    z_count = lax.axis_size("z")
    pair_rows = seq_devs * pair_slots
    parcel = (z_count, 2 * pair_rows + half * 8, units // z_count)
    smem, vmem = pl.BlockSpec(memory_space=pltpu.SMEM), pl.BlockSpec(memory_space=pltpu.VMEM)
    far, any_place = pl.BlockSpec(memory_space=pltpu.HBM), pl.BlockSpec(memory_space=pl.ANY)
    return pl.pallas_call(
        gate_up_kernel,
        in_specs=[smem, any_place, vmem, far, any_place, far, any_place],
        out_specs=far,
        out_shape=pltpu.HBM(parcel, BF16),
        scratch_shapes=[
            pltpu.VMEM(incoming.shape, BF16),
            pltpu.VMEM((half, 2, 2, width, units), BF16),
            pltpu.VMEM(parcel, BF16),
            pltpu.SemaphoreType.DMA((1 + 4 * half,)),
            pltpu.SemaphoreType.DMA((1 + 2 * half,)),
        ],
        compiler_params=pltpu.CompilerParams(vmem_limit_bytes=62 * 2**20),
        cost_estimate=cost(8 * pair_rows * width * units, 8 * half * width * units),
        name="gate_up",
    )(at, incoming, gain, gate, gate_par, up, up_par)


def dispatch_kernel(spread, own_in, par_in, outgoing, own, par, arrivals):
    copies = [
        pltpu.make_async_copy(source, target, arrivals.at[i])
        for i, (source, target) in enumerate(((own_in, own), (par_in, par)))
    ]
    for copy in copies:
        copy.start()
    for copy in copies:
        copy.wait()
    shape = outgoing.shape[:1] + outgoing.shape[2:]
    for part, rows in enumerate((own, par)):
        outgoing[:, part] = dot32(spread[...], rows[...]).astype(BF16).reshape(shape)


def dispatch(spread, own, par, ep_count):
    slots, (_, width) = spread.shape[0], own.shape
    vmem = pl.BlockSpec(memory_space=pltpu.VMEM)
    return pl.pallas_call(
        dispatch_kernel,
        out_shape=jax.ShapeDtypeStruct((ep_count, 2, slots // ep_count, width), BF16),
        in_specs=[vmem, pl.BlockSpec(memory_space=pl.ANY), pl.BlockSpec(memory_space=pl.ANY)],
        out_specs=vmem,
        scratch_shapes=[
            pltpu.VMEM(own.shape, BF16),
            pltpu.VMEM(own.shape, BF16),
            pltpu.SemaphoreType.DMA((2,)),
        ],
        compiler_params=ROOM,
        cost_estimate=cost(4 * spread.size * width, 4 * slots * width),
        name="dispatch",
    )(spread, own, par)


def combine_kernel(weights, arrived, own, given, returned, arrival):
    fetch(arrived, returned, arrival)
    high, low = two_parts(weights[...])
    rows, width = weights.shape[1], returned.shape[3]
    for part, out in enumerate((own, given)):
        values = returned[:, part].reshape(rows, width)
        out[...] = (dot32(high, values) + dot32(low, values)).astype(out.dtype)


def combined(weights, returned):
    shape = (weights.shape[0], returned.shape[3])
    vmem = pl.BlockSpec(memory_space=pltpu.VMEM)
    return pl.pallas_call(
        combine_kernel,
        out_shape=(jax.ShapeDtypeStruct(shape, F32), jax.ShapeDtypeStruct(shape, BF16)),
        in_specs=[vmem, pl.BlockSpec(memory_space=pl.ANY)],
        out_specs=(vmem, vmem),
        scratch_shapes=[pltpu.VMEM(returned.shape, BF16), pltpu.SemaphoreType.DMA],
        compiler_params=ROOM,
        cost_estimate=cost(8 * weights.size * shape[1], 2 * returned.size),
        name="combine",
    )(weights, returned)


def shared_kernel(at, pieces, gain, gate_t, up_t, down_t, kept, given):
    c, z = at[0], at[1] // 2
    seqs, width = kept.shape[1:]
    squares = jnp.zeros((seqs, 1), F32)
    gate = jnp.zeros((seqs, gate_t.shape[0]), F32)
    up = gate
    chips = grown_order(kept.shape[0])
    for part, place in ((0, c), (1, 1 - c)):
        rows = [piece[part][i] for piece in pieces for i in range(piece[part].shape[0])]
        for chip, values in zip(chips, rows, strict=True):
            values = values.astype(F32)
            squares = squares + jnp.sum(values * values, axis=-1, keepdims=True)
            first = (2 * jnp.bitwise_xor(z, chip) + place) * width
            features = pl.ds(pl.multiple_of(first, width), width)
            scaled = (values * gain[:, features]).astype(BF16)
            gate = gate + dot_nt(scaled, gate_t[:, features])
            up = up + dot_nt(scaled, up_t[:, features])
    factor = lax.rsqrt(squares / (2 * len(chips) * width) + EPS)
    gate, up = gate * factor, up * factor
    inner = (gate / (1.0 + jnp.exp(-gate)) * up).astype(BF16)
    for chip in range(len(chips)):
        for out, place in ((kept, c), (given, 1 - c)):
            first = (2 * jnp.bitwise_xor(z, chip) + place) * width
            features = pl.ds(pl.multiple_of(first, width), width)
            out[chip] = dot32(inner, down_t[:, features]).astype(out.dtype)


def growing(chips):
    far = chips // 2
    return [far] + [1 << i for i in range(far.bit_length() - 1)]


def grown_order(chips):
    order = [0]
    for bit in growing(chips):
        order = order + [owner ^ bit for owner in order]
    return order


def shared_parts(at, pieces, gain, gate_t, up_t, w_down, after):
    smem, vmem = pl.BlockSpec(memory_space=pltpu.SMEM), pl.BlockSpec(memory_space=pltpu.VMEM)
    flat = [rows for piece in pieces for rows in piece]
    (seqs, width), z_count = flat[0].shape[1:], sum(rows.shape[0] for rows in flat) // 2

    def kernel(at, *refs):
        rows, rest = refs[: len(flat)], refs[len(flat) :]
        paired = [(rows[i], rows[i + 1]) for i in range(0, len(flat), 2)]
        shared_kernel(at, paired, *rest[:4], *rest[5:])

    return pl.pallas_call(
        kernel,
        out_shape=(
            jax.ShapeDtypeStruct((z_count, seqs, width), F32),
            jax.ShapeDtypeStruct((z_count, seqs, width), BF16),
        ),
        in_specs=[smem] + [vmem] * (len(flat) + 4) + [pl.BlockSpec(memory_space=pl.ANY)],
        out_specs=(vmem, vmem),
        compiler_params=ROOM,
        cost_estimate=cost(seqs * 6 * w_down.size, 6 * w_down.size),
        name="shared",
    )(at, *flat, gain, gate_t, up_t, w_down, after)


def inner_kernel(model_width, half, arrived, inner, parcels, arrival):
    fetch(arrived, parcels, arrival)
    totals = parcels[0].astype(F32)
    z_count = parcels.shape[0]
    for z in range(1, z_count):
        totals = totals + parcels[z].astype(F32)
    lanes = totals.shape[1]
    pair_rows = inner.shape[1]
    rows = pair_rows // half
    for e in range(half):
        line = 2 * pair_rows + 8 * e
        squares = totals[line : line + 1] + totals[line + 1 : line + 2]
        factor = lax.rsqrt(squares / model_width + EPS)
        factor = jnp.broadcast_to(factor, (lanes, rows)).T
        gate = totals[e * rows : (e + 1) * rows] * factor
        up = totals[pair_rows + e * rows : pair_rows + (e + 1) * rows] * factor
        done = (gate / (1.0 + jnp.exp(-gate)) * up).astype(BF16)
        for z in range(z_count):
            inner[z, e * rows : (e + 1) * rows, :] = done


def inner_copies(parcels, model_width, half):
    z_count, depth, lanes = parcels.shape
    pair_rows = (depth - half * 8) // 2
    return pl.pallas_call(
        functools.partial(inner_kernel, model_width, half),
        out_shape=jax.ShapeDtypeStruct((z_count, pair_rows, lanes), BF16),
        in_specs=[pl.BlockSpec(memory_space=pl.ANY)],
        out_specs=pl.BlockSpec(memory_space=pltpu.VMEM),
        scratch_shapes=[pltpu.VMEM(parcels.shape, BF16), pltpu.SemaphoreType.DMA],
        compiler_params=ROOM,
        cost_estimate=cost(parcels.size * 4, parcels.size * 4),
        name="inner",
    )(parcels)


def down_kernel(at, arrived, own, par, sent, inner, weights, results, ins, outs):
    half = weights.shape[0]
    first = pltpu.make_async_copy(arrived, inner, ins.at[0])
    first.start()
    loads = []
    for e in range(half):
        for part, source in enumerate((own.at[half * at[0] + e], par.at[e])):
            arrival = ins.at[1 + 2 * e + part]
            copy = pltpu.make_async_copy(source, weights.at[e, part], arrival)
            copy.start()
            loads.append(copy)
    first.wait()
    rows = inner.shape[1] // half
    seq_devs, _, pair_slots, width = results.shape
    capacity = pair_slots // half
    stores = []
    for e in range(half):
        row = [inner[z, e * rows : (e + 1) * rows, :] for z in range(inner.shape[0])]
        row = jnp.concatenate(row, axis=1)
        place = slice(e * capacity, (e + 1) * capacity)
        for part in range(2):
            loads[2 * e + part].wait()
            out = dot32(row, weights[e, part]).astype(BF16)
            results[:, part, place, :] = out.reshape(seq_devs, capacity, width)
        place = pl.ds(e * capacity, capacity)
        copy = pltpu.make_async_copy(
            results.at[:, :, place, :], sent.at[:, :, place, :], outs.at[e]
        )
        copy.start()
        stores.append(copy)
    for copy in stores:
        copy.wait()


def down(at, inner, w_down, w_par, seq_devs, capacity):
    half, units, width = w_par.shape
    results = (seq_devs, 2, half * capacity, width)
    smem, any_place = pl.BlockSpec(memory_space=pltpu.SMEM), pl.BlockSpec(memory_space=pl.ANY)
    return pl.pallas_call(
        down_kernel,
        in_specs=[smem, any_place, any_place, any_place],
        out_specs=pl.BlockSpec(memory_space=pltpu.HBM),
        out_shape=pltpu.HBM(results, BF16),
        scratch_shapes=[
            pltpu.VMEM(inner.shape, BF16),
            pltpu.VMEM((half, 2, units, width), BF16),
            pltpu.VMEM(results, BF16),
            pltpu.SemaphoreType.DMA((1 + 2 * half,)),
            pltpu.SemaphoreType.DMA((half,)),
        ],
        compiler_params=ROOM,
        cost_estimate=cost(4 * inner.shape[1] * units * width, 4 * half * units * width),
        name="down",
    )(at, inner, w_down, w_par)


def local(
    tokens,
    norm_gain,
    ffn_gain,
    w_in,
    decay_rate,
    frequency,
    log_step,
    input_real,
    input_imag,
    readout_real,
    readout_imag,
    skip_gain,
    state_real,
    state_imag,
    w_out,
    shared_gate,
    shared_up,
    shared_down,
    expert_gate,
    expert_up,
    expert_down,
    routing,
    route_weight,
):
    seq_count, model_width = tokens.shape
    ep_count, z_count = lax.axis_size("ep"), lax.axis_size("z")
    z, c = lax.axis_index("z"), lax.axis_index("c")
    core = c.reshape(1)
    slice_width = model_width // (2 * z_count)
    offset = (2 * z + c) * slice_width

    partner = []
    for w in (expert_gate, expert_up, expert_down):
        cut = of_pair(w, 1 - c, 0)
        partner.append(swapped(cut))
    gate_par, up_par, down_par = partner

    new_real, new_imag, kept, given = front(
        core,
        log_step,
        tokens,
        norm_gain.reshape(1, -1),
        w_in,
        decay_rate.reshape(1, -1),
        frequency.reshape(1, -1),
        input_real,
        input_imag,
        readout_real,
        readout_imag,
        skip_gain.reshape(1, -1),
        state_real,
        state_imag,
        w_out,
    )
    both = (kept + swapped(given).astype(F32)).astype(BF16)
    mixer_own = lax.all_to_all(both, "z", split_axis=0, concat_axis=0, tiled=True)
    mixer_own = mixer_own.astype(F32).sum(axis=0)
    own_tokens = lax.dynamic_slice_in_dim(tokens, offset, slice_width, 1)
    resid_own = (own_tokens.astype(F32) + mixer_own).astype(BF16)
    resid_par = swapped(resid_own)

    expert_dev = expert_gate.shape[0]
    half = expert_dev // 2
    top_count = routing.shape[1]
    capacity = 2 * seq_count * top_count // (expert_dev * ep_count)
    slot_count = half * ep_count * capacity
    flat_ids = routing.reshape(-1)
    one_hot = (
        flat_ids[:, None] == jnp.arange(expert_dev * ep_count, dtype=jnp.int32)[None, :]
    ).astype(jnp.int32)
    earlier = jnp.cumsum(one_hot, axis=0) - one_hot
    slot_rank = jnp.sum(earlier * one_hot, axis=1)
    home, within = flat_ids // expert_dev, flat_ids % expert_dev
    target = (home * half + within % half) * capacity + slot_rank
    target = jnp.where(within // half == c, target, -1)
    slot_ids = jnp.arange(slot_count, dtype=jnp.int32)
    placed = (target[None, :] == slot_ids[:, None]).reshape(slot_count, seq_count, top_count)
    spread = jnp.sum(placed.astype(F32), axis=2).astype(BF16)
    outgoing = dispatch(spread, resid_own, resid_par, ep_count)
    incoming = lax.all_to_all(outgoing, "ep", split_axis=0, concat_axis=0, tiled=True)

    at = jnp.array([1, 1, -1], jnp.int32) * c + jnp.array([0, 2, 2], jnp.int32) * z
    at = at + jnp.array([0, 0, 1], jnp.int32)
    gain = ffn_gain.reshape(1, -1)
    parcel = gate_up(at, incoming, gain, expert_gate, gate_par, expert_up, up_par)
    parcels = lax.all_to_all(parcel, "z", split_axis=0, concat_axis=0, tiled=True)
    copies = inner_copies(parcels, model_width, half)
    inner_all = lax.all_to_all(copies, "z", split_axis=0, concat_axis=0, tiled=True)
    results = down(at, inner_all, expert_down, down_par, ep_count, capacity)
    returned = lax.all_to_all(results, "ep", split_axis=0, concat_axis=0, tiled=True)

    pieces = [(resid_own[None], resid_par[None])]
    for bit in growing(z_count):
        held = jnp.concatenate([piece[0] for piece in pieces])
        theirs = exchanged(held, "z", bit)
        pieces.append((theirs, swapped(theirs)))
    kept, given = shared_parts(
        at, pieces, gain, shared_gate.T, shared_up.T, shared_down, copies
    )
    got = swapped(given)
    shared_own = kept + got.astype(F32)
    count = z_count // 2
    while count > 0:
        theirs = exchanged(shared_own[count:].astype(BF16), "z", count)
        shared_own = shared_own[:count] + theirs.astype(F32)
        count //= 2
    shared_own = shared_own[0]

    weights = route_weight / jnp.sum(route_weight, axis=1, keepdims=True) * ROUTED_SCALE
    chosen = target.reshape(seq_count, top_count)[:, :, None] == slot_ids[None, None, :]
    combine = jnp.sum(jnp.where(chosen, weights[:, :, None], 0.0), axis=1)
    routed, routed_par = combined(combine, returned)
    routed = routed + swapped(routed_par).astype(F32)
    mixed = (resid_own.astype(F32) + shared_own + routed).astype(BF16)
    return (mixed, new_real, new_imag)


def solution(mesh):
    ep_count, tp_count = mesh.devices.shape
    cores = Mesh(mesh.devices.reshape(ep_count, tp_count // 2, 2), ("ep", "z", "c"))
    placed = (
        P("ep", None),
        P(),
        P(),
        P(None, TP),
        P(TP),
        P(TP),
        P(TP),
        P(None, TP),
        P(None, TP),
        P(None, TP),
        P(None, TP),
        P(TP),
        P("ep", TP),
        P("ep", TP),
        P(TP, None),
        P(None, TP),
        P(None, TP),
        P(TP, None),
        P("ep", TP, None),
        P("ep", TP, None),
        P("ep", None, TP),
        P("ep", None),
        P("ep", None),
    )

    def step(*arrays):
        return local(*arrays)

    step = jax.shard_map(
        step,
        mesh=cores,
        in_specs=placed,
        out_specs=(P("ep", TP), P("ep", TP), P("ep", TP)),
        check_vma=False,
    )
    return step
```

```python
import functools

import jax
import jax.numpy as jnp
from jax import lax
from jax.experimental import pallas as pl
from jax.experimental.pallas import tpu as pltpu
from jax.sharding import Mesh
from jax.sharding import PartitionSpec as P


EPS = 1e-06
ROUTED_SCALE = 2.5
TP = ("z", "c")
F32, BF16 = jnp.float32, jnp.bfloat16
ROOM = pltpu.CompilerParams(vmem_limit_bytes=20 * 2**20)


def swapped(x):
    return lax.ppermute(x, "c", [(0, 1), (1, 0)])


def moved(x, axis, steps):
    count = lax.axis_size(axis)
    return lax.ppermute(x, axis, [(i, (i + steps) % count) for i in range(count)])


def exchanged(x, axis, bit):
    return lax.ppermute(x, axis, [(i, i ^ bit) for i in range(lax.axis_size(axis))])


def of_pair(x, which, dim):
    width = x.shape[dim] // 2
    return lax.dynamic_slice_in_dim(x, which * width, width, dim)


def rms_scale(values_in, gains):
    values = values_in.astype(F32)
    factor = lax.rsqrt(jnp.mean(values * values, axis=-1, keepdims=True) + EPS)
    return (values * factor * gains).astype(BF16)


def dot32(a, b):
    return jnp.dot(a, b, preferred_element_type=F32)


def dot_nt(a, b):
    return lax.dot_general(a, b, (((1,), (1,)), ((), ())), preferred_element_type=F32)


def two_parts(x):
    high = x.astype(BF16)
    return high, (x - high.astype(F32)).astype(BF16)


def cost(flops, moved):
    return pl.CostEstimate(flops=flops, bytes_accessed=moved, transcendentals=0)


def fetch(source, target, arrival):
    copy = pltpu.make_async_copy(source, target, arrival)
    copy.start()
    copy.wait()


def front_kernel(
    core,
    log_step,
    tokens,
    norm_gain,
    w_in,
    decay_rate,
    frequency,
    input_real,
    input_imag,
    readout_real,
    readout_imag,
    skip_gain,
    state_real,
    state_imag,
    w_out,
    new_real,
    new_imag,
    kept,
    given,
):
    groups = log_step.shape[0]
    chan_count, entries = input_real.shape
    channels = skip_gain.shape[1]
    width = entries // groups
    normed = rms_scale(tokens[...], norm_gain[...])
    drive = dot32(normed, w_in[...]).astype(BF16)
    group_of = lax.broadcasted_iota(jnp.int32, (1, entries), 1) // width
    step_size = jnp.zeros((1, entries), F32)
    for g in range(groups):
        step_size = jnp.where(group_of == g, log_step[g], step_size)
    step_size = jnp.exp(step_size)
    decays, omegas = decay_rate[...], frequency[...]
    pole_mag = jnp.exp(-decays * step_size)
    pole_angle = omegas * step_size
    pole_re = pole_mag * jnp.cos(pole_angle)
    pole_im = pole_mag * jnp.sin(pole_angle)
    pole_norm = decays * decays + omegas * omegas
    diff_re = pole_re - 1.0
    lift_re = (-decays * diff_re + omegas * pole_im) / pole_norm
    lift_im = (-decays * pole_im - omegas * diff_re) / pole_norm
    row_group = lax.broadcasted_iota(jnp.int32, (channels, entries), 0) // chan_count
    col_group = lax.broadcasted_iota(jnp.int32, (channels, entries), 1) // width
    same = row_group == col_group

    def spread(block):
        return two_parts(jnp.where(same, jnp.concatenate([block[...]] * groups, axis=0), 0.0))

    def push_of(block):
        high, low = spread(block)
        return dot32(drive, high) + dot32(drive, low)

    push_re, push_im = push_of(input_real), push_of(input_imag)
    old_re, old_im = state_real[...], state_imag[...]
    new_re = pole_re * old_re - pole_im * old_im + lift_re * push_re - lift_im * push_im
    new_im = pole_re * old_im + pole_im * old_re + lift_re * push_im + lift_im * push_re
    new_real[...] = new_re
    new_imag[...] = new_im

    def read_of(state, block):
        (high, low), (block_high, block_low) = two_parts(state), spread(block)
        return dot_nt(high, block_high) + dot_nt(high, block_low) + dot_nt(low, block_high)

    read = read_of(new_re, readout_real) - read_of(new_im, readout_imag)
    read = read + skip_gain[...] * drive.astype(F32)
    bent = jnp.tanh(0.7978845608028654 * (read + 0.044715 * (read * read * read)))
    activated = (0.5 * read * (1.0 + bent)).astype(BF16)
    wide = kept.shape[2]
    for z in range(kept.shape[0]):
        for out, c in ((kept, core[0]), (given, 1 - core[0])):
            at = pl.multiple_of((2 * z + c) * wide, wide)
            out[z] = dot32(activated, w_out[:, pl.ds(at, wide)]).astype(out.dtype)


def front(core, log_step, *arrays):
    tokens, w_out, state = arrays[0], arrays[-1], arrays[-2]
    seqs, model_width = tokens.shape
    z_count = lax.axis_size("z")
    part = (z_count, seqs, model_width // (2 * z_count))
    smem, vmem = pl.BlockSpec(memory_space=pltpu.SMEM), pl.BlockSpec(memory_space=pltpu.VMEM)
    return pl.pallas_call(
        front_kernel,
        out_shape=(
            jax.ShapeDtypeStruct(state.shape, F32),
            jax.ShapeDtypeStruct(state.shape, F32),
            jax.ShapeDtypeStruct(part, F32),
            jax.ShapeDtypeStruct(part, BF16),
        ),
        in_specs=[smem, smem] + [vmem] * len(arrays),
        out_specs=(vmem,) * 4,
        cost_estimate=cost(4 * seqs * model_width * w_out.shape[0], 2 * w_out.size * 2),
        name="front",
    )(core, log_step, *arrays)


def gate_up_kernel(
    at, arrived, gain, gate, gate_par, up, up_par, *refs
):
    *sent, near, far, incoming, weights, parcel, ins, outs = refs
    half, _, _, width, _ = weights.shape
    seq_devs, _, pair_slots, _ = incoming.shape
    z_count, _, lanes = parcel.shape
    capacity = pair_slots // half
    rows = seq_devs * capacity
    first = pltpu.make_async_copy(arrived, incoming, ins.at[0])
    first.start()
    loads = {}
    for e in range(half):
        for m, (own, par) in enumerate(((gate, gate_par), (up, up_par))):
            for part, source in enumerate((own.at[half * at[0] + e], par.at[e])):
                arrival = ins.at[1 + 4 * e + 2 * m + part]
                copy = pltpu.make_async_copy(source, weights.at[e, m, part], arrival)
                copy.start()
                loads[e, m, part] = copy
    ones = jnp.ones((8, width), BF16)
    features = [pl.ds(pl.multiple_of(at[1 + part] * width, width), width) for part in range(2)]
    first.wait()
    stores = []

    def store(source, target):
        copy = pltpu.make_async_copy(source, target, outs.at[len(stores)])
        copy.start()
        stores.append(copy)

    def put(depth, size, block_of):
        for chip in range(z_count):
            steps = lax.rem(chip - at[3] + z_count, z_count)
            parcel[steps, depth : depth + size, :] = block_of(chip)

    scaled = {}
    for e in range(half):
        squares = jnp.zeros((8, rows), F32)
        for part in range(2):
            values = incoming[:, part, e * capacity : (e + 1) * capacity, :]
            values = values.reshape(rows, width).astype(F32)
            scaled[e, part] = (values * gain[:, features[part]]).astype(BF16)
            high, low = two_parts(values * values)
            squares = squares + dot_nt(ones, high) + dot_nt(ones, low)
        high, low = two_parts(squares)
        line = lax.broadcasted_iota(jnp.int32, squares.shape, 0)
        both = jnp.where(line == 0, high.astype(F32), jnp.where(line == 1, low.astype(F32), 0.0))
        depth = 2 * half * rows + e * 8
        put(depth, 8, lambda chip, both=both: both.astype(BF16))
    for e in range(half):
        for m in range(2):
            for part in range(2):
                loads[e, m, part].wait()
            sums = dot32(scaled[e, 0], weights[e, m, 0]) + dot32(scaled[e, 1], weights[e, m, 1])
            sums = sums.astype(BF16)
            depth = (half * m + e) * rows
            put(depth, rows, lambda chip, sums=sums: sums[:, chip * lanes : (chip + 1) * lanes])
    middle, split = z_count // 2, near.shape[0]
    store(parcel.at[middle, pl.ds(0, split), :], near)
    store(parcel.at[middle, pl.ds(split, far.shape[0]), :], far)
    for steps in range(middle):
        store(parcel.at[steps], sent[steps])
    for steps in range(middle + 1, z_count):
        store(parcel.at[steps], sent[steps - 1])
    for copy in stores:
        copy.wait()


def gate_up(at, incoming, gain, gate, gate_par, up, up_par):
    seq_devs, _, pair_slots, width = incoming.shape
    half, _, units = gate_par.shape
    z_count = lax.axis_size("z")
    pair_rows = seq_devs * pair_slots
    parcel = (z_count, 2 * pair_rows + half * 8, units // z_count)
    smem, vmem = pl.BlockSpec(memory_space=pltpu.SMEM), pl.BlockSpec(memory_space=pltpu.VMEM)
    far, any_place = pl.BlockSpec(memory_space=pltpu.HBM), pl.BlockSpec(memory_space=pl.ANY)
    return pl.pallas_call(
        gate_up_kernel,
        in_specs=[smem, any_place, vmem, far, any_place, far, any_place],
        out_specs=(far,) * (z_count + 1),
        out_shape=(pltpu.HBM(parcel[1:], BF16),) * (z_count - 1)
        + (pltpu.HBM((parcel[1] // 2, parcel[2]), BF16),) * 2,
        scratch_shapes=[
            pltpu.VMEM(incoming.shape, BF16),
            pltpu.VMEM((half, 2, 2, width, units), BF16),
            pltpu.VMEM(parcel, BF16),
            pltpu.SemaphoreType.DMA((1 + 4 * half,)),
            pltpu.SemaphoreType.DMA((z_count + 1,)),
        ],
        compiler_params=pltpu.CompilerParams(vmem_limit_bytes=62 * 2**20),
        cost_estimate=cost(8 * pair_rows * width * units, 8 * half * width * units),
        name="gate_up",
    )(at, incoming, gain, gate, gate_par, up, up_par)


def dispatch_kernel(spread, own_in, par_in, outgoing, own, par, arrivals):
    copies = [
        pltpu.make_async_copy(source, target, arrivals.at[i])
        for i, (source, target) in enumerate(((own_in, own), (par_in, par)))
    ]
    for copy in copies:
        copy.start()
    for copy in copies:
        copy.wait()
    shape = outgoing.shape[:1] + outgoing.shape[2:]
    for part, rows in enumerate((own, par)):
        outgoing[:, part] = dot32(spread[...], rows[...]).astype(BF16).reshape(shape)


def dispatch(spread, own, par, ep_count):
    slots, (_, width) = spread.shape[0], own.shape
    vmem = pl.BlockSpec(memory_space=pltpu.VMEM)
    return pl.pallas_call(
        dispatch_kernel,
        out_shape=jax.ShapeDtypeStruct((ep_count, 2, slots // ep_count, width), BF16),
        in_specs=[vmem, pl.BlockSpec(memory_space=pl.ANY), pl.BlockSpec(memory_space=pl.ANY)],
        out_specs=vmem,
        scratch_shapes=[
            pltpu.VMEM(own.shape, BF16),
            pltpu.VMEM(own.shape, BF16),
            pltpu.SemaphoreType.DMA((2,)),
        ],
        compiler_params=ROOM,
        cost_estimate=cost(4 * spread.size * width, 4 * slots * width),
        name="dispatch",
    )(spread, own, par)


def combine_kernel(weights, arrived, own, given, returned, arrival):
    fetch(arrived, returned, arrival)
    high, low = two_parts(weights[...])
    rows, width = weights.shape[1], returned.shape[3]
    for part, out in enumerate((own, given)):
        values = returned[:, part].reshape(rows, width)
        out[...] = (dot32(high, values) + dot32(low, values)).astype(out.dtype)


def combined(weights, returned):
    shape = (weights.shape[0], returned.shape[3])
    vmem = pl.BlockSpec(memory_space=pltpu.VMEM)
    return pl.pallas_call(
        combine_kernel,
        out_shape=(jax.ShapeDtypeStruct(shape, F32), jax.ShapeDtypeStruct(shape, BF16)),
        in_specs=[vmem, pl.BlockSpec(memory_space=pl.ANY)],
        out_specs=(vmem, vmem),
        scratch_shapes=[pltpu.VMEM(returned.shape, BF16), pltpu.SemaphoreType.DMA],
        compiler_params=ROOM,
        cost_estimate=cost(8 * weights.size * shape[1], 2 * returned.size),
        name="combine",
    )(weights, returned)


def shared_kernel(at, pieces, gain, gate_t, up_t, down_t, kept, given):
    c, z = at[0], at[3]
    seqs, width = kept.shape[1:]
    squares = jnp.zeros((seqs, 1), F32)
    gate = jnp.zeros((seqs, gate_t.shape[0]), F32)
    up = gate
    chips = grown_order(kept.shape[0])
    for part, place in ((0, c), (1, 1 - c)):
        rows = [piece[part][i] for piece in pieces for i in range(piece[part].shape[0])]
        for chip, values in zip(chips, rows, strict=True):
            values = values.astype(F32)
            squares = squares + jnp.sum(values * values, axis=-1, keepdims=True)
            first = (2 * jnp.bitwise_xor(z, chip) + place) * width
            features = pl.ds(pl.multiple_of(first, width), width)
            scaled = (values * gain[:, features]).astype(BF16)
            gate = gate + dot_nt(scaled, gate_t[:, features])
            up = up + dot_nt(scaled, up_t[:, features])
    factor = lax.rsqrt(squares / (2 * len(chips) * width) + EPS)
    gate, up = gate * factor, up * factor
    inner = (gate / (1.0 + jnp.exp(-gate)) * up).astype(BF16)
    for chip in range(len(chips)):
        for out, place in ((kept, c), (given, 1 - c)):
            first = (2 * jnp.bitwise_xor(z, chip) + place) * width
            features = pl.ds(pl.multiple_of(first, width), width)
            out[chip] = dot32(inner, down_t[:, features]).astype(out.dtype)


def growing(chips):
    far = chips // 2
    return [far] + [1 << i for i in range(far.bit_length() - 1)]


def grown_order(chips):
    order = [0]
    for bit in growing(chips):
        order = order + [owner ^ bit for owner in order]
    return order


def shared_parts(at, pieces, gain, gate_t, up_t, w_down, after):
    smem, vmem = pl.BlockSpec(memory_space=pltpu.SMEM), pl.BlockSpec(memory_space=pltpu.VMEM)
    flat = [rows for piece in pieces for rows in piece]
    (seqs, width), z_count = flat[0].shape[1:], sum(rows.shape[0] for rows in flat) // 2

    def kernel(at, *refs):
        rows, rest = refs[: len(flat)], refs[len(flat) :]
        paired = [(rows[i], rows[i + 1]) for i in range(0, len(flat), 2)]
        shared_kernel(at, paired, *rest[:4], *rest[5:])

    return pl.pallas_call(
        kernel,
        out_shape=(
            jax.ShapeDtypeStruct((z_count, seqs, width), F32),
            jax.ShapeDtypeStruct((z_count, seqs, width), BF16),
        ),
        in_specs=[smem] + [vmem] * (len(flat) + 4) + [pl.BlockSpec(memory_space=pl.ANY)],
        out_specs=(vmem, vmem),
        compiler_params=ROOM,
        cost_estimate=cost(seqs * 6 * w_down.size, 6 * w_down.size),
        name="shared",
    )(at, *flat, gain, gate_t, up_t, w_down, after)


def inner_kernel(model_width, half, *refs):
    *arrived, inner, parcels, arrivals = refs
    copies = [
        pltpu.make_async_copy(source, parcels.at[i], arrivals.at[i])
        for i, source in enumerate(arrived)
    ]
    for copy in copies:
        copy.start()
    for i, copy in enumerate(copies):
        copy.wait()
        totals = totals + parcels[i].astype(F32) if i > 0 else parcels[i].astype(F32)
    lanes = totals.shape[1]
    z_count, pair_rows, _ = inner.shape
    rows = pair_rows // half
    for e in range(half):
        line = 2 * pair_rows + 8 * e
        squares = totals[line : line + 1] + totals[line + 1 : line + 2]
        factor = lax.rsqrt(squares / model_width + EPS)
        factor = jnp.broadcast_to(factor, (lanes, rows)).T
        gate = totals[e * rows : (e + 1) * rows] * factor
        up = totals[pair_rows + e * rows : pair_rows + (e + 1) * rows] * factor
        done = (gate / (1.0 + jnp.exp(-gate)) * up).astype(BF16)
        for z in range(z_count):
            inner[z, e * rows : (e + 1) * rows, :] = done


def inner_copies(parcels, z_count, model_width, half):
    depth, lanes = parcels[0].shape
    pair_rows = (depth - half * 8) // 2
    count = len(parcels)
    return pl.pallas_call(
        functools.partial(inner_kernel, model_width, half),
        out_shape=jax.ShapeDtypeStruct((z_count, pair_rows, lanes), BF16),
        in_specs=[pl.BlockSpec(memory_space=pl.ANY)] * count,
        out_specs=pl.BlockSpec(memory_space=pltpu.VMEM),
        scratch_shapes=[
            pltpu.VMEM((count, depth, lanes), BF16),
            pltpu.SemaphoreType.DMA((count,)),
        ],
        compiler_params=ROOM,
        cost_estimate=cost(depth * lanes * 32, depth * lanes * 32),
        name="inner",
    )(*parcels)


def down_kernel(at, arrived, own, par, sent, inner, weights, results, ins, outs):
    half = weights.shape[0]
    first = pltpu.make_async_copy(arrived, inner, ins.at[0])
    first.start()
    loads = []
    for e in range(half):
        for part, source in enumerate((own.at[half * at[0] + e], par.at[e])):
            arrival = ins.at[1 + 2 * e + part]
            copy = pltpu.make_async_copy(source, weights.at[e, part], arrival)
            copy.start()
            loads.append(copy)
    first.wait()
    rows = inner.shape[1] // half
    seq_devs, _, pair_slots, width = results.shape
    capacity = pair_slots // half
    stores = []
    for e in range(half):
        row = [inner[z, e * rows : (e + 1) * rows, :] for z in range(inner.shape[0])]
        row = jnp.concatenate(row, axis=1)
        place = slice(e * capacity, (e + 1) * capacity)
        for part in range(2):
            loads[2 * e + part].wait()
            out = dot32(row, weights[e, part]).astype(BF16)
            results[:, part, place, :] = out.reshape(seq_devs, capacity, width)
        place = pl.ds(e * capacity, capacity)
        copy = pltpu.make_async_copy(
            results.at[:, :, place, :], sent.at[:, :, place, :], outs.at[e]
        )
        copy.start()
        stores.append(copy)
    for copy in stores:
        copy.wait()


def down(at, inner, w_down, w_par, seq_devs, capacity):
    half, units, width = w_par.shape
    results = (seq_devs, 2, half * capacity, width)
    smem, any_place = pl.BlockSpec(memory_space=pltpu.SMEM), pl.BlockSpec(memory_space=pl.ANY)
    return pl.pallas_call(
        down_kernel,
        in_specs=[smem, any_place, any_place, any_place],
        out_specs=pl.BlockSpec(memory_space=pltpu.HBM),
        out_shape=pltpu.HBM(results, BF16),
        scratch_shapes=[
            pltpu.VMEM(inner.shape, BF16),
            pltpu.VMEM((half, 2, units, width), BF16),
            pltpu.VMEM(results, BF16),
            pltpu.SemaphoreType.DMA((1 + 2 * half,)),
            pltpu.SemaphoreType.DMA((half,)),
        ],
        compiler_params=ROOM,
        cost_estimate=cost(4 * inner.shape[1] * units * width, 4 * half * units * width),
        name="down",
    )(at, inner, w_down, w_par)


def local(
    tokens,
    norm_gain,
    ffn_gain,
    w_in,
    decay_rate,
    frequency,
    log_step,
    input_real,
    input_imag,
    readout_real,
    readout_imag,
    skip_gain,
    state_real,
    state_imag,
    w_out,
    shared_gate,
    shared_up,
    shared_down,
    expert_gate,
    expert_up,
    expert_down,
    routing,
    route_weight,
):
    seq_count, model_width = tokens.shape
    ep_count, z_count = lax.axis_size("ep"), lax.axis_size("z")
    z, c = lax.axis_index("z"), lax.axis_index("c")
    core = c.reshape(1)
    slice_width = model_width // (2 * z_count)
    offset = (2 * z + c) * slice_width

    partner = []
    for w in (expert_gate, expert_up, expert_down):
        cut = of_pair(w, 1 - c, 0)
        partner.append(swapped(cut))
    gate_par, up_par, down_par = partner

    new_real, new_imag, kept, given = front(
        core,
        log_step,
        tokens,
        norm_gain.reshape(1, -1),
        w_in,
        decay_rate.reshape(1, -1),
        frequency.reshape(1, -1),
        input_real,
        input_imag,
        readout_real,
        readout_imag,
        skip_gain.reshape(1, -1),
        state_real,
        state_imag,
        w_out,
    )
    both = (kept + swapped(given).astype(F32)).astype(BF16)
    mixer_own = lax.all_to_all(both, "z", split_axis=0, concat_axis=0, tiled=True)
    mixer_own = mixer_own.astype(F32).sum(axis=0)
    own_tokens = lax.dynamic_slice_in_dim(tokens, offset, slice_width, 1)
    resid_own = (own_tokens.astype(F32) + mixer_own).astype(BF16)
    resid_par = swapped(resid_own)

    expert_dev = expert_gate.shape[0]
    half = expert_dev // 2
    top_count = routing.shape[1]
    capacity = 2 * seq_count * top_count // (expert_dev * ep_count)
    slot_count = half * ep_count * capacity
    flat_ids = routing.reshape(-1)
    one_hot = (
        flat_ids[:, None] == jnp.arange(expert_dev * ep_count, dtype=jnp.int32)[None, :]
    ).astype(jnp.int32)
    earlier = jnp.cumsum(one_hot, axis=0) - one_hot
    slot_rank = jnp.sum(earlier * one_hot, axis=1)
    home, within = flat_ids // expert_dev, flat_ids % expert_dev
    target = (home * half + within % half) * capacity + slot_rank
    target = jnp.where(within // half == c, target, -1)
    slot_ids = jnp.arange(slot_count, dtype=jnp.int32)
    placed = (target[None, :] == slot_ids[:, None]).reshape(slot_count, seq_count, top_count)
    spread = jnp.sum(placed.astype(F32), axis=2).astype(BF16)
    outgoing = dispatch(spread, resid_own, resid_par, ep_count)
    incoming = lax.all_to_all(outgoing, "ep", split_axis=0, concat_axis=0, tiled=True)

    at = jnp.array([1, 1, -1, 0], jnp.int32) * c + jnp.array([0, 2, 2, 1], jnp.int32) * z
    at = at + jnp.array([0, 0, 1, 0], jnp.int32)
    gain = ffn_gain.reshape(1, -1)
    *sent, near, far = gate_up(at, incoming, gain, expert_gate, gate_par, expert_up, up_par)
    middle = z_count // 2
    chunks = dict(zip([k for k in range(z_count) if k != middle], sent, strict=True))
    from_below = moved(near, "z", 1)
    from_above = moved(far, "z", -1)
    split = near.shape[0]
    chunk = chunks[middle - 1]
    chunk_low = (chunk[:split].astype(F32) + from_below.astype(F32)).astype(BF16)
    chunks[middle - 1] = jnp.concatenate([chunk_low, chunk[split:]])
    chunk = chunks[middle + 1]
    chunk_high = (chunk[split:].astype(F32) + from_above.astype(F32)).astype(BF16)
    chunks[middle + 1] = jnp.concatenate([chunk[:split], chunk_high])
    parcels = [chunks[0]]
    for steps in range(1, middle):
        parcels.append(moved(chunks[steps], "z", steps))
        parcels.append(moved(chunks[z_count - steps], "z", -steps))
    copies = inner_copies(parcels, z_count, model_width, half)
    inner_all = lax.all_to_all(copies, "z", split_axis=0, concat_axis=0, tiled=True)
    results = down(at, inner_all, expert_down, down_par, ep_count, capacity)
    returned = lax.all_to_all(results, "ep", split_axis=0, concat_axis=0, tiled=True)

    pieces = [(resid_own[None], resid_par[None])]
    for bit in growing(z_count):
        held = jnp.concatenate([piece[0] for piece in pieces])
        theirs = exchanged(held, "z", bit)
        pieces.append((theirs, swapped(theirs)))
    kept, given = shared_parts(
        at, pieces, gain, shared_gate.T, shared_up.T, shared_down, copies
    )
    got = swapped(given)
    shared_own = kept + got.astype(F32)
    count = z_count // 2
    while count > 0:
        theirs = exchanged(shared_own[count:].astype(BF16), "z", count)
        shared_own = shared_own[:count] + theirs.astype(F32)
        count //= 2
    shared_own = shared_own[0]

    weights = route_weight / jnp.sum(route_weight, axis=1, keepdims=True) * ROUTED_SCALE
    chosen = target.reshape(seq_count, top_count)[:, :, None] == slot_ids[None, None, :]
    combine = jnp.sum(jnp.where(chosen, weights[:, :, None], 0.0), axis=1)
    routed, routed_par = combined(combine, returned)
    routed = routed + swapped(routed_par).astype(F32)
    mixed = (resid_own.astype(F32) + shared_own + routed).astype(BF16)
    return (mixed, new_real, new_imag)


def solution(mesh):
    ep_count, tp_count = mesh.devices.shape
    cores = Mesh(mesh.devices.reshape(ep_count, tp_count // 2, 2), ("ep", "z", "c"))
    placed = (
        P("ep", None),
        P(),
        P(),
        P(None, TP),
        P(TP),
        P(TP),
        P(TP),
        P(None, TP),
        P(None, TP),
        P(None, TP),
        P(None, TP),
        P(TP),
        P("ep", TP),
        P("ep", TP),
        P(TP, None),
        P(None, TP),
        P(None, TP),
        P(TP, None),
        P("ep", TP, None),
        P("ep", TP, None),
        P("ep", None, TP),
        P("ep", None),
        P("ep", None),
    )

    def step(*arrays):
        return local(*arrays)

    step = jax.shard_map(
        step,
        mesh=cores,
        in_specs=placed,
        out_specs=(P("ep", TP), P("ep", TP), P("ep", TP)),
        check_vma=False,
    )
    return step
```

```python
import functools

import jax
import jax.numpy as jnp
from jax import lax
from jax.experimental import pallas as pl
from jax.experimental.pallas import tpu as pltpu
from jax.sharding import Mesh
from jax.sharding import PartitionSpec as P


EPS = 1e-06
ROUTED_SCALE = 2.5
TP = ("z", "c")
F32, BF16 = jnp.float32, jnp.bfloat16
FULL = 53 * 2**20
ROOM = pltpu.CompilerParams(vmem_limit_bytes=20 * 2**20)


def swapped(x):
    return lax.ppermute(x, "c", [(0, 1), (1, 0)])


def moved(x, axis, steps):
    count = lax.axis_size(axis)
    return lax.ppermute(x, axis, [(i, (i + steps) % count) for i in range(count)])


def exchanged(x, axis, bit):
    return lax.ppermute(x, axis, [(i, i ^ bit) for i in range(lax.axis_size(axis))])


def added(x, part, first):
    rest = x.shape[0] - first - part.shape[0]
    part = lax.pad(part.astype(F32), jnp.zeros((), F32), ((first, rest, 0), (0, 0, 0)))
    return (x.astype(F32) + part).astype(BF16)


def rms_scale(values_in, gains):
    values = values_in.astype(F32)
    factor = lax.rsqrt(jnp.mean(values * values, axis=-1, keepdims=True) + EPS)
    return (values * factor * gains).astype(BF16)


def dot32(a, b):
    return jnp.dot(a, b, preferred_element_type=F32)


def dot_nt(a, b):
    return lax.dot_general(a, b, (((1,), (1,)), ((), ())), preferred_element_type=F32)


def two_parts(x):
    high = x.astype(BF16)
    return high, (x - high.astype(F32)).astype(BF16)


def cost(flops, moved):
    return pl.CostEstimate(flops=flops, bytes_accessed=moved, transcendentals=0)


def fetch(source, target, arrival):
    copy = pltpu.make_async_copy(source, target, arrival)
    copy.start()
    copy.wait()


def front_kernel(
    core,
    log_step,
    tokens,
    norm_gain,
    w_in,
    decay_rate,
    frequency,
    input_real,
    input_imag,
    readout_real,
    readout_imag,
    skip_gain,
    state_real,
    state_imag,
    w_out,
    new_real,
    new_imag,
    kept,
    given,
):
    groups = log_step.shape[0]
    chan_count, entries = input_real.shape
    channels = skip_gain.shape[1]
    width = entries // groups
    normed = rms_scale(tokens[...], norm_gain[...])
    drive = dot32(normed, w_in[...]).astype(BF16)
    group_of = lax.broadcasted_iota(jnp.int32, (1, entries), 1) // width
    step_size = jnp.zeros((1, entries), F32)
    for g in range(groups):
        step_size = jnp.where(group_of == g, log_step[g], step_size)
    step_size = jnp.exp(step_size)
    decays, omegas = decay_rate[...], frequency[...]
    pole_mag = jnp.exp(-decays * step_size)
    pole_angle = omegas * step_size
    pole_re = pole_mag * jnp.cos(pole_angle)
    pole_im = pole_mag * jnp.sin(pole_angle)
    pole_norm = decays * decays + omegas * omegas
    diff_re = pole_re - 1.0
    lift_re = (-decays * diff_re + omegas * pole_im) / pole_norm
    lift_im = (-decays * pole_im - omegas * diff_re) / pole_norm
    row_group = lax.broadcasted_iota(jnp.int32, (channels, entries), 0) // chan_count
    col_group = lax.broadcasted_iota(jnp.int32, (channels, entries), 1) // width
    same = row_group == col_group

    def spread(block):
        return two_parts(jnp.where(same, jnp.concatenate([block[...]] * groups, axis=0), 0.0))

    def push_of(block):
        high, low = spread(block)
        return dot32(drive, high) + dot32(drive, low)

    push_re, push_im = push_of(input_real), push_of(input_imag)
    old_re, old_im = state_real[...], state_imag[...]
    new_re = pole_re * old_re - pole_im * old_im + lift_re * push_re - lift_im * push_im
    new_im = pole_re * old_im + pole_im * old_re + lift_re * push_im + lift_im * push_re
    new_real[...] = new_re
    new_imag[...] = new_im

    def read_of(state, block):
        (high, low), (block_high, block_low) = two_parts(state), spread(block)
        return dot_nt(high, block_high) + dot_nt(high, block_low) + dot_nt(low, block_high)

    read = read_of(new_re, readout_real) - read_of(new_im, readout_imag)
    read = read + skip_gain[...] * drive.astype(F32)
    bent = jnp.tanh(0.7978845608028654 * (read + 0.044715 * (read * read * read)))
    activated = (0.5 * read * (1.0 + bent)).astype(BF16)
    wide = kept.shape[2]
    for z in range(kept.shape[0]):
        for out, c in ((kept, core[0]), (given, 1 - core[0])):
            at = pl.multiple_of((2 * z + c) * wide, wide)
            out[z] = dot32(activated, w_out[:, pl.ds(at, wide)]).astype(out.dtype)


def front(core, log_step, *arrays):
    tokens, w_out, state = arrays[0], arrays[-1], arrays[-2]
    seqs, model_width = tokens.shape
    z_count = lax.axis_size("z")
    part = (z_count, seqs, model_width // (2 * z_count))
    smem, vmem = pl.BlockSpec(memory_space=pltpu.SMEM), pl.BlockSpec(memory_space=pltpu.VMEM)
    return pl.pallas_call(
        front_kernel,
        out_shape=(
            jax.ShapeDtypeStruct(state.shape, F32),
            jax.ShapeDtypeStruct(state.shape, F32),
            jax.ShapeDtypeStruct(part, BF16),
            jax.ShapeDtypeStruct(part, BF16),
        ),
        in_specs=[smem, smem] + [vmem] * len(arrays),
        out_specs=(vmem,) * 4,
        cost_estimate=cost(4 * seqs * model_width * w_out.shape[0], 2 * w_out.size * 2),
        name="front",
    )(core, log_step, *arrays)


def gate_up_kernel(
    at, arrived, gain, gate, gate_par, up, up_par, *refs
):
    *sent, near, far, incoming, weights, parcel, ins, outs = refs
    half, _, _, width, _ = weights.shape
    seq_devs, _, pair_slots, _ = incoming.shape
    z_count, _, lanes = parcel.shape
    capacity = pair_slots // half
    rows = seq_devs * capacity
    first = pltpu.make_async_copy(arrived, incoming, ins.at[0])
    first.start()
    loads = {}
    for e in range(half):
        for m, (own, par) in enumerate(((gate, gate_par), (up, up_par))):
            for part, source in enumerate((own.at[half * at[0] + e], par.at[half * at[0] + e])):
                arrival = ins.at[1 + 4 * e + 2 * m + part]
                copy = pltpu.make_async_copy(source, weights.at[e, m, part], arrival)
                copy.start()
                loads[e, m, part] = copy
    ones = jnp.ones((8, width), BF16)
    features = [pl.ds(pl.multiple_of(at[1 + part] * width, width), width) for part in range(2)]
    first.wait()
    stores = []

    def store(source, target):
        copy = pltpu.make_async_copy(source, target, outs.at[len(stores)])
        copy.start()
        stores.append(copy)

    def put(depth, size, block_of):
        for chip in range(z_count):
            steps = lax.rem(chip - at[3] + z_count, z_count)
            parcel[steps, depth : depth + size, :] = block_of(chip)

    scaled = {}
    for e in range(half):
        squares = jnp.zeros((8, rows), F32)
        for part in range(2):
            values = incoming[:, part, e * capacity : (e + 1) * capacity, :]
            values = values.reshape(rows, width).astype(F32)
            scaled[e, part] = (values * gain[:, features[part]]).astype(BF16)
            high, low = two_parts(values * values)
            squares = squares + dot_nt(ones, high) + dot_nt(ones, low)
        high, low = two_parts(squares)
        line = lax.broadcasted_iota(jnp.int32, squares.shape, 0)
        both = jnp.where(line == 0, high.astype(F32), jnp.where(line == 1, low.astype(F32), 0.0))
        depth = 2 * half * rows + e * 8
        put(depth, 8, lambda chip, both=both: both.astype(BF16))
    for e in range(half):
        for m in range(2):
            for part in range(2):
                loads[e, m, part].wait()
            sums = dot32(scaled[e, 0], weights[e, m, 0]) + dot32(scaled[e, 1], weights[e, m, 1])
            sums = sums.astype(BF16)
            depth = (half * m + e) * rows
            put(depth, rows, lambda chip, sums=sums: sums[:, chip * lanes : (chip + 1) * lanes])
    middle, split = z_count // 2, near.shape[0]
    store(parcel.at[middle, pl.ds(0, split), :], near)
    store(parcel.at[middle, pl.ds(split, far.shape[0]), :], far)
    for steps in range(middle):
        store(parcel.at[steps], sent[steps])
    for steps in range(middle + 1, z_count):
        store(parcel.at[steps], sent[steps - 1])
    for copy in stores:
        copy.wait()


def gate_up(at, incoming, gain, gate, gate_par, up, up_par):
    seq_devs, _, pair_slots, width = incoming.shape
    half, units = gate.shape[0] // 2, gate.shape[2]
    z_count = lax.axis_size("z")
    pair_rows = seq_devs * pair_slots
    parcel = (z_count, 2 * pair_rows + half * 8, units // z_count)
    smem, vmem = pl.BlockSpec(memory_space=pltpu.SMEM), pl.BlockSpec(memory_space=pltpu.VMEM)
    far, any_place = pl.BlockSpec(memory_space=pltpu.HBM), pl.BlockSpec(memory_space=pl.ANY)
    return pl.pallas_call(
        gate_up_kernel,
        in_specs=[smem, any_place, vmem, far, any_place, far, any_place],
        out_specs=(any_place,) * (z_count + 1),
        out_shape=(jax.ShapeDtypeStruct(parcel[1:], BF16),) * (z_count - 1)
        + (jax.ShapeDtypeStruct((parcel[1] // 2, parcel[2]), BF16),) * 2,
        scratch_shapes=[
            pltpu.VMEM(incoming.shape, BF16),
            pltpu.VMEM((half, 2, 2, width, units), BF16),
            pltpu.VMEM(parcel, BF16),
            pltpu.SemaphoreType.DMA((1 + 4 * half,)),
            pltpu.SemaphoreType.DMA((z_count + 1,)),
        ],
        compiler_params=pltpu.CompilerParams(vmem_limit_bytes=52 * 2**20),
        cost_estimate=cost(8 * pair_rows * width * units, 8 * half * width * units),
        name="gate_up",
    )(at, incoming, gain, gate, gate_par, up, up_par)


def dispatch_kernel(spread, own_in, par_in, outgoing, own, par, arrivals):
    copies = [
        pltpu.make_async_copy(source, target, arrivals.at[i])
        for i, (source, target) in enumerate(((own_in, own), (par_in, par)))
    ]
    for copy in copies:
        copy.start()
    for copy in copies:
        copy.wait()
    shape = outgoing.shape[:1] + outgoing.shape[2:]
    for part, rows in enumerate((own, par)):
        outgoing[:, part] = dot32(spread[...], rows[...]).astype(BF16).reshape(shape)


def dispatch(spread, own, par, ep_count):
    slots, (_, width) = spread.shape[0], own.shape
    vmem = pl.BlockSpec(memory_space=pltpu.VMEM)
    return pl.pallas_call(
        dispatch_kernel,
        out_shape=jax.ShapeDtypeStruct((ep_count, 2, slots // ep_count, width), BF16),
        in_specs=[vmem, pl.BlockSpec(memory_space=pl.ANY), pl.BlockSpec(memory_space=pl.ANY)],
        out_specs=vmem,
        scratch_shapes=[
            pltpu.VMEM(own.shape, BF16),
            pltpu.VMEM(own.shape, BF16),
            pltpu.SemaphoreType.DMA((2,)),
        ],
        compiler_params=ROOM,
        cost_estimate=cost(4 * spread.size * width, 4 * slots * width),
        name="dispatch",
    )(spread, own, par)


def combine_kernel(weights, arrived, own, given, returned, arrival):
    fetch(arrived, returned, arrival)
    high, low = two_parts(weights[...])
    rows, width = weights.shape[1], returned.shape[3]
    for part, out in enumerate((own, given)):
        values = returned[:, part].reshape(rows, width)
        out[...] = (dot32(high, values) + dot32(low, values)).astype(out.dtype)


def combined(weights, returned):
    shape = (weights.shape[0], returned.shape[3])
    vmem = pl.BlockSpec(memory_space=pltpu.VMEM)
    return pl.pallas_call(
        combine_kernel,
        out_shape=(jax.ShapeDtypeStruct(shape, F32), jax.ShapeDtypeStruct(shape, BF16)),
        in_specs=[vmem, pl.BlockSpec(memory_space=pl.ANY)],
        out_specs=(vmem, vmem),
        scratch_shapes=[pltpu.VMEM(returned.shape, BF16), pltpu.SemaphoreType.DMA],
        compiler_params=ROOM,
        cost_estimate=cost(8 * weights.size * shape[1], 2 * returned.size),
        name="combine",
    )(weights, returned)


def shared_kernel(at, pieces, gain, sources, kept, given, gate_t, up_t, down_t, arrivals):
    copies = [
        pltpu.make_async_copy(source, target, arrivals.at[i])
        for i, (source, target) in enumerate(zip(sources, (gate_t, up_t, down_t), strict=True))
    ]
    for copy in copies:
        copy.start()
    for copy in copies:
        copy.wait()
    c, z = at[0], at[3]
    seqs, width = kept.shape[1:]
    squares = jnp.zeros((seqs, 1), F32)
    gate = jnp.zeros((seqs, gate_t.shape[0]), F32)
    up = gate
    chips = grown_order(kept.shape[0])
    for part, place in ((0, c), (1, 1 - c)):
        rows = [piece[part][i] for piece in pieces for i in range(piece[part].shape[0])]
        for chip, values in zip(chips, rows, strict=True):
            values = values.astype(F32)
            squares = squares + jnp.sum(values * values, axis=-1, keepdims=True)
            first = (2 * jnp.bitwise_xor(z, chip) + place) * width
            features = pl.ds(pl.multiple_of(first, width), width)
            scaled = (values * gain[:, features]).astype(BF16)
            gate = gate + dot_nt(scaled, gate_t[:, features])
            up = up + dot_nt(scaled, up_t[:, features])
    factor = lax.rsqrt(squares / (2 * len(chips) * width) + EPS)
    gate, up = gate * factor, up * factor
    inner = (gate / (1.0 + jnp.exp(-gate)) * up).astype(BF16)
    for chip in range(len(chips)):
        for out, place in ((kept, c), (given, 1 - c)):
            first = (2 * jnp.bitwise_xor(z, chip) + place) * width
            features = pl.ds(pl.multiple_of(first, width), width)
            out[chip] = dot32(inner, down_t[:, features]).astype(out.dtype)


def growing(chips):
    return [1] + [chips >> i for i in range(1, chips.bit_length() - 1)]


def grown_order(chips):
    order = [0]
    for bit in growing(chips):
        order = order + [owner ^ bit for owner in order]
    return order


def shared_parts(at, pieces, gain, gate_t, up_t, w_down, after):
    smem, vmem = pl.BlockSpec(memory_space=pltpu.SMEM), pl.BlockSpec(memory_space=pltpu.VMEM)
    flat = [rows for piece in pieces for rows in piece]
    (seqs, width), z_count = flat[0].shape[1:], sum(rows.shape[0] for rows in flat) // 2

    def kernel(at, *refs):
        rows, (gain, *rest) = refs[: len(flat)], refs[len(flat) :]
        paired = [(rows[i], rows[i + 1]) for i in range(0, len(flat), 2)]
        shared_kernel(at, paired, gain, rest[:3], *rest[4:])

    return pl.pallas_call(
        kernel,
        out_shape=(
            jax.ShapeDtypeStruct((z_count, seqs, width), F32),
            jax.ShapeDtypeStruct((z_count, seqs, width), BF16),
        ),
        in_specs=[smem] + [vmem] * (len(flat) + 1) + [pl.BlockSpec(memory_space=pl.ANY)] * 4,
        out_specs=(vmem, vmem),
        scratch_shapes=[
            pltpu.VMEM(gate_t.shape, BF16),
            pltpu.VMEM(up_t.shape, BF16),
            pltpu.VMEM(w_down.shape, BF16),
            pltpu.SemaphoreType.DMA((3,)),
        ],
        compiler_params=pltpu.CompilerParams(vmem_limit_bytes=FULL),
        cost_estimate=cost(seqs * 6 * w_down.size, 6 * w_down.size),
        name="shared",
    )(at, *flat, gain, gate_t, up_t, w_down, after)


def inner_kernel(model_width, half, *refs):
    *arrived, inner, parcels, arrivals = refs
    copies = [
        pltpu.make_async_copy(source, parcels.at[i], arrivals.at[i])
        for i, source in enumerate(arrived)
    ]
    for copy in copies:
        copy.start()
    for copy in copies:
        copy.wait()
    totals = parcels[0].astype(F32)
    for i in range(1, len(copies)):
        totals = totals + parcels[i].astype(F32)
    lanes = totals.shape[1]
    z_count, pair_rows, _ = inner.shape
    rows = pair_rows // half
    for e in range(half):
        line = 2 * pair_rows + 8 * e
        squares = totals[line : line + 1] + totals[line + 1 : line + 2]
        factor = lax.rsqrt(squares / model_width + EPS)
        factor = jnp.broadcast_to(factor, (lanes, rows)).T
        gate = totals[e * rows : (e + 1) * rows] * factor
        up = totals[pair_rows + e * rows : pair_rows + (e + 1) * rows] * factor
        done = (gate / (1.0 + jnp.exp(-gate)) * up).astype(BF16)
        for z in range(z_count):
            inner[z, e * rows : (e + 1) * rows, :] = done


def inner_copies(parcels, z_count, model_width, half):
    depth, lanes = parcels[0].shape
    pair_rows = (depth - half * 8) // 2
    count = len(parcels)
    return pl.pallas_call(
        functools.partial(inner_kernel, model_width, half),
        out_shape=jax.ShapeDtypeStruct((z_count, pair_rows, lanes), BF16),
        in_specs=[pl.BlockSpec(memory_space=pl.ANY)] * count,
        out_specs=pl.BlockSpec(memory_space=pltpu.VMEM),
        scratch_shapes=[
            pltpu.VMEM((count, depth, lanes), BF16),
            pltpu.SemaphoreType.DMA((count,)),
        ],
        compiler_params=ROOM,
        cost_estimate=cost(depth * lanes * 32, depth * lanes * 32),
        name="inner",
    )(*parcels)


def down_kernel(at, arrived, own, par, sent, inner, weights, results, ins, outs):
    half = weights.shape[0]
    first = pltpu.make_async_copy(arrived, inner, ins.at[0])
    first.start()
    loads = []
    for e in range(half):
        for part, source in enumerate((own.at[half * at[0] + e], par.at[half * at[0] + e])):
            arrival = ins.at[1 + 2 * e + part]
            copy = pltpu.make_async_copy(source, weights.at[e, part], arrival)
            copy.start()
            loads.append(copy)
    first.wait()
    rows = inner.shape[1] // half
    seq_devs, _, pair_slots, width = results.shape
    capacity = pair_slots // half
    stores = []
    for e in range(half):
        row = [inner[z, e * rows : (e + 1) * rows, :] for z in range(inner.shape[0])]
        row = jnp.concatenate(row, axis=1)
        place = slice(e * capacity, (e + 1) * capacity)
        for part in range(2):
            loads[2 * e + part].wait()
            out = dot32(row, weights[e, part]).astype(BF16)
            results[:, part, place, :] = out.reshape(seq_devs, capacity, width)
        place = pl.ds(e * capacity, capacity)
        copy = pltpu.make_async_copy(
            results.at[:, :, place, :], sent.at[:, :, place, :], outs.at[e]
        )
        copy.start()
        stores.append(copy)
    for copy in stores:
        copy.wait()


def down(at, inner, w_down, w_par, seq_devs, capacity):
    half, units, width = w_par.shape[0] // 2, *w_par.shape[1:]
    results = (seq_devs, 2, half * capacity, width)
    smem, any_place = pl.BlockSpec(memory_space=pltpu.SMEM), pl.BlockSpec(memory_space=pl.ANY)
    return pl.pallas_call(
        down_kernel,
        in_specs=[smem, any_place, any_place, any_place],
        out_specs=pl.BlockSpec(memory_space=pltpu.HBM),
        out_shape=pltpu.HBM(results, BF16),
        scratch_shapes=[
            pltpu.VMEM(inner.shape, BF16),
            pltpu.VMEM((half, 2, units, width), BF16),
            pltpu.VMEM(results, BF16),
            pltpu.SemaphoreType.DMA((1 + 2 * half,)),
            pltpu.SemaphoreType.DMA((half,)),
        ],
        compiler_params=ROOM,
        cost_estimate=cost(4 * inner.shape[1] * units * width, 4 * half * units * width),
        name="down",
    )(at, inner, w_down, w_par)


def local(
    tokens,
    norm_gain,
    ffn_gain,
    w_in,
    decay_rate,
    frequency,
    log_step,
    input_real,
    input_imag,
    readout_real,
    readout_imag,
    skip_gain,
    state_real,
    state_imag,
    w_out,
    shared_gate,
    shared_up,
    shared_down,
    expert_gate,
    expert_up,
    expert_down,
    routing,
    route_weight,
):
    seq_count, model_width = tokens.shape
    ep_count, z_count = lax.axis_size("ep"), lax.axis_size("z")
    z, c = lax.axis_index("z"), lax.axis_index("c")
    core = c.reshape(1)
    slice_width = model_width // (2 * z_count)
    offset = (2 * z + c) * slice_width

    new_real, new_imag, kept, given = front(
        core,
        log_step,
        tokens,
        norm_gain.reshape(1, -1),
        w_in,
        decay_rate.reshape(1, -1),
        frequency.reshape(1, -1),
        input_real,
        input_imag,
        readout_real,
        readout_imag,
        skip_gain.reshape(1, -1),
        state_real,
        state_imag,
        w_out,
    )
    got = swapped(given)
    both = (kept.astype(F32) + got.astype(F32)).astype(BF16)

    gate_par, up_par, down_par = (swapped(w) for w in (expert_gate, expert_up, expert_down))

    mixer_own = lax.all_to_all(both, "z", split_axis=0, concat_axis=0, tiled=True)
    mixer_own = mixer_own.astype(F32).sum(axis=0)
    own_tokens = lax.dynamic_slice_in_dim(tokens, offset, slice_width, 1)
    resid_own = (own_tokens.astype(F32) + mixer_own).astype(BF16)
    resid_par = swapped(resid_own)

    expert_dev = expert_gate.shape[0]
    half = expert_dev // 2
    top_count = routing.shape[1]
    capacity = 2 * seq_count * top_count // (expert_dev * ep_count)
    slot_count = half * ep_count * capacity
    flat_ids = routing.reshape(-1)
    one_hot = (
        flat_ids[:, None] == jnp.arange(expert_dev * ep_count, dtype=jnp.int32)[None, :]
    ).astype(jnp.int32)
    earlier = jnp.cumsum(one_hot, axis=0) - one_hot
    slot_rank = jnp.sum(earlier * one_hot, axis=1)
    home, within = flat_ids // expert_dev, flat_ids % expert_dev
    target = (home * half + within % half) * capacity + slot_rank
    target = jnp.where(within // half == c, target, -1)
    slot_ids = jnp.arange(slot_count, dtype=jnp.int32)
    placed = (target[None, :] == slot_ids[:, None]).reshape(slot_count, seq_count, top_count)
    spread = jnp.sum(placed.astype(F32), axis=2).astype(BF16)
    outgoing = dispatch(spread, resid_own, resid_par, ep_count)
    incoming = lax.all_to_all(outgoing, "ep", split_axis=0, concat_axis=0, tiled=True)

    at = jnp.array([1, 1, -1, 0], jnp.int32) * c + jnp.array([0, 2, 2, 1], jnp.int32) * z
    at = at + jnp.array([0, 0, 1, 0], jnp.int32)
    gain = ffn_gain.reshape(1, -1)
    *sent, near, far = gate_up(at, incoming, gain, expert_gate, gate_par, expert_up, up_par)
    middle = z_count // 2
    chunks = dict(zip([k for k in range(z_count) if k != middle], sent, strict=True))
    from_below = moved(near, "z", 1)
    from_above = moved(far, "z", -1)
    chunks[middle - 1] = added(chunks[middle - 1], from_below, 0)
    chunks[middle + 1] = added(chunks[middle + 1], from_above, near.shape[0])
    parcels = [chunks[0]]
    for steps in range(1, middle):
        parcels.append(moved(chunks[steps], "z", steps))
        parcels.append(moved(chunks[z_count - steps], "z", -steps))
    copies = inner_copies(parcels, z_count, model_width, half)
    inner_all = lax.all_to_all(copies, "z", split_axis=0, concat_axis=0, tiled=True)
    results = down(at, inner_all, expert_down, down_par, ep_count, capacity)
    returned = lax.all_to_all(results, "ep", split_axis=0, concat_axis=0, tiled=True)

    pieces = [(resid_own[None], resid_par[None])]
    for bit in growing(z_count):
        held = jnp.concatenate([piece[0] for piece in pieces])
        theirs = exchanged(held, "z", bit)
        pieces.append((theirs, swapped(theirs)))
    kept, given = shared_parts(
        at, pieces, gain, shared_gate.T, shared_up.T, shared_down, copies
    )
    got = swapped(given)
    shared_own = kept + got.astype(F32)
    count = z_count // 2
    while count > 0:
        theirs = exchanged(shared_own[count:].astype(BF16), "z", count)
        shared_own = shared_own[:count] + theirs.astype(F32)
        count //= 2
    shared_own = shared_own[0]

    weights = route_weight / jnp.sum(route_weight, axis=1, keepdims=True) * ROUTED_SCALE
    chosen = target.reshape(seq_count, top_count)[:, :, None] == slot_ids[None, None, :]
    combine = jnp.sum(jnp.where(chosen, weights[:, :, None], 0.0), axis=1)
    routed, routed_par = combined(combine, returned)
    routed = routed + swapped(routed_par).astype(F32)
    mixed = (resid_own.astype(F32) + shared_own + routed).astype(BF16)
    return (mixed, new_real, new_imag)


def solution(mesh):
    ep_count, tp_count = mesh.devices.shape
    cores = Mesh(mesh.devices.reshape(ep_count, tp_count // 2, 2), ("ep", "z", "c"))
    placed = (
        P("ep", None),
        P(),
        P(),
        P(None, TP),
        P(TP),
        P(TP),
        P(TP),
        P(None, TP),
        P(None, TP),
        P(None, TP),
        P(None, TP),
        P(TP),
        P("ep", TP),
        P("ep", TP),
        P(TP, None),
        P(None, TP),
        P(None, TP),
        P(TP, None),
        P("ep", TP, None),
        P("ep", TP, None),
        P("ep", None, TP),
        P("ep", None),
        P("ep", None),
    )

    def step(*arrays):
        return local(*arrays)

    step = jax.shard_map(
        step,
        mesh=cores,
        in_specs=placed,
        out_specs=(P("ep", TP), P("ep", TP), P("ep", TP)),
        check_vma=False,
    )
    return step
```

```python
import functools

import jax
import jax.numpy as jnp
from jax import lax
from jax.experimental import pallas as pl
from jax.experimental.pallas import tpu as pltpu
from jax.sharding import Mesh
from jax.sharding import PartitionSpec as P


EPS = 1e-06
ROUTED_SCALE = 2.5
TP = ("z", "c")
F32, BF16 = jnp.float32, jnp.bfloat16
FULL = 53 * 2**20
ROOM = pltpu.CompilerParams(vmem_limit_bytes=20 * 2**20)


def swapped(x):
    return lax.ppermute(x, "c", [(0, 1), (1, 0)])


def moved(x, axis, steps):
    count = lax.axis_size(axis)
    return lax.ppermute(x, axis, [(i, (i + steps) % count) for i in range(count)])


def both_ways(x, steps):
    count = lax.axis_size("z")
    ups = [(2 * i, 2 * ((i + steps) % count)) for i in range(count)]
    downs = [(2 * i + 1, 2 * ((i - steps) % count) + 1) for i in range(count)]
    return lax.ppermute(x, TP, ups + downs)


def added(x, part, first):
    rest = x.shape[0] - first - part.shape[0]
    part = lax.pad(part.astype(F32), jnp.zeros((), F32), ((first, rest, 0), (0, 0, 0)))
    return (x.astype(F32) + part).astype(BF16)


def rms_scale(values_in, gains):
    values = values_in.astype(F32)
    factor = lax.rsqrt(jnp.mean(values * values, axis=-1, keepdims=True) + EPS)
    return (values * factor * gains).astype(BF16)


def dot32(a, b):
    return jnp.dot(a, b, preferred_element_type=F32)


def dot_nt(a, b):
    return lax.dot_general(a, b, (((1,), (1,)), ((), ())), preferred_element_type=F32)


def two_parts(x):
    high = x.astype(BF16)
    return high, (x - high.astype(F32)).astype(BF16)


def cost(flops, moved):
    return pl.CostEstimate(flops=flops, bytes_accessed=moved, transcendentals=0)


def fetch(source, target, arrival):
    copy = pltpu.make_async_copy(source, target, arrival)
    copy.start()
    copy.wait()


def front_kernel(
    core,
    log_step,
    tokens,
    norm_gain,
    w_in,
    decay_rate,
    frequency,
    input_real,
    input_imag,
    readout_real,
    readout_imag,
    skip_gain,
    state_real,
    state_imag,
    w_out,
    new_real,
    new_imag,
    kept,
    given,
):
    groups = log_step.shape[0]
    chan_count, entries = input_real.shape
    channels = skip_gain.shape[1]
    width = entries // groups
    normed = rms_scale(tokens[...], norm_gain[...])
    drive = dot32(normed, w_in[...]).astype(BF16)
    group_of = lax.broadcasted_iota(jnp.int32, (1, entries), 1) // width
    step_size = jnp.zeros((1, entries), F32)
    for g in range(groups):
        step_size = jnp.where(group_of == g, log_step[g], step_size)
    step_size = jnp.exp(step_size)
    decays, omegas = decay_rate[...], frequency[...]
    pole_mag = jnp.exp(-decays * step_size)
    pole_angle = omegas * step_size
    pole_re = pole_mag * jnp.cos(pole_angle)
    pole_im = pole_mag * jnp.sin(pole_angle)
    pole_norm = decays * decays + omegas * omegas
    diff_re = pole_re - 1.0
    lift_re = (-decays * diff_re + omegas * pole_im) / pole_norm
    lift_im = (-decays * pole_im - omegas * diff_re) / pole_norm
    row_group = lax.broadcasted_iota(jnp.int32, (channels, entries), 0) // chan_count
    col_group = lax.broadcasted_iota(jnp.int32, (channels, entries), 1) // width
    same = row_group == col_group

    def spread(block):
        return two_parts(jnp.where(same, jnp.concatenate([block[...]] * groups, axis=0), 0.0))

    def push_of(block):
        high, low = spread(block)
        return dot32(drive, high) + dot32(drive, low)

    push_re, push_im = push_of(input_real), push_of(input_imag)
    old_re, old_im = state_real[...], state_imag[...]
    new_re = pole_re * old_re - pole_im * old_im + lift_re * push_re - lift_im * push_im
    new_im = pole_re * old_im + pole_im * old_re + lift_re * push_im + lift_im * push_re
    new_real[...] = new_re
    new_imag[...] = new_im

    def read_of(state, block):
        (high, low), (block_high, block_low) = two_parts(state), spread(block)
        return dot_nt(high, block_high) + dot_nt(high, block_low) + dot_nt(low, block_high)

    read = read_of(new_re, readout_real) - read_of(new_im, readout_imag)
    read = read + skip_gain[...] * drive.astype(F32)
    bent = jnp.tanh(0.7978845608028654 * (read + 0.044715 * (read * read * read)))
    activated = (0.5 * read * (1.0 + bent)).astype(BF16)
    wide = kept.shape[2]
    for z in range(kept.shape[0]):
        for out, c in ((kept, core[0]), (given, 1 - core[0])):
            at = pl.multiple_of((2 * z + c) * wide, wide)
            out[z] = dot32(activated, w_out[:, pl.ds(at, wide)]).astype(out.dtype)


def front(core, log_step, *arrays):
    tokens, w_out, state = arrays[0], arrays[-1], arrays[-2]
    seqs, model_width = tokens.shape
    z_count = lax.axis_size("z")
    part = (z_count, seqs, model_width // (2 * z_count))
    smem, vmem = pl.BlockSpec(memory_space=pltpu.SMEM), pl.BlockSpec(memory_space=pltpu.VMEM)
    return pl.pallas_call(
        front_kernel,
        out_shape=(
            jax.ShapeDtypeStruct(state.shape, F32),
            jax.ShapeDtypeStruct(state.shape, F32),
            jax.ShapeDtypeStruct(part, BF16),
            jax.ShapeDtypeStruct(part, BF16),
        ),
        in_specs=[smem, smem] + [vmem] * len(arrays),
        out_specs=(vmem,) * 4,
        cost_estimate=cost(4 * seqs * model_width * w_out.shape[0], 2 * w_out.size * 2),
        name="front",
    )(core, log_step, *arrays)


def gate_up_kernel(
    at, arrived, gain, gate, gate_par, up, up_par, *refs
):
    *sent, near, far, incoming, weights, parcel, ins, outs = refs
    half, _, _, width, _ = weights.shape
    seq_devs, _, pair_slots, _ = incoming.shape
    z_count, _, lanes = parcel.shape
    capacity = pair_slots // half
    rows = seq_devs * capacity
    first = pltpu.make_async_copy(arrived, incoming, ins.at[0])
    first.start()
    loads = {}
    for e in range(half):
        for m, (own, par) in enumerate(((gate, gate_par), (up, up_par))):
            for part, source in enumerate((own.at[half * at[0] + e], par.at[half * at[0] + e])):
                arrival = ins.at[1 + 4 * e + 2 * m + part]
                copy = pltpu.make_async_copy(source, weights.at[e, m, part], arrival)
                copy.start()
                loads[e, m, part] = copy
    ones = jnp.ones((8, width), BF16)
    features = [pl.ds(pl.multiple_of(at[1 + part] * width, width), width) for part in range(2)]
    first.wait()
    stores = []

    def store(source, target):
        copy = pltpu.make_async_copy(source, target, outs.at[len(stores)])
        copy.start()
        stores.append(copy)

    def put(depth, size, block_of):
        for chip in range(z_count):
            steps = lax.rem(chip - at[3] + z_count, z_count)
            parcel[steps, depth : depth + size, :] = block_of(chip)

    scaled = {}
    for e in range(half):
        squares = jnp.zeros((8, rows), F32)
        for part in range(2):
            values = incoming[:, part, e * capacity : (e + 1) * capacity, :]
            values = values.reshape(rows, width).astype(F32)
            scaled[e, part] = (values * gain[:, features[part]]).astype(BF16)
            high, low = two_parts(values * values)
            squares = squares + dot_nt(ones, high) + dot_nt(ones, low)
        high, low = two_parts(squares)
        line = lax.broadcasted_iota(jnp.int32, squares.shape, 0)
        both = jnp.where(line == 0, high.astype(F32), jnp.where(line == 1, low.astype(F32), 0.0))
        depth = 2 * half * rows + e * 8
        put(depth, 8, lambda chip, both=both: both.astype(BF16))
    for e in range(half):
        for m in range(2):
            for part in range(2):
                loads[e, m, part].wait()
            sums = dot32(scaled[e, 0], weights[e, m, 0]) + dot32(scaled[e, 1], weights[e, m, 1])
            sums = sums.astype(BF16)
            depth = (half * m + e) * rows
            put(depth, rows, lambda chip, sums=sums: sums[:, chip * lanes : (chip + 1) * lanes])
    middle, split = z_count // 2, near.shape[0]
    store(parcel.at[middle, pl.ds(0, split), :], near)
    store(parcel.at[middle, pl.ds(split, far.shape[0]), :], far)
    for steps in range(middle):
        store(parcel.at[steps], sent[steps])
    for steps in range(middle + 1, z_count):
        store(parcel.at[steps], sent[steps - 1])
    for copy in stores:
        copy.wait()


def gate_up(at, incoming, gain, gate, gate_par, up, up_par):
    seq_devs, _, pair_slots, width = incoming.shape
    half, units = gate.shape[0] // 2, gate.shape[2]
    z_count = lax.axis_size("z")
    pair_rows = seq_devs * pair_slots
    parcel = (z_count, 2 * pair_rows + half * 8, units // z_count)
    smem, vmem = pl.BlockSpec(memory_space=pltpu.SMEM), pl.BlockSpec(memory_space=pltpu.VMEM)
    far, any_place = pl.BlockSpec(memory_space=pltpu.HBM), pl.BlockSpec(memory_space=pl.ANY)
    return pl.pallas_call(
        gate_up_kernel,
        in_specs=[smem, any_place, vmem, far, any_place, far, any_place],
        out_specs=(any_place,) * (z_count + 1),
        out_shape=(jax.ShapeDtypeStruct(parcel[1:], BF16),) * (z_count - 1)
        + (jax.ShapeDtypeStruct((parcel[1] // 2, parcel[2]), BF16),) * 2,
        scratch_shapes=[
            pltpu.VMEM(incoming.shape, BF16),
            pltpu.VMEM((half, 2, 2, width, units), BF16),
            pltpu.VMEM(parcel, BF16),
            pltpu.SemaphoreType.DMA((1 + 4 * half,)),
            pltpu.SemaphoreType.DMA((z_count + 1,)),
        ],
        compiler_params=pltpu.CompilerParams(vmem_limit_bytes=52 * 2**20),
        cost_estimate=cost(8 * pair_rows * width * units, 8 * half * width * units),
        name="gate_up",
    )(at, incoming, gain, gate, gate_par, up, up_par)


def dispatch_kernel(spread, own_in, par_in, outgoing, own, par, arrivals):
    copies = [
        pltpu.make_async_copy(source, target, arrivals.at[i])
        for i, (source, target) in enumerate(((own_in, own), (par_in, par)))
    ]
    for copy in copies:
        copy.start()
    for copy in copies:
        copy.wait()
    shape = outgoing.shape[:1] + outgoing.shape[2:]
    for part, rows in enumerate((own, par)):
        outgoing[:, part] = dot32(spread[...], rows[...]).astype(BF16).reshape(shape)


def dispatch(spread, own, par, ep_count):
    slots, (_, width) = spread.shape[0], own.shape
    vmem = pl.BlockSpec(memory_space=pltpu.VMEM)
    return pl.pallas_call(
        dispatch_kernel,
        out_shape=jax.ShapeDtypeStruct((ep_count, 2, slots // ep_count, width), BF16),
        in_specs=[vmem, pl.BlockSpec(memory_space=pl.ANY), pl.BlockSpec(memory_space=pl.ANY)],
        out_specs=vmem,
        scratch_shapes=[
            pltpu.VMEM(own.shape, BF16),
            pltpu.VMEM(own.shape, BF16),
            pltpu.SemaphoreType.DMA((2,)),
        ],
        compiler_params=ROOM,
        cost_estimate=cost(4 * spread.size * width, 4 * slots * width),
        name="dispatch",
    )(spread, own, par)


def combine_kernel(weights, arrived, base, *refs):
    *parts, own, given, returned, arrival = refs
    fetch(arrived, returned, arrival)
    high, low = two_parts(weights[...])
    rows, width = weights.shape[1], returned.shape[3]
    for slot, out in enumerate((own, given)):
        values = returned[:, slot].reshape(rows, width)
        total = dot32(high, values) + dot32(low, values)
        if slot == 0:
            total = total + base[...]
        for part in parts:
            if slot < part.shape[0]:
                total = total + part[slot].astype(F32)
        out[...] = total.astype(out.dtype)


def combined(weights, returned, base, parts):
    shape = (weights.shape[0], returned.shape[3])
    vmem = pl.BlockSpec(memory_space=pltpu.VMEM)
    return pl.pallas_call(
        combine_kernel,
        out_shape=(jax.ShapeDtypeStruct(shape, F32), jax.ShapeDtypeStruct(shape, BF16)),
        in_specs=[vmem, pl.BlockSpec(memory_space=pl.ANY)] + [vmem] * (1 + len(parts)),
        out_specs=(vmem, vmem),
        scratch_shapes=[pltpu.VMEM(returned.shape, BF16), pltpu.SemaphoreType.DMA],
        compiler_params=ROOM,
        cost_estimate=cost(8 * weights.size * shape[1], 2 * returned.size),
        name="combine",
    )(weights, returned, base, *parts)


def shared_kernel(at, own, par, mine, theirs, gain, sources, kept, given, *scratch):
    *weights, arrivals = scratch
    copies = [
        pltpu.make_async_copy(source, target, arrivals.at[i])
        for i, (source, target) in enumerate(zip(sources, weights, strict=True))
    ]
    for copy in copies:
        copy.start()
    for copy in copies:
        copy.wait()
    gate_t, up_t, down_t = weights
    c, z = at[0], at[3]
    seqs, width = kept.shape[1:]
    chips = gain.shape[1] // (2 * width)
    way = 1 - 2 * c

    def features(steps, place):
        chip = lax.rem(z + way * steps + 2 * chips, chips)
        return pl.ds(pl.multiple_of((2 * chip + place) * width, width), width)

    squares = jnp.zeros((seqs, 1), F32)
    gate = jnp.zeros((seqs, gate_t.shape[0]), F32)
    up = gate
    rows = [(own[...], features(0, c)), (par[...], features(0, 1 - c))]
    for pieces, first, sign in ((mine, c, -1), (theirs, 1 - c, 1)):
        for k, piece in enumerate(pieces):
            rows.append((piece[0], features(sign * (k + 1), first)))
            if piece.shape[0] > 1:
                rows.append((piece[1], features(sign * (k + 1), 1 - first)))
    for values, place in rows:
        values = values.astype(F32)
        squares = squares + jnp.sum(values * values, axis=-1, keepdims=True)
        scaled = (values * gain[:, place]).astype(BF16)
        gate = gate + dot_nt(scaled, gate_t[:, place])
        up = up + dot_nt(scaled, up_t[:, place])
    factor = lax.rsqrt(squares / gain.shape[1] + EPS)
    gate, up = gate * factor, up * factor
    inner = (gate / (1.0 + jnp.exp(-gate)) * up).astype(BF16)
    for out, first, sign in ((kept, c, 1), (given, 1 - c, -1)):
        order = [(sign * k, place) for k in range(chips // 2 - 1, 0, -1) for place in (first, 1 - first)]
        for i, (steps, place) in enumerate([*order, (chips // 2, first), (0, first)]):
            out[i] = dot32(inner, down_t[:, features(steps, place)]).astype(out.dtype)


def shared_parts(at, own, par, mine, theirs, gain, gate_t, up_t, w_down, after):
    smem, vmem = pl.BlockSpec(memory_space=pltpu.SMEM), pl.BlockSpec(memory_space=pltpu.VMEM)
    (seqs, width), count = own.shape, len(mine)

    def kernel(at, own, par, *refs):
        first, second, (gain, *rest) = refs[:count], refs[count : 2 * count], refs[2 * count :]
        shared_kernel(at, own, par, first, second, gain, rest[:3], *rest[4:])

    return pl.pallas_call(
        kernel,
        out_shape=(
            jax.ShapeDtypeStruct((2 * count, seqs, width), F32),
            jax.ShapeDtypeStruct((2 * count, seqs, width), BF16),
        ),
        in_specs=[smem] + [vmem] * (2 * count + 3) + [pl.BlockSpec(memory_space=pl.ANY)] * 4,
        out_specs=(vmem, vmem),
        scratch_shapes=[
            pltpu.VMEM(gate_t.shape, BF16),
            pltpu.VMEM(up_t.shape, BF16),
            pltpu.VMEM(w_down.shape, BF16),
            pltpu.SemaphoreType.DMA((3,)),
        ],
        compiler_params=pltpu.CompilerParams(vmem_limit_bytes=FULL),
        cost_estimate=cost(seqs * 6 * w_down.size, 6 * w_down.size),
        name="shared",
    )(at, own, par, *mine, *theirs, gain, gate_t, up_t, w_down, after)


def inner_kernel(model_width, half, *refs):
    *arrived, inner, parcels, arrivals = refs
    copies = [
        pltpu.make_async_copy(source, parcels.at[i], arrivals.at[i])
        for i, source in enumerate(arrived)
    ]
    for copy in copies:
        copy.start()
    for copy in copies:
        copy.wait()
    totals = parcels[0].astype(F32)
    for i in range(1, len(copies)):
        totals = totals + parcels[i].astype(F32)
    lanes = totals.shape[1]
    z_count, pair_rows, _ = inner.shape
    rows = pair_rows // half
    for e in range(half):
        line = 2 * pair_rows + 8 * e
        squares = totals[line : line + 1] + totals[line + 1 : line + 2]
        factor = lax.rsqrt(squares / model_width + EPS)
        factor = jnp.broadcast_to(factor, (lanes, rows)).T
        gate = totals[e * rows : (e + 1) * rows] * factor
        up = totals[pair_rows + e * rows : pair_rows + (e + 1) * rows] * factor
        done = (gate / (1.0 + jnp.exp(-gate)) * up).astype(BF16)
        for z in range(z_count):
            inner[z, e * rows : (e + 1) * rows, :] = done


def inner_copies(parcels, z_count, model_width, half):
    depth, lanes = parcels[0].shape
    pair_rows = (depth - half * 8) // 2
    count = len(parcels)
    return pl.pallas_call(
        functools.partial(inner_kernel, model_width, half),
        out_shape=jax.ShapeDtypeStruct((z_count, pair_rows, lanes), BF16),
        in_specs=[pl.BlockSpec(memory_space=pl.ANY)] * count,
        out_specs=pl.BlockSpec(memory_space=pltpu.VMEM),
        scratch_shapes=[
            pltpu.VMEM((count, depth, lanes), BF16),
            pltpu.SemaphoreType.DMA((count,)),
        ],
        compiler_params=ROOM,
        cost_estimate=cost(depth * lanes * 32, depth * lanes * 32),
        name="inner",
    )(*parcels)


def down_kernel(at, arrived, own, par, sent, inner, weights, results, ins, outs):
    half = weights.shape[0]
    first = pltpu.make_async_copy(arrived, inner, ins.at[0])
    first.start()
    loads = []
    for e in range(half):
        for part, source in enumerate((own.at[half * at[0] + e], par.at[half * at[0] + e])):
            arrival = ins.at[1 + 2 * e + part]
            copy = pltpu.make_async_copy(source, weights.at[e, part], arrival)
            copy.start()
            loads.append(copy)
    first.wait()
    rows = inner.shape[1] // half
    seq_devs, _, pair_slots, width = results.shape
    capacity = pair_slots // half
    stores = []
    for e in range(half):
        row = [inner[z, e * rows : (e + 1) * rows, :] for z in range(inner.shape[0])]
        row = jnp.concatenate(row, axis=1)
        place = slice(e * capacity, (e + 1) * capacity)
        for part in range(2):
            loads[2 * e + part].wait()
            out = dot32(row, weights[e, part]).astype(BF16)
            results[:, part, place, :] = out.reshape(seq_devs, capacity, width)
        place = pl.ds(e * capacity, capacity)
        copy = pltpu.make_async_copy(
            results.at[:, :, place, :], sent.at[:, :, place, :], outs.at[e]
        )
        copy.start()
        stores.append(copy)
    for copy in stores:
        copy.wait()


def down(at, inner, w_down, w_par, seq_devs, capacity):
    half, units, width = w_par.shape[0] // 2, *w_par.shape[1:]
    results = (seq_devs, 2, half * capacity, width)
    smem, any_place = pl.BlockSpec(memory_space=pltpu.SMEM), pl.BlockSpec(memory_space=pl.ANY)
    return pl.pallas_call(
        down_kernel,
        in_specs=[smem, any_place, any_place, any_place],
        out_specs=pl.BlockSpec(memory_space=pltpu.HBM),
        out_shape=pltpu.HBM(results, BF16),
        scratch_shapes=[
            pltpu.VMEM(inner.shape, BF16),
            pltpu.VMEM((half, 2, units, width), BF16),
            pltpu.VMEM(results, BF16),
            pltpu.SemaphoreType.DMA((1 + 2 * half,)),
            pltpu.SemaphoreType.DMA((half,)),
        ],
        compiler_params=ROOM,
        cost_estimate=cost(4 * inner.shape[1] * units * width, 4 * half * units * width),
        name="down",
    )(at, inner, w_down, w_par)


def local(
    tokens,
    norm_gain,
    ffn_gain,
    w_in,
    decay_rate,
    frequency,
    log_step,
    input_real,
    input_imag,
    readout_real,
    readout_imag,
    skip_gain,
    state_real,
    state_imag,
    w_out,
    shared_gate,
    shared_up,
    shared_down,
    expert_gate,
    expert_up,
    expert_down,
    routing,
    route_weight,
):
    seq_count, model_width = tokens.shape
    ep_count, z_count = lax.axis_size("ep"), lax.axis_size("z")
    z, c = lax.axis_index("z"), lax.axis_index("c")
    core = c.reshape(1)
    slice_width = model_width // (2 * z_count)
    offset = (2 * z + c) * slice_width

    new_real, new_imag, kept, given = front(
        core,
        log_step,
        tokens,
        norm_gain.reshape(1, -1),
        w_in,
        decay_rate.reshape(1, -1),
        frequency.reshape(1, -1),
        input_real,
        input_imag,
        readout_real,
        readout_imag,
        skip_gain.reshape(1, -1),
        state_real,
        state_imag,
        w_out,
    )
    got = swapped(given)
    both = (kept.astype(F32) + got.astype(F32)).astype(BF16)

    gate_par, up_par, down_par = (swapped(w) for w in (expert_gate, expert_up, expert_down))

    mixer_own = lax.all_to_all(both, "z", split_axis=0, concat_axis=0, tiled=True)
    mixer_own = mixer_own.astype(F32).sum(axis=0)
    own_tokens = lax.dynamic_slice_in_dim(tokens, offset, slice_width, 1)
    resid_own = (own_tokens.astype(F32) + mixer_own).astype(BF16)
    resid_par = swapped(resid_own)

    expert_dev = expert_gate.shape[0]
    half = expert_dev // 2
    top_count = routing.shape[1]
    capacity = 2 * seq_count * top_count // (expert_dev * ep_count)
    slot_count = half * ep_count * capacity
    flat_ids = routing.reshape(-1)
    one_hot = (
        flat_ids[:, None] == jnp.arange(expert_dev * ep_count, dtype=jnp.int32)[None, :]
    ).astype(jnp.int32)
    earlier = jnp.cumsum(one_hot, axis=0) - one_hot
    slot_rank = jnp.sum(earlier * one_hot, axis=1)
    home, within = flat_ids // expert_dev, flat_ids % expert_dev
    target = (home * half + within % half) * capacity + slot_rank
    target = jnp.where(within // half == c, target, -1)
    slot_ids = jnp.arange(slot_count, dtype=jnp.int32)
    placed = (target[None, :] == slot_ids[:, None]).reshape(slot_count, seq_count, top_count)
    spread = jnp.sum(placed.astype(F32), axis=2).astype(BF16)
    outgoing = dispatch(spread, resid_own, resid_par, ep_count)
    incoming = lax.all_to_all(outgoing, "ep", split_axis=0, concat_axis=0, tiled=True)

    at = jnp.array([1, 1, -1, 0], jnp.int32) * c + jnp.array([0, 2, 2, 1], jnp.int32) * z
    at = at + jnp.array([0, 0, 1, 0], jnp.int32)
    gain = ffn_gain.reshape(1, -1)
    *sent, near, far = gate_up(at, incoming, gain, expert_gate, gate_par, expert_up, up_par)
    middle = z_count // 2
    chunks = dict(zip([k for k in range(z_count) if k != middle], sent, strict=True))
    from_below = moved(near, "z", 1)
    from_above = moved(far, "z", -1)
    chunks[middle - 1] = added(chunks[middle - 1], from_below, 0)
    chunks[middle + 1] = added(chunks[middle + 1], from_above, near.shape[0])
    parcels = [chunks[0]]
    for steps in range(1, middle):
        parcels.append(moved(chunks[steps], "z", steps))
        parcels.append(moved(chunks[z_count - steps], "z", -steps))
    copies = inner_copies(parcels, z_count, model_width, half)
    inner_all = lax.all_to_all(copies, "z", split_axis=0, concat_axis=0, tiled=True)
    results = down(at, inner_all, expert_down, down_par, ep_count, capacity)
    returned = lax.all_to_all(results, "ep", split_axis=0, concat_axis=0, tiled=True)

    held = jnp.stack([resid_own, resid_par])
    mine, theirs = [], []
    for steps in range(1, middle + 1):
        mine.append(both_ways(held if steps < middle else resid_own[None], steps))
        theirs.append(swapped(mine[-1]))
    kept, given = shared_parts(
        at,
        resid_own,
        resid_par,
        mine,
        theirs,
        gain,
        shared_gate.T,
        shared_up.T,
        shared_down,
        copies,
    )
    got = swapped(given)
    shared_sums = kept + got.astype(F32)
    leaving = shared_sums.astype(BF16)
    shared_chip = []
    for steps in range(1, middle + 1):
        first = 2 * (middle - 1 - steps) if steps < middle else 2 * (middle - 1)
        part = leaving[first : first + (2 if steps < middle else 1)]
        shared_chip.append(both_ways(part, steps))

    weights = route_weight / jnp.sum(route_weight, axis=1, keepdims=True) * ROUTED_SCALE
    chosen = target.reshape(seq_count, top_count)[:, :, None] == slot_ids[None, None, :]
    combine = jnp.sum(jnp.where(chosen, weights[:, :, None], 0.0), axis=1)
    own, given = combined(combine, returned, shared_sums[-1], shared_chip)
    got = swapped(given)
    mixed = (resid_own.astype(F32) + own + got.astype(F32)).astype(BF16)
    return (mixed, new_real, new_imag)


def solution(mesh):
    ep_count, tp_count = mesh.devices.shape
    cores = Mesh(mesh.devices.reshape(ep_count, tp_count // 2, 2), ("ep", "z", "c"))
    placed = (
        P("ep", None),
        P(),
        P(),
        P(None, TP),
        P(TP),
        P(TP),
        P(TP),
        P(None, TP),
        P(None, TP),
        P(None, TP),
        P(None, TP),
        P(TP),
        P("ep", TP),
        P("ep", TP),
        P(TP, None),
        P(None, TP),
        P(None, TP),
        P(TP, None),
        P("ep", TP, None),
        P("ep", TP, None),
        P("ep", None, TP),
        P("ep", None),
        P("ep", None),
    )

    def step(*arrays):
        return local(*arrays)

    step = jax.shard_map(
        step,
        mesh=cores,
        in_specs=placed,
        out_specs=(P("ep", TP), P("ep", TP), P("ep", TP)),
        check_vma=False,
    )
    return step
```

```python
import functools

import jax
import jax.numpy as jnp
from jax import lax
from jax.experimental import pallas as pl
from jax.experimental.pallas import tpu as pltpu
from jax.sharding import Mesh
from jax.sharding import PartitionSpec as P


EPS = 1e-06
ROUTED_SCALE = 2.5
TP = ("z", "c")
F32, BF16 = jnp.float32, jnp.bfloat16
FULL = 53 * 2**20
ROOM = pltpu.CompilerParams(vmem_limit_bytes=20 * 2**20)


def swapped(x):
    return lax.ppermute(x, "c", [(0, 1), (1, 0)])


def moved(x, axis, steps):
    count = lax.axis_size(axis)
    return lax.ppermute(x, axis, [(i, (i + steps) % count) for i in range(count)])


def both_ways(x, steps):
    count = lax.axis_size("z")
    ups = [(2 * i, 2 * ((i + steps) % count)) for i in range(count)]
    downs = [(2 * i + 1, 2 * ((i - steps) % count) + 1) for i in range(count)]
    return lax.ppermute(x, TP, ups + downs)


def added(x, part, first):
    rest = x.shape[0] - first - part.shape[0]
    part = lax.pad(part.astype(F32), jnp.zeros((), F32), ((first, rest, 0), (0, 0, 0)))
    return (x.astype(F32) + part).astype(BF16)


def rms_scale(values_in, gains):
    values = values_in.astype(F32)
    factor = lax.rsqrt(jnp.mean(values * values, axis=-1, keepdims=True) + EPS)
    return (values * factor * gains).astype(BF16)


def dot32(a, b):
    return jnp.dot(a, b, preferred_element_type=F32)


def dot_nt(a, b):
    return lax.dot_general(a, b, (((1,), (1,)), ((), ())), preferred_element_type=F32)


def two_parts(x):
    high = x.astype(BF16)
    return high, (x - high.astype(F32)).astype(BF16)


def cost(flops, moved):
    return pl.CostEstimate(flops=flops, bytes_accessed=moved, transcendentals=0)


def fetch(source, target, arrival):
    copy = pltpu.make_async_copy(source, target, arrival)
    copy.start()
    copy.wait()


def front_kernel(
    core,
    log_step,
    tokens,
    norm_gain,
    w_in,
    decay_rate,
    frequency,
    input_real,
    input_imag,
    readout_real,
    readout_imag,
    skip_gain,
    state_real,
    state_imag,
    w_out,
    new_real,
    new_imag,
    kept,
    given,
):
    groups = log_step.shape[0]
    chan_count, entries = input_real.shape
    channels = skip_gain.shape[1]
    width = entries // groups
    normed = rms_scale(tokens[...], norm_gain[...])
    drive = dot32(normed, w_in[...]).astype(BF16)
    group_of = lax.broadcasted_iota(jnp.int32, (1, entries), 1) // width
    step_size = jnp.zeros((1, entries), F32)
    for g in range(groups):
        step_size = jnp.where(group_of == g, log_step[g], step_size)
    step_size = jnp.exp(step_size)
    decays, omegas = decay_rate[...], frequency[...]
    pole_mag = jnp.exp(-decays * step_size)
    pole_angle = omegas * step_size
    pole_re = pole_mag * jnp.cos(pole_angle)
    pole_im = pole_mag * jnp.sin(pole_angle)
    pole_norm = decays * decays + omegas * omegas
    diff_re = pole_re - 1.0
    lift_re = (-decays * diff_re + omegas * pole_im) / pole_norm
    lift_im = (-decays * pole_im - omegas * diff_re) / pole_norm
    row_group = lax.broadcasted_iota(jnp.int32, (channels, entries), 0) // chan_count
    col_group = lax.broadcasted_iota(jnp.int32, (channels, entries), 1) // width
    same = row_group == col_group

    def spread(block):
        return two_parts(jnp.where(same, jnp.concatenate([block[...]] * groups, axis=0), 0.0))

    def push_of(block):
        high, low = spread(block)
        return dot32(drive, high) + dot32(drive, low)

    push_re, push_im = push_of(input_real), push_of(input_imag)
    old_re, old_im = state_real[...], state_imag[...]
    new_re = pole_re * old_re - pole_im * old_im + lift_re * push_re - lift_im * push_im
    new_im = pole_re * old_im + pole_im * old_re + lift_re * push_im + lift_im * push_re
    new_real[...] = new_re
    new_imag[...] = new_im

    def read_of(state, block):
        (high, low), (block_high, block_low) = two_parts(state), spread(block)
        return dot_nt(high, block_high) + dot_nt(high, block_low) + dot_nt(low, block_high)

    read = read_of(new_re, readout_real) - read_of(new_im, readout_imag)
    read = read + skip_gain[...] * drive.astype(F32)
    bent = jnp.tanh(0.7978845608028654 * (read + 0.044715 * (read * read * read)))
    activated = (0.5 * read * (1.0 + bent)).astype(BF16)
    wide = kept.shape[2]
    for z in range(kept.shape[0]):
        for out, c in ((kept, core[0]), (given, 1 - core[0])):
            at = pl.multiple_of((2 * z + c) * wide, wide)
            out[z] = dot32(activated, w_out[:, pl.ds(at, wide)]).astype(out.dtype)


def front(core, log_step, *arrays):
    tokens, w_out, state = arrays[0], arrays[-1], arrays[-2]
    seqs, model_width = tokens.shape
    z_count = lax.axis_size("z")
    part = (z_count, seqs, model_width // (2 * z_count))
    smem, vmem = pl.BlockSpec(memory_space=pltpu.SMEM), pl.BlockSpec(memory_space=pltpu.VMEM)
    return pl.pallas_call(
        front_kernel,
        out_shape=(
            jax.ShapeDtypeStruct(state.shape, F32),
            jax.ShapeDtypeStruct(state.shape, F32),
            jax.ShapeDtypeStruct(part, BF16),
            jax.ShapeDtypeStruct(part, BF16),
        ),
        in_specs=[smem, smem] + [vmem] * len(arrays),
        out_specs=(vmem,) * 4,
        cost_estimate=cost(4 * seqs * model_width * w_out.shape[0], 2 * w_out.size * 2),
        name="front",
    )(core, log_step, *arrays)


def gate_up_kernel(
    at, arrived, gain, gate, gate_par, up, up_par, *refs
):
    *sent, incoming, weights, parcel, ins, outs = refs
    half, _, _, width, _ = weights.shape
    seq_devs, _, pair_slots, _ = incoming.shape
    z_count, _, lanes = parcel.shape
    capacity = pair_slots // half
    rows = seq_devs * capacity
    first = pltpu.make_async_copy(arrived, incoming, ins.at[0])
    first.start()
    loads = {}
    for e in range(half):
        for m, (own, par) in enumerate(((gate, gate_par), (up, up_par))):
            for part, source in enumerate((own.at[half * at[0] + e], par.at[half * at[0] + e])):
                arrival = ins.at[1 + 4 * e + 2 * m + part]
                copy = pltpu.make_async_copy(source, weights.at[e, m, part], arrival)
                copy.start()
                loads[e, m, part] = copy
    ones = jnp.ones((8, width), BF16)
    features = [pl.ds(pl.multiple_of(at[1 + part] * width, width), width) for part in range(2)]
    first.wait()
    stores = []

    def store(source, target):
        copy = pltpu.make_async_copy(source, target, outs.at[len(stores)])
        copy.start()
        stores.append(copy)

    def put(depth, size, block_of):
        for chip in range(z_count):
            steps = lax.rem(chip - at[3] + z_count, z_count)
            parcel[steps, depth : depth + size, :] = block_of(chip)

    scaled = {}
    for e in range(half):
        squares = jnp.zeros((8, rows), F32)
        for part in range(2):
            values = incoming[:, part, e * capacity : (e + 1) * capacity, :]
            values = values.reshape(rows, width).astype(F32)
            scaled[e, part] = (values * gain[:, features[part]]).astype(BF16)
            high, low = two_parts(values * values)
            squares = squares + dot_nt(ones, high) + dot_nt(ones, low)
        high, low = two_parts(squares)
        line = lax.broadcasted_iota(jnp.int32, squares.shape, 0)
        both = jnp.where(line == 0, high.astype(F32), jnp.where(line == 1, low.astype(F32), 0.0))
        depth = 2 * half * rows + e * 8
        put(depth, 8, lambda chip, both=both: both.astype(BF16))
    for e in range(half):
        for m in range(2):
            for part in range(2):
                loads[e, m, part].wait()
            sums = dot32(scaled[e, 0], weights[e, m, 0]) + dot32(scaled[e, 1], weights[e, m, 1])
            sums = sums.astype(BF16)
            depth = (half * m + e) * rows
            put(depth, rows, lambda chip, sums=sums: sums[:, chip * lanes : (chip + 1) * lanes])
    middle, depth = z_count // 2, parcel.shape[1]
    split = depth // 2
    targets = [sent[0], *sent[1:middle], None, *sent[middle:]]
    for steps, target in enumerate(targets):
        if steps in (1, z_count - 1):
            first = 0 if steps == 1 else split
            store(parcel.at[middle, pl.ds(first, split), :], target.at[pl.ds(depth, split), :])
            target = target.at[pl.ds(0, depth), :]
        if steps != middle:
            store(parcel.at[steps], target)
    for copy in stores:
        copy.wait()


def gate_up(at, incoming, gain, gate, gate_par, up, up_par):
    seq_devs, _, pair_slots, width = incoming.shape
    half, units = gate.shape[0] // 2, gate.shape[2]
    z_count = lax.axis_size("z")
    pair_rows = seq_devs * pair_slots
    parcel = (z_count, 2 * pair_rows + half * 8, units // z_count)
    long = parcel[1] + parcel[1] // 2
    smem, vmem = pl.BlockSpec(memory_space=pltpu.SMEM), pl.BlockSpec(memory_space=pltpu.VMEM)
    far, any_place = pl.BlockSpec(memory_space=pltpu.HBM), pl.BlockSpec(memory_space=pl.ANY)
    return pl.pallas_call(
        gate_up_kernel,
        in_specs=[smem, any_place, vmem, far, any_place, far, any_place],
        out_specs=(any_place,) * (z_count - 1),
        out_shape=tuple(
            jax.ShapeDtypeStruct((depth, parcel[2]), BF16)
            for depth in (parcel[1], long, *(parcel[1],) * (z_count - 4), long)
        ),
        scratch_shapes=[
            pltpu.VMEM(incoming.shape, BF16),
            pltpu.VMEM((half, 2, 2, width, units), BF16),
            pltpu.VMEM(parcel, BF16),
            pltpu.SemaphoreType.DMA((1 + 4 * half,)),
            pltpu.SemaphoreType.DMA((z_count + 1,)),
        ],
        compiler_params=pltpu.CompilerParams(vmem_limit_bytes=52 * 2**20),
        cost_estimate=cost(8 * pair_rows * width * units, 8 * half * width * units),
        name="gate_up",
    )(at, incoming, gain, gate, gate_par, up, up_par)


def dispatch_kernel(spread, own_in, par_in, outgoing, own, par, arrivals):
    copies = [
        pltpu.make_async_copy(source, target, arrivals.at[i])
        for i, (source, target) in enumerate(((own_in, own), (par_in, par)))
    ]
    for copy in copies:
        copy.start()
    for copy in copies:
        copy.wait()
    shape = outgoing.shape[:1] + outgoing.shape[2:]
    for part, rows in enumerate((own, par)):
        outgoing[:, part] = dot32(spread[...], rows[...]).astype(BF16).reshape(shape)


def dispatch(spread, own, par, ep_count):
    slots, (_, width) = spread.shape[0], own.shape
    vmem = pl.BlockSpec(memory_space=pltpu.VMEM)
    return pl.pallas_call(
        dispatch_kernel,
        out_shape=jax.ShapeDtypeStruct((ep_count, 2, slots // ep_count, width), BF16),
        in_specs=[vmem, pl.BlockSpec(memory_space=pl.ANY), pl.BlockSpec(memory_space=pl.ANY)],
        out_specs=vmem,
        scratch_shapes=[
            pltpu.VMEM(own.shape, BF16),
            pltpu.VMEM(own.shape, BF16),
            pltpu.SemaphoreType.DMA((2,)),
        ],
        compiler_params=ROOM,
        cost_estimate=cost(4 * spread.size * width, 4 * slots * width),
        name="dispatch",
    )(spread, own, par)


def combine_kernel(weights, arrived, base, *refs):
    *parts, own, given, returned, arrival = refs
    fetch(arrived, returned, arrival)
    high, low = two_parts(weights[...])
    rows, width = weights.shape[1], returned.shape[3]
    for slot, out in enumerate((own, given)):
        values = returned[:, slot].reshape(rows, width)
        total = dot32(high, values) + dot32(low, values)
        if slot == 0:
            total = total + base[...].astype(F32)
        for part in parts:
            if slot < part.shape[0]:
                total = total + part[slot].astype(F32)
        out[...] = total.astype(out.dtype)


def combined(weights, returned, base, parts):
    shape = (weights.shape[0], returned.shape[3])
    vmem = pl.BlockSpec(memory_space=pltpu.VMEM)
    return pl.pallas_call(
        combine_kernel,
        out_shape=(jax.ShapeDtypeStruct(shape, F32), jax.ShapeDtypeStruct(shape, BF16)),
        in_specs=[vmem, pl.BlockSpec(memory_space=pl.ANY)] + [vmem] * (1 + len(parts)),
        out_specs=(vmem, vmem),
        scratch_shapes=[pltpu.VMEM(returned.shape, BF16), pltpu.SemaphoreType.DMA],
        compiler_params=ROOM,
        cost_estimate=cost(8 * weights.size * shape[1], 2 * returned.size),
        name="combine",
    )(weights, returned, base, *parts)


def shared_kernel(at, own, par, mine, theirs, gain, sources, kept, given, *scratch):
    *weights, arrivals = scratch
    copies = [
        pltpu.make_async_copy(source, target, arrivals.at[i])
        for i, (source, target) in enumerate(zip(sources, weights, strict=True))
    ]
    for copy in copies:
        copy.start()
    for copy in copies:
        copy.wait()
    gate_t, up_t, down_t = weights
    c, z = at[0], at[3]
    seqs, width = kept.shape[1:]
    chips = gain.shape[1] // (2 * width)
    way = 1 - 2 * c

    def features(steps, place):
        chip = lax.rem(z + way * steps + 2 * chips, chips)
        return pl.ds(pl.multiple_of((2 * chip + place) * width, width), width)

    squares = jnp.zeros((seqs, 1), F32)
    gate = jnp.zeros((seqs, gate_t.shape[0]), F32)
    up = gate
    rows = [(own[...], features(0, c)), (par[...], features(0, 1 - c))]
    for pieces, first, sign in ((mine, c, -1), (theirs, 1 - c, 1)):
        for k, piece in enumerate(pieces):
            rows.append((piece[0], features(sign * (k + 1), first)))
            if piece.shape[0] > 1:
                rows.append((piece[1], features(sign * (k + 1), 1 - first)))
    for values, place in rows:
        values = values.astype(F32)
        squares = squares + jnp.sum(values * values, axis=-1, keepdims=True)
        scaled = (values * gain[:, place]).astype(BF16)
        gate = gate + dot_nt(scaled, gate_t[:, place])
        up = up + dot_nt(scaled, up_t[:, place])
    factor = lax.rsqrt(squares / gain.shape[1] + EPS)
    gate, up = gate * factor, up * factor
    inner = (gate / (1.0 + jnp.exp(-gate)) * up).astype(BF16)
    for out, first, sign in ((kept, c, 1), (given, 1 - c, -1)):
        order = [(sign * k, place) for k in range(chips // 2 - 1, 0, -1) for place in (first, 1 - first)]
        for i, (steps, place) in enumerate([*order, (chips // 2, first), (0, first)]):
            out[i] = dot32(inner, down_t[:, features(steps, place)]).astype(out.dtype)


def shared_parts(at, own, par, mine, theirs, gain, gate_t, up_t, w_down):
    smem, vmem = pl.BlockSpec(memory_space=pltpu.SMEM), pl.BlockSpec(memory_space=pltpu.VMEM)
    (seqs, width), count = own.shape, len(mine)

    def kernel(at, own, par, *refs):
        first, second, (gain, *rest) = refs[:count], refs[count : 2 * count], refs[2 * count :]
        shared_kernel(at, own, par, first, second, gain, rest[:3], *rest[3:])

    return pl.pallas_call(
        kernel,
        out_shape=(
            jax.ShapeDtypeStruct((2 * count, seqs, width), BF16),
            jax.ShapeDtypeStruct((2 * count, seqs, width), BF16),
        ),
        in_specs=[smem] + [vmem] * (2 * count + 3) + [pl.BlockSpec(memory_space=pl.ANY)] * 3,
        out_specs=(vmem, vmem),
        scratch_shapes=[
            pltpu.VMEM(gate_t.shape, BF16),
            pltpu.VMEM(up_t.shape, BF16),
            pltpu.VMEM(w_down.shape, BF16),
            pltpu.SemaphoreType.DMA((3,)),
        ],
        compiler_params=pltpu.CompilerParams(vmem_limit_bytes=FULL),
        cost_estimate=cost(seqs * 6 * w_down.size, 6 * w_down.size),
        name="shared",
    )(at, own, par, *mine, *theirs, gain, gate_t, up_t, w_down)


def inner_kernel(model_width, half, *refs):
    *arrived, inner, parcels, arrivals = refs
    copies = [
        pltpu.make_async_copy(
            source.at[pl.ds(0, parcels.shape[1]), :], parcels.at[i], arrivals.at[i]
        )
        for i, source in enumerate(arrived)
    ]
    for copy in copies:
        copy.start()
    for copy in copies:
        copy.wait()
    totals = parcels[0].astype(F32)
    for i in range(1, len(copies)):
        totals = totals + parcels[i].astype(F32)
    lanes = totals.shape[1]
    z_count, pair_rows, _ = inner.shape
    rows = pair_rows // half
    for e in range(half):
        line = 2 * pair_rows + 8 * e
        squares = totals[line : line + 1] + totals[line + 1 : line + 2]
        factor = lax.rsqrt(squares / model_width + EPS)
        factor = jnp.broadcast_to(factor, (lanes, rows)).T
        gate = totals[e * rows : (e + 1) * rows] * factor
        up = totals[pair_rows + e * rows : pair_rows + (e + 1) * rows] * factor
        done = (gate / (1.0 + jnp.exp(-gate)) * up).astype(BF16)
        for z in range(z_count):
            inner[z, e * rows : (e + 1) * rows, :] = done


def inner_copies(parcels, z_count, model_width, half):
    depth, lanes = parcels[0].shape
    pair_rows = (depth - half * 8) // 2
    count = len(parcels)
    return pl.pallas_call(
        functools.partial(inner_kernel, model_width, half),
        out_shape=jax.ShapeDtypeStruct((z_count, pair_rows, lanes), BF16),
        in_specs=[pl.BlockSpec(memory_space=pl.ANY)] * count,
        out_specs=pl.BlockSpec(memory_space=pltpu.VMEM),
        scratch_shapes=[
            pltpu.VMEM((count, depth, lanes), BF16),
            pltpu.SemaphoreType.DMA((count,)),
        ],
        compiler_params=ROOM,
        cost_estimate=cost(depth * lanes * 32, depth * lanes * 32),
        name="inner",
    )(*parcels)


def down_kernel(at, arrived, own, par, sent, inner, weights, results, ins, outs):
    half = weights.shape[0]
    first = pltpu.make_async_copy(arrived, inner, ins.at[0])
    first.start()
    loads = []
    for e in range(half):
        for part, source in enumerate((own.at[half * at[0] + e], par.at[half * at[0] + e])):
            arrival = ins.at[1 + 2 * e + part]
            copy = pltpu.make_async_copy(source, weights.at[e, part], arrival)
            copy.start()
            loads.append(copy)
    first.wait()
    rows = inner.shape[1] // half
    seq_devs, _, pair_slots, width = results.shape
    capacity = pair_slots // half
    stores = []
    for e in range(half):
        row = [inner[z, e * rows : (e + 1) * rows, :] for z in range(inner.shape[0])]
        row = jnp.concatenate(row, axis=1)
        place = slice(e * capacity, (e + 1) * capacity)
        for part in range(2):
            loads[2 * e + part].wait()
            out = dot32(row, weights[e, part]).astype(BF16)
            results[:, part, place, :] = out.reshape(seq_devs, capacity, width)
        place = pl.ds(e * capacity, capacity)
        copy = pltpu.make_async_copy(
            results.at[:, :, place, :], sent.at[:, :, place, :], outs.at[e]
        )
        copy.start()
        stores.append(copy)
    for copy in stores:
        copy.wait()


def down(at, inner, w_down, w_par, seq_devs, capacity):
    half, units, width = w_par.shape[0] // 2, *w_par.shape[1:]
    results = (seq_devs, 2, half * capacity, width)
    smem, any_place = pl.BlockSpec(memory_space=pltpu.SMEM), pl.BlockSpec(memory_space=pl.ANY)
    return pl.pallas_call(
        down_kernel,
        in_specs=[smem, any_place, any_place, any_place],
        out_specs=pl.BlockSpec(memory_space=pltpu.HBM),
        out_shape=pltpu.HBM(results, BF16),
        scratch_shapes=[
            pltpu.VMEM(inner.shape, BF16),
            pltpu.VMEM((half, 2, units, width), BF16),
            pltpu.VMEM(results, BF16),
            pltpu.SemaphoreType.DMA((1 + 2 * half,)),
            pltpu.SemaphoreType.DMA((half,)),
        ],
        compiler_params=ROOM,
        cost_estimate=cost(4 * inner.shape[1] * units * width, 4 * half * units * width),
        name="down",
    )(at, inner, w_down, w_par)


def local(
    tokens,
    norm_gain,
    ffn_gain,
    w_in,
    decay_rate,
    frequency,
    log_step,
    input_real,
    input_imag,
    readout_real,
    readout_imag,
    skip_gain,
    state_real,
    state_imag,
    w_out,
    shared_gate,
    shared_up,
    shared_down,
    expert_gate,
    expert_up,
    expert_down,
    routing,
    route_weight,
):
    seq_count, model_width = tokens.shape
    ep_count, z_count = lax.axis_size("ep"), lax.axis_size("z")
    z, c = lax.axis_index("z"), lax.axis_index("c")
    core = c.reshape(1)
    slice_width = model_width // (2 * z_count)
    offset = (2 * z + c) * slice_width

    new_real, new_imag, kept, given = front(
        core,
        log_step,
        tokens,
        norm_gain.reshape(1, -1),
        w_in,
        decay_rate.reshape(1, -1),
        frequency.reshape(1, -1),
        input_real,
        input_imag,
        readout_real,
        readout_imag,
        skip_gain.reshape(1, -1),
        state_real,
        state_imag,
        w_out,
    )
    got = swapped(given)
    both = (kept.astype(F32) + got.astype(F32)).astype(BF16)

    gate_par, up_par, down_par = (swapped(w) for w in (expert_gate, expert_up, expert_down))

    mixer_own = lax.all_to_all(both, "z", split_axis=0, concat_axis=0, tiled=True)
    mixer_own = mixer_own.astype(F32).sum(axis=0)
    own_tokens = lax.dynamic_slice_in_dim(tokens, offset, slice_width, 1)
    resid_own = (own_tokens.astype(F32) + mixer_own).astype(BF16)
    resid_par = swapped(resid_own)

    expert_dev = expert_gate.shape[0]
    half = expert_dev // 2
    top_count = routing.shape[1]
    capacity = 2 * seq_count * top_count // (expert_dev * ep_count)
    slot_count = half * ep_count * capacity
    flat_ids = routing.reshape(-1)
    one_hot = (
        flat_ids[:, None] == jnp.arange(expert_dev * ep_count, dtype=jnp.int32)[None, :]
    ).astype(jnp.int32)
    earlier = jnp.cumsum(one_hot, axis=0) - one_hot
    slot_rank = jnp.sum(earlier * one_hot, axis=1)
    home, within = flat_ids // expert_dev, flat_ids % expert_dev
    target = (home * half + within % half) * capacity + slot_rank
    target = jnp.where(within // half == c, target, -1)
    slot_ids = jnp.arange(slot_count, dtype=jnp.int32)
    placed = (target[None, :] == slot_ids[:, None]).reshape(slot_count, seq_count, top_count)
    spread = jnp.sum(placed.astype(F32), axis=2).astype(BF16)
    outgoing = dispatch(spread, resid_own, resid_par, ep_count)
    incoming = lax.all_to_all(outgoing, "ep", split_axis=0, concat_axis=0, tiled=True)

    at = jnp.array([1, 1, -1, 0], jnp.int32) * c + jnp.array([0, 2, 2, 1], jnp.int32) * z
    at = at + jnp.array([0, 0, 1, 0], jnp.int32)
    gain = ffn_gain.reshape(1, -1)
    sent = gate_up(at, incoming, gain, expert_gate, gate_par, expert_up, up_par)
    middle, depth = z_count // 2, sent[0].shape[0]
    chunks = dict(zip([k for k in range(z_count) if k != middle], sent, strict=True))
    parcels = [chunks[0]]
    for steps in range(1, middle):
        if steps == middle - 1:
            chunks[steps] = added(chunks[steps], parcels[1][depth:], 0)
            chunks[z_count - steps] = added(chunks[z_count - steps], parcels[2][depth:], depth // 2)
        parcels.append(moved(chunks[steps], "z", steps))
        parcels.append(moved(chunks[z_count - steps], "z", -steps))
    copies = inner_copies(parcels, z_count, model_width, half)
    inner_all = lax.all_to_all(copies, "z", split_axis=0, concat_axis=0, tiled=True)
    results = down(at, inner_all, expert_down, down_par, ep_count, capacity)
    returned = lax.all_to_all(results, "ep", split_axis=0, concat_axis=0, tiled=True)

    held = jnp.stack([resid_own, resid_par])
    mine, theirs = [], []
    for steps in range(1, middle + 1):
        if steps < middle:
            mine.append(both_ways(held, steps))
        else:
            mine.append(both_ways(mine[-1][:1], 1))
        theirs.append(swapped(mine[-1]))
    kept, given = shared_parts(
        at,
        resid_own,
        resid_par,
        mine,
        theirs,
        gain,
        shared_gate.T,
        shared_up.T,
        shared_down,
    )
    got = swapped(given)
    leaving = (kept.astype(F32) + got.astype(F32)).astype(BF16)
    shared_chip = []
    for steps in range(1, middle + 1):
        first = 2 * (middle - 1 - steps) if steps < middle else 2 * (middle - 1)
        part = leaving[first : first + (2 if steps < middle else 1)]
        shared_chip.append(both_ways(part, steps))

    weights = route_weight / jnp.sum(route_weight, axis=1, keepdims=True) * ROUTED_SCALE
    chosen = target.reshape(seq_count, top_count)[:, :, None] == slot_ids[None, None, :]
    combine = jnp.sum(jnp.where(chosen, weights[:, :, None], 0.0), axis=1)
    own, given = combined(combine, returned, leaving[-1], shared_chip)
    got = swapped(given)
    mixed = (resid_own.astype(F32) + own + got.astype(F32)).astype(BF16)
    return (mixed, new_real, new_imag)


def solution(mesh):
    ep_count, tp_count = mesh.devices.shape
    cores = Mesh(mesh.devices.reshape(ep_count, tp_count // 2, 2), ("ep", "z", "c"))
    placed = (
        P("ep", None),
        P(),
        P(),
        P(None, TP),
        P(TP),
        P(TP),
        P(TP),
        P(None, TP),
        P(None, TP),
        P(None, TP),
        P(None, TP),
        P(TP),
        P("ep", TP),
        P("ep", TP),
        P(TP, None),
        P(None, TP),
        P(None, TP),
        P(TP, None),
        P("ep", TP, None),
        P("ep", TP, None),
        P("ep", None, TP),
        P("ep", None),
        P("ep", None),
    )

    def step(*arrays):
        return local(*arrays)

    step = jax.shard_map(
        step,
        mesh=cores,
        in_specs=placed,
        out_specs=(P("ep", TP), P("ep", TP), P("ep", TP)),
        check_vma=False,
    )
    return step
```

```python
import functools

import jax
import jax.numpy as jnp
from jax import lax
from jax.experimental import pallas as pl
from jax.experimental.pallas import tpu as pltpu
from jax.sharding import Mesh
from jax.sharding import PartitionSpec as P


EPS = 1e-06
ROUTED_SCALE = 2.5
TP = ("z", "c")
F32, BF16 = jnp.float32, jnp.bfloat16
FULL = 53 * 2**20
ROOM = pltpu.CompilerParams(vmem_limit_bytes=20 * 2**20)


def swapped(x):
    return lax.ppermute(x, "c", [(0, 1), (1, 0)])


def moved(x, axis, steps):
    count = lax.axis_size(axis)
    return lax.ppermute(x, axis, [(i, (i + steps) % count) for i in range(count)])


def both_ways(x, steps):
    count = lax.axis_size("z")
    ups = [(2 * i, 2 * ((i + steps) % count)) for i in range(count)]
    downs = [(2 * i + 1, 2 * ((i - steps) % count) + 1) for i in range(count)]
    return lax.ppermute(x, TP, ups + downs)


def ring_sums(kept, got):
    sums = (kept.astype(F32) + got.astype(F32)).astype(BF16)
    middle, arrived = kept.shape[0] // 2, []
    for steps in range(1, middle + 1):
        first, count = (2 * (middle - 1 - steps), 2) if steps < middle else (2 * (middle - 1), 1)
        arrived.append(both_ways(sums[first : first + count], steps))
    return sums[-1], arrived


def added(x, part, first):
    rest = x.shape[0] - first - part.shape[0]
    part = lax.pad(part.astype(F32), jnp.zeros((), F32), ((first, rest, 0), (0, 0, 0)))
    return (x.astype(F32) + part).astype(BF16)


def rms_scale(values_in, gains):
    values = values_in.astype(F32)
    factor = lax.rsqrt(jnp.mean(values * values, axis=-1, keepdims=True) + EPS)
    return (values * factor * gains).astype(BF16)


def dot32(a, b):
    return jnp.dot(a, b, preferred_element_type=F32)


def dot_nt(a, b):
    return lax.dot_general(a, b, (((1,), (1,)), ((), ())), preferred_element_type=F32)


def two_parts(x):
    high = x.astype(BF16)
    return high, (x - high.astype(F32)).astype(BF16)


def cost(flops, moved):
    return pl.CostEstimate(flops=flops, bytes_accessed=moved, transcendentals=0)


def fetch(source, target, arrival):
    copy = pltpu.make_async_copy(source, target, arrival)
    copy.start()
    copy.wait()


def along_ring(z, c, chips, width):
    way = 1 - 2 * c

    def features(steps, place):
        chip = lax.rem(z + way * steps + 2 * chips, chips)
        return pl.ds(pl.multiple_of((2 * chip + place) * width, width), width)

    return features


def ring_order(chips, first, sign):
    order = [(sign * k, at) for k in range(chips // 2 - 1, 0, -1) for at in (first, 1 - first)]
    return [*order, (chips // 2, first), (0, first)]


def front_kernel(
    core,
    chip,
    log_step,
    tokens,
    norm_gain,
    w_in,
    decay_rate,
    frequency,
    input_real,
    input_imag,
    readout_real,
    readout_imag,
    skip_gain,
    state_real,
    state_imag,
    w_out,
    new_real,
    new_imag,
    kept,
    given,
):
    groups = log_step.shape[0]
    chan_count, entries = input_real.shape
    channels = skip_gain.shape[1]
    width = entries // groups
    normed = rms_scale(tokens[...], norm_gain[...])
    drive = dot32(normed, w_in[...]).astype(BF16)
    group_of = lax.broadcasted_iota(jnp.int32, (1, entries), 1) // width
    step_size = jnp.zeros((1, entries), F32)
    for g in range(groups):
        step_size = jnp.where(group_of == g, log_step[g], step_size)
    step_size = jnp.exp(step_size)
    decays, omegas = decay_rate[...], frequency[...]
    pole_mag = jnp.exp(-decays * step_size)
    pole_angle = omegas * step_size
    pole_re = pole_mag * jnp.cos(pole_angle)
    pole_im = pole_mag * jnp.sin(pole_angle)
    pole_norm = decays * decays + omegas * omegas
    diff_re = pole_re - 1.0
    lift_re = (-decays * diff_re + omegas * pole_im) / pole_norm
    lift_im = (-decays * pole_im - omegas * diff_re) / pole_norm
    row_group = lax.broadcasted_iota(jnp.int32, (channels, entries), 0) // chan_count
    col_group = lax.broadcasted_iota(jnp.int32, (channels, entries), 1) // width
    same = row_group == col_group

    def spread(block):
        return two_parts(jnp.where(same, jnp.concatenate([block[...]] * groups, axis=0), 0.0))

    def push_of(block):
        high, low = spread(block)
        return dot32(drive, high) + dot32(drive, low)

    push_re, push_im = push_of(input_real), push_of(input_imag)
    old_re, old_im = state_real[...], state_imag[...]
    new_re = pole_re * old_re - pole_im * old_im + lift_re * push_re - lift_im * push_im
    new_im = pole_re * old_im + pole_im * old_re + lift_re * push_im + lift_im * push_re
    new_real[...] = new_re
    new_imag[...] = new_im

    def read_of(state, block):
        (high, low), (block_high, block_low) = two_parts(state), spread(block)
        return dot_nt(high, block_high) + dot_nt(high, block_low) + dot_nt(low, block_high)

    read = read_of(new_re, readout_real) - read_of(new_im, readout_imag)
    read = read + skip_gain[...] * drive.astype(F32)
    bent = jnp.tanh(0.7978845608028654 * (read + 0.044715 * (read * read * read)))
    activated = (0.5 * read * (1.0 + bent)).astype(BF16)
    c, chips = core[0], kept.shape[0]
    features = along_ring(chip[0], c, chips, kept.shape[2])
    for out, first, sign in ((kept, c, 1), (given, 1 - c, -1)):
        for i, place in enumerate(ring_order(chips, first, sign)):
            out[i] = dot32(activated, w_out[:, features(*place)]).astype(out.dtype)


def front(core, chip, log_step, *arrays):
    tokens, w_out, state = arrays[0], arrays[-1], arrays[-2]
    seqs, model_width = tokens.shape
    z_count = lax.axis_size("z")
    part = (z_count, seqs, model_width // (2 * z_count))
    smem, vmem = pl.BlockSpec(memory_space=pltpu.SMEM), pl.BlockSpec(memory_space=pltpu.VMEM)
    return pl.pallas_call(
        front_kernel,
        out_shape=(
            jax.ShapeDtypeStruct(state.shape, F32),
            jax.ShapeDtypeStruct(state.shape, F32),
            jax.ShapeDtypeStruct(part, BF16),
            jax.ShapeDtypeStruct(part, BF16),
        ),
        in_specs=[smem] * 3 + [vmem] * len(arrays),
        out_specs=(vmem,) * 4,
        cost_estimate=cost(4 * seqs * model_width * w_out.shape[0], 2 * w_out.size * 2),
        name="front",
    )(core, chip, log_step, *arrays)


def gate_up_kernel(
    at, arrived, gain, gate, gate_par, up, up_par, *refs
):
    *sent, incoming, weights, parcel, ins, outs = refs
    half, _, _, width, _ = weights.shape
    seq_devs, _, pair_slots, _ = incoming.shape
    z_count, _, lanes = parcel.shape
    capacity = pair_slots // half
    rows = seq_devs * capacity
    first = pltpu.make_async_copy(arrived, incoming, ins.at[0])
    first.start()
    loads = {}
    for e in range(half):
        for m, (own, par) in enumerate(((gate, gate_par), (up, up_par))):
            for part, source in enumerate((own.at[half * at[0] + e], par.at[half * at[0] + e])):
                arrival = ins.at[1 + 4 * e + 2 * m + part]
                copy = pltpu.make_async_copy(source, weights.at[e, m, part], arrival)
                copy.start()
                loads[e, m, part] = copy
    ones = jnp.ones((8, width), BF16)
    features = [pl.ds(pl.multiple_of(at[1 + part] * width, width), width) for part in range(2)]
    first.wait()
    stores = []

    def store(source, target):
        copy = pltpu.make_async_copy(source, target, outs.at[len(stores)])
        copy.start()
        stores.append(copy)

    def put(depth, size, block_of):
        for chip in range(z_count):
            steps = lax.rem(chip - at[3] + z_count, z_count)
            parcel[steps, depth : depth + size, :] = block_of(chip)

    scaled = {}
    for e in range(half):
        squares = jnp.zeros((8, rows), F32)
        for part in range(2):
            values = incoming[:, part, e * capacity : (e + 1) * capacity, :]
            values = values.reshape(rows, width).astype(F32)
            scaled[e, part] = (values * gain[:, features[part]]).astype(BF16)
            high, low = two_parts(values * values)
            squares = squares + dot_nt(ones, high) + dot_nt(ones, low)
        high, low = two_parts(squares)
        line = lax.broadcasted_iota(jnp.int32, squares.shape, 0)
        both = jnp.where(line == 0, high.astype(F32), jnp.where(line == 1, low.astype(F32), 0.0))
        depth = 2 * half * rows + e * 8
        put(depth, 8, lambda chip, both=both: both.astype(BF16))
    for e in range(half):
        for m in range(2):
            for part in range(2):
                loads[e, m, part].wait()
            sums = dot32(scaled[e, 0], weights[e, m, 0]) + dot32(scaled[e, 1], weights[e, m, 1])
            sums = sums.astype(BF16)
            depth = (half * m + e) * rows
            put(depth, rows, lambda chip, sums=sums: sums[:, chip * lanes : (chip + 1) * lanes])
    middle, depth = z_count // 2, parcel.shape[1]
    split = depth // 2
    targets = [sent[0], *sent[1:middle], None, *sent[middle:]]
    for steps, target in enumerate(targets):
        if steps in (1, z_count - 1):
            first = 0 if steps == 1 else split
            store(parcel.at[middle, pl.ds(first, split), :], target.at[pl.ds(depth, split), :])
            target = target.at[pl.ds(0, depth), :]
        if steps != middle:
            store(parcel.at[steps], target)
    for copy in stores:
        copy.wait()


def gate_up(at, incoming, gain, gate, gate_par, up, up_par):
    seq_devs, _, pair_slots, width = incoming.shape
    half, units = gate.shape[0] // 2, gate.shape[2]
    z_count = lax.axis_size("z")
    pair_rows = seq_devs * pair_slots
    parcel = (z_count, 2 * pair_rows + half * 8, units // z_count)
    long = parcel[1] + parcel[1] // 2
    smem, vmem = pl.BlockSpec(memory_space=pltpu.SMEM), pl.BlockSpec(memory_space=pltpu.VMEM)
    far, any_place = pl.BlockSpec(memory_space=pltpu.HBM), pl.BlockSpec(memory_space=pl.ANY)
    return pl.pallas_call(
        gate_up_kernel,
        in_specs=[smem, any_place, vmem, far, any_place, far, any_place],
        out_specs=(any_place,) * (z_count - 1),
        out_shape=tuple(
            jax.ShapeDtypeStruct((depth, parcel[2]), BF16)
            for depth in (parcel[1], long, *(parcel[1],) * (z_count - 4), long)
        ),
        scratch_shapes=[
            pltpu.VMEM(incoming.shape, BF16),
            pltpu.VMEM((half, 2, 2, width, units), BF16),
            pltpu.VMEM(parcel, BF16),
            pltpu.SemaphoreType.DMA((1 + 4 * half,)),
            pltpu.SemaphoreType.DMA((z_count + 1,)),
        ],
        compiler_params=pltpu.CompilerParams(vmem_limit_bytes=52 * 2**20),
        cost_estimate=cost(8 * pair_rows * width * units, 8 * half * width * units),
        name="gate_up",
    )(at, incoming, gain, gate, gate_par, up, up_par)


def dispatch_kernel(spread, own_in, par_in, outgoing, own, par, arrivals):
    copies = [
        pltpu.make_async_copy(source, target, arrivals.at[i])
        for i, (source, target) in enumerate(((own_in, own), (par_in, par)))
    ]
    for copy in copies:
        copy.start()
    for copy in copies:
        copy.wait()
    shape = outgoing.shape[:1] + outgoing.shape[2:]
    for part, rows in enumerate((own, par)):
        outgoing[:, part] = dot32(spread[...], rows[...]).astype(BF16).reshape(shape)


def dispatch(spread, own, par, ep_count):
    slots, (_, width) = spread.shape[0], own.shape
    vmem = pl.BlockSpec(memory_space=pltpu.VMEM)
    return pl.pallas_call(
        dispatch_kernel,
        out_shape=jax.ShapeDtypeStruct((ep_count, 2, slots // ep_count, width), BF16),
        in_specs=[vmem, pl.BlockSpec(memory_space=pl.ANY), pl.BlockSpec(memory_space=pl.ANY)],
        out_specs=vmem,
        scratch_shapes=[
            pltpu.VMEM(own.shape, BF16),
            pltpu.VMEM(own.shape, BF16),
            pltpu.SemaphoreType.DMA((2,)),
        ],
        compiler_params=ROOM,
        cost_estimate=cost(4 * spread.size * width, 4 * slots * width),
        name="dispatch",
    )(spread, own, par)


def combine_kernel(weights, arrived, base, *refs):
    *parts, own, given, returned, arrival = refs
    fetch(arrived, returned, arrival)
    high, low = two_parts(weights[...])
    rows, width = weights.shape[1], returned.shape[3]
    for slot, out in enumerate((own, given)):
        values = returned[:, slot].reshape(rows, width)
        total = dot32(high, values) + dot32(low, values)
        if slot == 0:
            total = total + base[...].astype(F32)
        for part in parts:
            if slot < part.shape[0]:
                total = total + part[slot].astype(F32)
        out[...] = total.astype(out.dtype)


def combined(weights, returned, base, parts):
    shape = (weights.shape[0], returned.shape[3])
    vmem = pl.BlockSpec(memory_space=pltpu.VMEM)
    return pl.pallas_call(
        combine_kernel,
        out_shape=(jax.ShapeDtypeStruct(shape, F32), jax.ShapeDtypeStruct(shape, BF16)),
        in_specs=[vmem, pl.BlockSpec(memory_space=pl.ANY)] + [vmem] * (1 + len(parts)),
        out_specs=(vmem, vmem),
        scratch_shapes=[pltpu.VMEM(returned.shape, BF16), pltpu.SemaphoreType.DMA],
        compiler_params=ROOM,
        cost_estimate=cost(8 * weights.size * shape[1], 2 * returned.size),
        name="combine",
    )(weights, returned, base, *parts)


def shared_kernel(at, own, par, mine, theirs, gain, sources, kept, given, *scratch):
    *weights, arrivals = scratch
    copies = [
        pltpu.make_async_copy(source, target, arrivals.at[i])
        for i, (source, target) in enumerate(zip(sources, weights, strict=True))
    ]
    for copy in copies:
        copy.start()
    for copy in copies:
        copy.wait()
    gate_t, up_t, down_t = weights
    c, z = at[0], at[3]
    seqs, width = kept.shape[1:]
    chips = gain.shape[1] // (2 * width)
    features = along_ring(z, c, chips, width)
    squares = jnp.zeros((seqs, 1), F32)
    gate = jnp.zeros((seqs, gate_t.shape[0]), F32)
    up = gate
    rows = [(own[...], features(0, c)), (par[...], features(0, 1 - c))]
    for pieces, first, sign in ((mine, c, -1), (theirs, 1 - c, 1)):
        for k, piece in enumerate(pieces):
            rows.append((piece[0], features(sign * (k + 1), first)))
            if piece.shape[0] > 1:
                rows.append((piece[1], features(sign * (k + 1), 1 - first)))
    for values, place in rows:
        values = values.astype(F32)
        squares = squares + jnp.sum(values * values, axis=-1, keepdims=True)
        scaled = (values * gain[:, place]).astype(BF16)
        gate = gate + dot_nt(scaled, gate_t[:, place])
        up = up + dot_nt(scaled, up_t[:, place])
    factor = lax.rsqrt(squares / gain.shape[1] + EPS)
    gate, up = gate * factor, up * factor
    inner = (gate / (1.0 + jnp.exp(-gate)) * up).astype(BF16)
    for out, first, sign in ((kept, c, 1), (given, 1 - c, -1)):
        for i, place in enumerate(ring_order(chips, first, sign)):
            out[i] = dot32(inner, down_t[:, features(*place)]).astype(out.dtype)


def shared_parts(at, own, par, mine, theirs, gain, gate_t, up_t, w_down):
    smem, vmem = pl.BlockSpec(memory_space=pltpu.SMEM), pl.BlockSpec(memory_space=pltpu.VMEM)
    (seqs, width), count = own.shape, len(mine)

    def kernel(at, own, par, *refs):
        first, second, (gain, *rest) = refs[:count], refs[count : 2 * count], refs[2 * count :]
        shared_kernel(at, own, par, first, second, gain, rest[:3], *rest[3:])

    return pl.pallas_call(
        kernel,
        out_shape=(
            jax.ShapeDtypeStruct((2 * count, seqs, width), BF16),
            jax.ShapeDtypeStruct((2 * count, seqs, width), BF16),
        ),
        in_specs=[smem] + [vmem] * (2 * count + 3) + [pl.BlockSpec(memory_space=pl.ANY)] * 3,
        out_specs=(vmem, vmem),
        scratch_shapes=[
            pltpu.VMEM(gate_t.shape, BF16),
            pltpu.VMEM(up_t.shape, BF16),
            pltpu.VMEM(w_down.shape, BF16),
            pltpu.SemaphoreType.DMA((3,)),
        ],
        compiler_params=pltpu.CompilerParams(vmem_limit_bytes=FULL),
        cost_estimate=cost(seqs * 6 * w_down.size, 6 * w_down.size),
        name="shared",
    )(at, own, par, *mine, *theirs, gain, gate_t, up_t, w_down)


def inner_kernel(model_width, half, *refs):
    *arrived, inner, parcels, arrivals = refs
    copies = [
        pltpu.make_async_copy(
            source.at[pl.ds(0, parcels.shape[1]), :], parcels.at[i], arrivals.at[i]
        )
        for i, source in enumerate(arrived)
    ]
    for copy in copies:
        copy.start()
    for copy in copies:
        copy.wait()
    totals = parcels[0].astype(F32)
    for i in range(1, len(copies)):
        totals = totals + parcels[i].astype(F32)
    lanes = totals.shape[1]
    z_count, pair_rows, _ = inner.shape
    rows = pair_rows // half
    for e in range(half):
        line = 2 * pair_rows + 8 * e
        squares = totals[line : line + 1] + totals[line + 1 : line + 2]
        factor = lax.rsqrt(squares / model_width + EPS)
        factor = jnp.broadcast_to(factor, (lanes, rows)).T
        gate = totals[e * rows : (e + 1) * rows] * factor
        up = totals[pair_rows + e * rows : pair_rows + (e + 1) * rows] * factor
        done = (gate / (1.0 + jnp.exp(-gate)) * up).astype(BF16)
        for z in range(z_count):
            inner[z, e * rows : (e + 1) * rows, :] = done


def inner_copies(parcels, z_count, model_width, half):
    depth, lanes = parcels[0].shape
    pair_rows = (depth - half * 8) // 2
    count = len(parcels)
    return pl.pallas_call(
        functools.partial(inner_kernel, model_width, half),
        out_shape=jax.ShapeDtypeStruct((z_count, pair_rows, lanes), BF16),
        in_specs=[pl.BlockSpec(memory_space=pl.ANY)] * count,
        out_specs=pl.BlockSpec(memory_space=pltpu.VMEM),
        scratch_shapes=[
            pltpu.VMEM((count, depth, lanes), BF16),
            pltpu.SemaphoreType.DMA((count,)),
        ],
        compiler_params=ROOM,
        cost_estimate=cost(depth * lanes * 32, depth * lanes * 32),
        name="inner",
    )(*parcels)


def down_kernel(at, arrived, own, par, sent, inner, weights, results, ins, outs):
    half = weights.shape[0]
    first = pltpu.make_async_copy(arrived, inner, ins.at[0])
    first.start()
    loads = []
    for e in range(half):
        for part, source in enumerate((own.at[half * at[0] + e], par.at[half * at[0] + e])):
            arrival = ins.at[1 + 2 * e + part]
            copy = pltpu.make_async_copy(source, weights.at[e, part], arrival)
            copy.start()
            loads.append(copy)
    first.wait()
    rows = inner.shape[1] // half
    seq_devs, _, pair_slots, width = results.shape
    capacity = pair_slots // half
    stores = []
    for e in range(half):
        row = [inner[z, e * rows : (e + 1) * rows, :] for z in range(inner.shape[0])]
        row = jnp.concatenate(row, axis=1)
        place = slice(e * capacity, (e + 1) * capacity)
        for part in range(2):
            loads[2 * e + part].wait()
            out = dot32(row, weights[e, part]).astype(BF16)
            results[:, part, place, :] = out.reshape(seq_devs, capacity, width)
        place = pl.ds(e * capacity, capacity)
        copy = pltpu.make_async_copy(
            results.at[:, :, place, :], sent.at[:, :, place, :], outs.at[e]
        )
        copy.start()
        stores.append(copy)
    for copy in stores:
        copy.wait()


def down(at, inner, w_down, w_par, seq_devs, capacity):
    half, units, width = w_par.shape[0] // 2, *w_par.shape[1:]
    results = (seq_devs, 2, half * capacity, width)
    smem, any_place = pl.BlockSpec(memory_space=pltpu.SMEM), pl.BlockSpec(memory_space=pl.ANY)
    return pl.pallas_call(
        down_kernel,
        in_specs=[smem, any_place, any_place, any_place],
        out_specs=pl.BlockSpec(memory_space=pltpu.HBM),
        out_shape=pltpu.HBM(results, BF16),
        scratch_shapes=[
            pltpu.VMEM(inner.shape, BF16),
            pltpu.VMEM((half, 2, units, width), BF16),
            pltpu.VMEM(results, BF16),
            pltpu.SemaphoreType.DMA((1 + 2 * half,)),
            pltpu.SemaphoreType.DMA((half,)),
        ],
        compiler_params=ROOM,
        cost_estimate=cost(4 * inner.shape[1] * units * width, 4 * half * units * width),
        name="down",
    )(at, inner, w_down, w_par)


def local(
    tokens,
    norm_gain,
    ffn_gain,
    w_in,
    decay_rate,
    frequency,
    log_step,
    input_real,
    input_imag,
    readout_real,
    readout_imag,
    skip_gain,
    state_real,
    state_imag,
    w_out,
    shared_gate,
    shared_up,
    shared_down,
    expert_gate,
    expert_up,
    expert_down,
    routing,
    route_weight,
):
    seq_count, model_width = tokens.shape
    ep_count, z_count = lax.axis_size("ep"), lax.axis_size("z")
    z, c = lax.axis_index("z"), lax.axis_index("c")
    slice_width = model_width // (2 * z_count)
    offset = (2 * z + c) * slice_width
    other_offset = (2 * z + 1 - c) * slice_width

    new_real, new_imag, kept, given = front(
        c.reshape(1),
        z.reshape(1),
        log_step,
        tokens,
        norm_gain.reshape(1, -1),
        w_in,
        decay_rate.reshape(1, -1),
        frequency.reshape(1, -1),
        input_real,
        input_imag,
        readout_real,
        readout_imag,
        skip_gain.reshape(1, -1),
        state_real,
        state_imag,
        w_out,
    )
    got = swapped(given)
    own_part, parts = ring_sums(kept, got)

    gate_par, up_par, down_par = (swapped(w) for w in (expert_gate, expert_up, expert_down))

    own_sum = own_part.astype(F32) + sum(part[0].astype(F32) for part in parts)
    other_sum = sum(part[1].astype(F32) for part in parts if part.shape[0] > 1)
    got = swapped(jnp.stack([own_sum, other_sum]).astype(BF16)).astype(F32)
    own_tokens = lax.dynamic_slice_in_dim(tokens, offset, slice_width, 1)
    other_tokens = lax.dynamic_slice_in_dim(tokens, other_offset, slice_width, 1)
    resid_own = (own_tokens.astype(F32) + (own_sum + got[1])).astype(BF16)
    resid_par = (other_tokens.astype(F32) + (other_sum + got[0])).astype(BF16)

    expert_dev = expert_gate.shape[0]
    half = expert_dev // 2
    top_count = routing.shape[1]
    capacity = 2 * seq_count * top_count // (expert_dev * ep_count)
    slot_count = half * ep_count * capacity
    flat_ids = routing.reshape(-1)
    one_hot = (
        flat_ids[:, None] == jnp.arange(expert_dev * ep_count, dtype=jnp.int32)[None, :]
    ).astype(jnp.int32)
    earlier = jnp.cumsum(one_hot, axis=0) - one_hot
    slot_rank = jnp.sum(earlier * one_hot, axis=1)
    home, within = flat_ids // expert_dev, flat_ids % expert_dev
    target = (home * half + within % half) * capacity + slot_rank
    target = jnp.where(within // half == c, target, -1)
    slot_ids = jnp.arange(slot_count, dtype=jnp.int32)
    placed = (target[None, :] == slot_ids[:, None]).reshape(slot_count, seq_count, top_count)
    spread = jnp.sum(placed.astype(F32), axis=2).astype(BF16)
    outgoing = dispatch(spread, resid_own, resid_par, ep_count)
    incoming = lax.all_to_all(outgoing, "ep", split_axis=0, concat_axis=0, tiled=True)

    at = jnp.array([1, 1, -1, 0], jnp.int32) * c + jnp.array([0, 2, 2, 1], jnp.int32) * z
    at = at + jnp.array([0, 0, 1, 0], jnp.int32)
    gain = ffn_gain.reshape(1, -1)
    sent = gate_up(at, incoming, gain, expert_gate, gate_par, expert_up, up_par)
    middle, depth = z_count // 2, sent[0].shape[0]
    chunks = dict(zip([k for k in range(z_count) if k != middle], sent, strict=True))
    parcels = [chunks[0]]
    for steps in range(1, middle):
        if steps == middle - 1:
            chunks[steps] = added(chunks[steps], parcels[1][depth:], 0)
            chunks[z_count - steps] = added(chunks[z_count - steps], parcels[2][depth:], depth // 2)
        parcels.append(moved(chunks[steps], "z", steps))
        parcels.append(moved(chunks[z_count - steps], "z", -steps))
    copies = inner_copies(parcels, z_count, model_width, half)
    inner_all = lax.all_to_all(copies, "z", split_axis=0, concat_axis=0, tiled=True)
    results = down(at, inner_all, expert_down, down_par, ep_count, capacity)
    returned = lax.all_to_all(results, "ep", split_axis=0, concat_axis=0, tiled=True)

    held = jnp.stack([resid_own, resid_par])
    mine, theirs = [], []
    for steps in range(1, middle + 1):
        if steps < middle:
            mine.append(both_ways(held, steps))
        else:
            mine.append(both_ways(mine[-1][:1], 1))
        theirs.append(swapped(mine[-1]))
    kept, given = shared_parts(
        at,
        resid_own,
        resid_par,
        mine,
        theirs,
        gain,
        shared_gate.T,
        shared_up.T,
        shared_down,
    )
    got = swapped(given)
    own_part, shared_chip = ring_sums(kept, got)

    weights = route_weight / jnp.sum(route_weight, axis=1, keepdims=True) * ROUTED_SCALE
    chosen = target.reshape(seq_count, top_count)[:, :, None] == slot_ids[None, None, :]
    combine = jnp.sum(jnp.where(chosen, weights[:, :, None], 0.0), axis=1)
    own, given = combined(combine, returned, own_part, shared_chip)
    got = swapped(given)
    mixed = (resid_own.astype(F32) + own + got.astype(F32)).astype(BF16)
    return (mixed, new_real, new_imag)


def solution(mesh):
    ep_count, tp_count = mesh.devices.shape
    cores = Mesh(mesh.devices.reshape(ep_count, tp_count // 2, 2), ("ep", "z", "c"))
    placed = (
        P("ep", None),
        P(),
        P(),
        P(None, TP),
        P(TP),
        P(TP),
        P(TP),
        P(None, TP),
        P(None, TP),
        P(None, TP),
        P(None, TP),
        P(TP),
        P("ep", TP),
        P("ep", TP),
        P(TP, None),
        P(None, TP),
        P(None, TP),
        P(TP, None),
        P("ep", TP, None),
        P("ep", TP, None),
        P("ep", None, TP),
        P("ep", None),
        P("ep", None),
    )

    def step(*arrays):
        return local(*arrays)

    step = jax.shard_map(
        step,
        mesh=cores,
        in_specs=placed,
        out_specs=(P("ep", TP), P("ep", TP), P("ep", TP)),
        check_vma=False,
    )
    return step
```

```python
import functools

import jax
import jax.numpy as jnp
from jax import lax
from jax.experimental import pallas as pl
from jax.experimental.pallas import tpu as pltpu
from jax.sharding import Mesh
from jax.sharding import PartitionSpec as P


EPS = 1e-06
ROUTED_SCALE = 2.5
TP = ("z", "c")
F32, BF16 = jnp.float32, jnp.bfloat16
FULL = 53 * 2**20
ROOM = pltpu.CompilerParams(vmem_limit_bytes=20 * 2**20)


def swapped(x):
    return lax.ppermute(x, "c", [(0, 1), (1, 0)])


def moved(x, axis, steps):
    count = lax.axis_size(axis)
    return lax.ppermute(x, axis, [(i, (i + steps) % count) for i in range(count)])


def both_ways(x, steps):
    count = lax.axis_size("z")
    ups = [(2 * i, 2 * ((i + steps) % count)) for i in range(count)]
    downs = [(2 * i + 1, 2 * ((i - steps) % count) + 1) for i in range(count)]
    return lax.ppermute(x, TP, ups + downs)


def ring_sums(kept, got):
    sums = (kept.astype(F32) + got.astype(F32)).astype(BF16)
    middle, arrived = kept.shape[0] // 2, []
    for steps in range(1, middle + 1):
        first, count = (2 * (middle - 1 - steps), 2) if steps < middle else (2 * (middle - 1), 1)
        arrived.append(both_ways(sums[first : first + count], steps))
    return sums[-1], arrived


def added(x, part, first):
    rest = x.shape[0] - first - part.shape[0]
    part = lax.pad(part.astype(F32), jnp.zeros((), F32), ((first, rest, 0), (0, 0, 0)))
    return (x.astype(F32) + part).astype(BF16)


def rms_scale(values_in, gains):
    values = values_in.astype(F32)
    factor = lax.rsqrt(jnp.mean(values * values, axis=-1, keepdims=True) + EPS)
    return (values * factor * gains).astype(BF16)


def dot32(a, b):
    return jnp.dot(a, b, preferred_element_type=F32)


def dot_nt(a, b):
    return lax.dot_general(a, b, (((1,), (1,)), ((), ())), preferred_element_type=F32)


def two_parts(x):
    high = x.astype(BF16)
    return high, (x - high.astype(F32)).astype(BF16)


def cost(flops, moved):
    return pl.CostEstimate(flops=flops, bytes_accessed=moved, transcendentals=0)


def fetch(source, target, arrival):
    copy = pltpu.make_async_copy(source, target, arrival)
    copy.start()
    copy.wait()


def along_ring(z, c, chips, width):
    way = 1 - 2 * c

    def features(steps, place):
        chip = lax.rem(z + way * steps + 2 * chips, chips)
        return pl.ds(pl.multiple_of((2 * chip + place) * width, width), width)

    return features


def ring_order(chips, first, sign):
    order = [(sign * k, at) for k in range(chips // 2 - 1, 0, -1) for at in (first, 1 - first)]
    return [*order, (chips // 2, first), (0, first)]


def front_kernel(
    core,
    chip,
    log_step,
    tokens,
    norm_gain,
    w_in,
    decay_rate,
    frequency,
    input_real,
    input_imag,
    readout_real,
    readout_imag,
    skip_gain,
    state_real,
    state_imag,
    w_out,
    new_real,
    new_imag,
    kept,
    given,
):
    groups = log_step.shape[0]
    chan_count, entries = input_real.shape
    channels = skip_gain.shape[1]
    width = entries // groups
    normed = rms_scale(tokens[...], norm_gain[...])
    drive = dot32(normed, w_in[...]).astype(BF16)
    group_of = lax.broadcasted_iota(jnp.int32, (1, entries), 1) // width
    step_size = jnp.zeros((1, entries), F32)
    for g in range(groups):
        step_size = jnp.where(group_of == g, log_step[g], step_size)
    step_size = jnp.exp(step_size)
    decays, omegas = decay_rate[...], frequency[...]
    pole_mag = jnp.exp(-decays * step_size)
    pole_angle = omegas * step_size
    pole_re = pole_mag * jnp.cos(pole_angle)
    pole_im = pole_mag * jnp.sin(pole_angle)
    pole_norm = decays * decays + omegas * omegas
    diff_re = pole_re - 1.0
    lift_re = (-decays * diff_re + omegas * pole_im) / pole_norm
    lift_im = (-decays * pole_im - omegas * diff_re) / pole_norm
    row_group = lax.broadcasted_iota(jnp.int32, (channels, entries), 0) // chan_count
    col_group = lax.broadcasted_iota(jnp.int32, (channels, entries), 1) // width
    same = row_group == col_group

    def spread(block):
        return two_parts(jnp.where(same, jnp.concatenate([block[...]] * groups, axis=0), 0.0))

    def push_of(block):
        high, low = spread(block)
        return dot32(drive, high) + dot32(drive, low)

    push_re, push_im = push_of(input_real), push_of(input_imag)
    old_re, old_im = state_real[...], state_imag[...]
    new_re = pole_re * old_re - pole_im * old_im + lift_re * push_re - lift_im * push_im
    new_im = pole_re * old_im + pole_im * old_re + lift_re * push_im + lift_im * push_re
    new_real[...] = new_re
    new_imag[...] = new_im

    def read_of(state, block):
        (high, low), (block_high, block_low) = two_parts(state), spread(block)
        return dot_nt(high, block_high) + dot_nt(high, block_low) + dot_nt(low, block_high)

    read = read_of(new_re, readout_real) - read_of(new_im, readout_imag)
    read = read + skip_gain[...] * drive.astype(F32)
    bent = jnp.tanh(0.7978845608028654 * (read + 0.044715 * (read * read * read)))
    activated = (0.5 * read * (1.0 + bent)).astype(BF16)
    c, chips = core[0], kept.shape[0]
    features = along_ring(chip[0], c, chips, kept.shape[2])
    for out, first, sign in ((kept, c, 1), (given, 1 - c, -1)):
        for i, place in enumerate(ring_order(chips, first, sign)):
            out[i] = dot32(activated, w_out[:, features(*place)]).astype(out.dtype)


def front(core, chip, log_step, *arrays):
    tokens, w_out, state = arrays[0], arrays[-1], arrays[-2]
    seqs, model_width = tokens.shape
    z_count = lax.axis_size("z")
    part = (z_count, seqs, model_width // (2 * z_count))
    smem, vmem = pl.BlockSpec(memory_space=pltpu.SMEM), pl.BlockSpec(memory_space=pltpu.VMEM)
    return pl.pallas_call(
        front_kernel,
        out_shape=(
            jax.ShapeDtypeStruct(state.shape, F32),
            jax.ShapeDtypeStruct(state.shape, F32),
            jax.ShapeDtypeStruct(part, BF16),
            jax.ShapeDtypeStruct(part, BF16),
        ),
        in_specs=[smem] * 3 + [vmem] * len(arrays),
        out_specs=(vmem,) * 4,
        cost_estimate=cost(4 * seqs * model_width * w_out.shape[0], 2 * w_out.size * 2),
        name="front",
    )(core, chip, log_step, *arrays)


def gate_up_kernel(
    at, arrived, gain, gate, gate_par, up, up_par, *refs
):
    *sent, incoming, weights, parcel, ins, outs = refs
    half, _, _, width, _ = weights.shape
    seq_devs, _, pair_slots, _ = incoming.shape
    z_count, _, lanes = parcel.shape
    capacity = pair_slots // half
    rows = seq_devs * capacity
    first = pltpu.make_async_copy(arrived, incoming, ins.at[0])
    first.start()
    loads = {}
    for e in range(half):
        for m, (own, par) in enumerate(((gate, gate_par), (up, up_par))):
            for part, source in enumerate((own.at[half * at[0] + e], par.at[half * at[0] + e])):
                arrival = ins.at[1 + 4 * e + 2 * m + part]
                copy = pltpu.make_async_copy(source, weights.at[e, m, part], arrival)
                copy.start()
                loads[e, m, part] = copy
    ones = jnp.ones((8, width), BF16)
    features = [pl.ds(pl.multiple_of(at[1 + part] * width, width), width) for part in range(2)]
    first.wait()
    stores = []

    def store(source, target):
        copy = pltpu.make_async_copy(source, target, outs.at[len(stores)])
        copy.start()
        stores.append(copy)

    def put(depth, size, block_of):
        for chip in range(z_count):
            steps = lax.rem(chip - at[3] + z_count, z_count)
            parcel[steps, depth : depth + size, :] = block_of(chip)

    scaled = {}
    for e in range(half):
        squares = jnp.zeros((8, rows), F32)
        for part in range(2):
            values = incoming[:, part, e * capacity : (e + 1) * capacity, :]
            values = values.reshape(rows, width).astype(F32)
            scaled[e, part] = (values * gain[:, features[part]]).astype(BF16)
            high, low = two_parts(values * values)
            squares = squares + dot_nt(ones, high) + dot_nt(ones, low)
        high, low = two_parts(squares)
        line = lax.broadcasted_iota(jnp.int32, squares.shape, 0)
        both = jnp.where(line == 0, high.astype(F32), jnp.where(line == 1, low.astype(F32), 0.0))
        depth = 2 * half * rows + e * 8
        put(depth, 8, lambda chip, both=both: both.astype(BF16))
    for e in range(half):
        for m in range(2):
            for part in range(2):
                loads[e, m, part].wait()
            sums = dot32(scaled[e, 0], weights[e, m, 0]) + dot32(scaled[e, 1], weights[e, m, 1])
            sums = sums.astype(BF16)
            depth = (half * m + e) * rows
            put(depth, rows, lambda chip, sums=sums: sums[:, chip * lanes : (chip + 1) * lanes])
    middle, depth = z_count // 2, parcel.shape[1]
    split = depth // 2
    targets = [sent[0], *sent[1:middle], None, *sent[middle:]]
    for steps, target in enumerate(targets):
        if steps in (1, z_count - 1):
            first = 0 if steps == 1 else split
            store(parcel.at[middle, pl.ds(first, split), :], target.at[pl.ds(depth, split), :])
            target = target.at[pl.ds(0, depth), :]
        if steps != middle:
            store(parcel.at[steps], target)
    for copy in stores:
        copy.wait()


def gate_up(at, incoming, gain, gate, gate_par, up, up_par):
    seq_devs, _, pair_slots, width = incoming.shape
    half, units = gate.shape[0] // 2, gate.shape[2]
    z_count = lax.axis_size("z")
    pair_rows = seq_devs * pair_slots
    parcel = (z_count, 2 * pair_rows + half * 8, units // z_count)
    long = parcel[1] + parcel[1] // 2
    smem, vmem = pl.BlockSpec(memory_space=pltpu.SMEM), pl.BlockSpec(memory_space=pltpu.VMEM)
    far, any_place = pl.BlockSpec(memory_space=pltpu.HBM), pl.BlockSpec(memory_space=pl.ANY)
    return pl.pallas_call(
        gate_up_kernel,
        in_specs=[smem, any_place, vmem, far, any_place, far, any_place],
        out_specs=(any_place,) * (z_count - 1),
        out_shape=tuple(
            jax.ShapeDtypeStruct((depth, parcel[2]), BF16)
            for depth in (parcel[1], long, *(parcel[1],) * (z_count - 4), long)
        ),
        scratch_shapes=[
            pltpu.VMEM(incoming.shape, BF16),
            pltpu.VMEM((half, 2, 2, width, units), BF16),
            pltpu.VMEM(parcel, BF16),
            pltpu.SemaphoreType.DMA((1 + 4 * half,)),
            pltpu.SemaphoreType.DMA((z_count + 1,)),
        ],
        compiler_params=pltpu.CompilerParams(vmem_limit_bytes=52 * 2**20),
        cost_estimate=cost(8 * pair_rows * width * units, 8 * half * width * units),
        name="gate_up",
    )(at, incoming, gain, gate, gate_par, up, up_par)


def dispatch_kernel(spread, own_in, par_in, outgoing, own, par, arrivals):
    copies = [
        pltpu.make_async_copy(source, target, arrivals.at[i])
        for i, (source, target) in enumerate(((own_in, own), (par_in, par)))
    ]
    for copy in copies:
        copy.start()
    for copy in copies:
        copy.wait()
    shape = outgoing.shape[:1] + outgoing.shape[2:]
    for part, rows in enumerate((own, par)):
        outgoing[:, part] = dot32(spread[...], rows[...]).astype(BF16).reshape(shape)


def dispatch(spread, own, par, ep_count):
    slots, (_, width) = spread.shape[0], own.shape
    vmem = pl.BlockSpec(memory_space=pltpu.VMEM)
    return pl.pallas_call(
        dispatch_kernel,
        out_shape=jax.ShapeDtypeStruct((ep_count, 2, slots // ep_count, width), BF16),
        in_specs=[vmem, pl.BlockSpec(memory_space=pl.ANY), pl.BlockSpec(memory_space=pl.ANY)],
        out_specs=vmem,
        scratch_shapes=[
            pltpu.VMEM(own.shape, BF16),
            pltpu.VMEM(own.shape, BF16),
            pltpu.SemaphoreType.DMA((2,)),
        ],
        compiler_params=ROOM,
        cost_estimate=cost(4 * spread.size * width, 4 * slots * width),
        name="dispatch",
    )(spread, own, par)


def combine_kernel(weights, arrived, base, *refs):
    *parts, own, given, returned, arrival = refs
    fetch(arrived, returned, arrival)
    high, low = two_parts(weights[...])
    rows, width = weights.shape[1], returned.shape[3]
    for slot, out in enumerate((own, given)):
        values = returned[:, slot].reshape(rows, width)
        total = dot32(high, values) + dot32(low, values)
        if slot == 0:
            total = total + base[...].astype(F32)
        for part in parts:
            if slot < part.shape[0]:
                total = total + part[slot].astype(F32)
        out[...] = total.astype(out.dtype)


def combined(weights, returned, base, parts):
    shape = (weights.shape[0], returned.shape[3])
    vmem = pl.BlockSpec(memory_space=pltpu.VMEM)
    return pl.pallas_call(
        combine_kernel,
        out_shape=(jax.ShapeDtypeStruct(shape, F32), jax.ShapeDtypeStruct(shape, BF16)),
        in_specs=[vmem, pl.BlockSpec(memory_space=pl.ANY)] + [vmem] * (1 + len(parts)),
        out_specs=(vmem, vmem),
        scratch_shapes=[pltpu.VMEM(returned.shape, BF16), pltpu.SemaphoreType.DMA],
        compiler_params=ROOM,
        cost_estimate=cost(8 * weights.size * shape[1], 2 * returned.size),
        name="combine",
    )(weights, returned, base, *parts)


def shared_kernel(at, own, par, mine, theirs, gain, sources, kept, given, *scratch):
    *weights, arrivals = scratch
    copies = [
        pltpu.make_async_copy(source, target, arrivals.at[i])
        for i, (source, target) in enumerate(zip(sources, weights, strict=True))
    ]
    for copy in copies:
        copy.start()
    for copy in copies:
        copy.wait()
    gate_t, up_t, down_t = weights
    c, z = at[0], at[3]
    seqs, width = kept.shape[1:]
    chips = gain.shape[1] // (2 * width)
    features = along_ring(z, c, chips, width)
    squares = jnp.zeros((seqs, 1), F32)
    gate = jnp.zeros((seqs, gate_t.shape[0]), F32)
    up = gate
    rows = [(own[...], features(0, c)), (par[...], features(0, 1 - c))]
    for pieces, first, sign in ((mine, c, -1), (theirs, 1 - c, 1)):
        for k, piece in enumerate(pieces):
            rows.append((piece[0], features(sign * (k + 1), first)))
            if piece.shape[0] > 1:
                rows.append((piece[1], features(sign * (k + 1), 1 - first)))
    for values, place in rows:
        values = values.astype(F32)
        squares = squares + jnp.sum(values * values, axis=-1, keepdims=True)
        scaled = (values * gain[:, place]).astype(BF16)
        gate = gate + dot_nt(scaled, gate_t[:, place])
        up = up + dot_nt(scaled, up_t[:, place])
    factor = lax.rsqrt(squares / gain.shape[1] + EPS)
    gate, up = gate * factor, up * factor
    inner = (gate / (1.0 + jnp.exp(-gate)) * up).astype(BF16)
    for out, first, sign in ((kept, c, 1), (given, 1 - c, -1)):
        for i, place in enumerate(ring_order(chips, first, sign)):
            out[i] = dot32(inner, down_t[:, features(*place)]).astype(out.dtype)


def shared_parts(at, own, par, mine, theirs, gain, gate_t, up_t, w_down):
    smem, vmem = pl.BlockSpec(memory_space=pltpu.SMEM), pl.BlockSpec(memory_space=pltpu.VMEM)
    (seqs, width), count = own.shape, len(mine)

    def kernel(at, own, par, *refs):
        first, second, (gain, *rest) = refs[:count], refs[count : 2 * count], refs[2 * count :]
        shared_kernel(at, own, par, first, second, gain, rest[:3], *rest[3:])

    return pl.pallas_call(
        kernel,
        out_shape=(
            jax.ShapeDtypeStruct((2 * count, seqs, width), BF16),
            jax.ShapeDtypeStruct((2 * count, seqs, width), BF16),
        ),
        in_specs=[smem] + [vmem] * (2 * count + 3) + [pl.BlockSpec(memory_space=pl.ANY)] * 3,
        out_specs=(vmem, vmem),
        scratch_shapes=[
            pltpu.VMEM(gate_t.shape, BF16),
            pltpu.VMEM(up_t.shape, BF16),
            pltpu.VMEM(w_down.shape, BF16),
            pltpu.SemaphoreType.DMA((3,)),
        ],
        compiler_params=pltpu.CompilerParams(vmem_limit_bytes=FULL),
        cost_estimate=cost(seqs * 6 * w_down.size, 6 * w_down.size),
        name="shared",
    )(at, own, par, *mine, *theirs, gain, gate_t, up_t, w_down)


def inner_kernel(model_width, half, *refs):
    *arrived, inner, parcels, arrivals = refs
    copies = [
        pltpu.make_async_copy(
            source.at[pl.ds(0, parcels.shape[1]), :], parcels.at[i], arrivals.at[i]
        )
        for i, source in enumerate(arrived)
    ]
    for copy in copies:
        copy.start()
    for copy in copies:
        copy.wait()
    totals = parcels[0].astype(F32)
    for i in range(1, len(copies)):
        totals = totals + parcels[i].astype(F32)
    lanes = totals.shape[1]
    pair_rows = inner.shape[0]
    rows = pair_rows // half
    for e in range(half):
        line = 2 * pair_rows + 8 * e
        squares = totals[line : line + 1] + totals[line + 1 : line + 2]
        factor = lax.rsqrt(squares / model_width + EPS)
        factor = jnp.broadcast_to(factor, (lanes, rows)).T
        gate = totals[e * rows : (e + 1) * rows] * factor
        up = totals[pair_rows + e * rows : pair_rows + (e + 1) * rows] * factor
        inner[e * rows : (e + 1) * rows, :] = (gate / (1.0 + jnp.exp(-gate)) * up).astype(BF16)


def inner_rows(parcels, model_width, half):
    depth, lanes = parcels[0].shape
    pair_rows = (depth - half * 8) // 2
    count = len(parcels)
    return pl.pallas_call(
        functools.partial(inner_kernel, model_width, half),
        out_shape=jax.ShapeDtypeStruct((pair_rows, lanes), BF16),
        in_specs=[pl.BlockSpec(memory_space=pl.ANY)] * count,
        out_specs=pl.BlockSpec(memory_space=pltpu.VMEM),
        scratch_shapes=[
            pltpu.VMEM((count, depth, lanes), BF16),
            pltpu.SemaphoreType.DMA((count,)),
        ],
        compiler_params=ROOM,
        cost_estimate=cost(depth * lanes * 32, depth * lanes * 32),
        name="inner",
    )(*parcels)


def down_kernel(at, mine, gathered, crossed, opposite, own, par, sent, *scratch):
    inner, weights, results, ins, outs = scratch
    half, lanes, chips = weights.shape[0], mine.shape[1], inner.shape[1] // mine.shape[1]
    way = 1 - 2 * at[0]
    pieces = [(mine, 0), (opposite, chips // 2)]
    for k, (piece, crossing) in enumerate(zip(gathered, crossed, strict=True)):
        pieces += [(piece.at[0], -(k + 1)), (crossing, k + 1)]
    arriving = []
    for i, (source, steps) in enumerate(pieces):
        chip = lax.rem(at[3] + way * steps + 2 * chips, chips)
        place = pl.ds(pl.multiple_of(chip * lanes, lanes), lanes)
        copy = pltpu.make_async_copy(source, inner.at[:, place], ins.at[i])
        copy.start()
        arriving.append(copy)
    loads = []
    for e in range(half):
        for part, source in enumerate((own, par)):
            arrival = ins.at[chips + 2 * e + part]
            copy = pltpu.make_async_copy(
                source.at[half * at[0] + e], weights.at[e, part], arrival
            )
            copy.start()
            loads.append(copy)
    for copy in arriving:
        copy.wait()
    rows = inner.shape[0] // half
    seq_devs, _, pair_slots, width = results.shape
    capacity = pair_slots // half
    stores = []
    for e in range(half):
        row = inner[e * rows : (e + 1) * rows, :]
        place = slice(e * capacity, (e + 1) * capacity)
        for part in range(2):
            loads[2 * e + part].wait()
            out = dot32(row, weights[e, part]).astype(BF16)
            results[:, part, place, :] = out.reshape(seq_devs, capacity, width)
        place = pl.ds(e * capacity, capacity)
        copy = pltpu.make_async_copy(
            results.at[:, :, place, :], sent.at[:, :, place, :], outs.at[e]
        )
        copy.start()
        stores.append(copy)
    for copy in stores:
        copy.wait()


def down(at, mine, gathered, crossed, opposite, w_down, w_par, seq_devs, capacity):
    half, units, width = w_par.shape[0] // 2, *w_par.shape[1:]
    results = (seq_devs, 2, half * capacity, width)
    smem, any_place = pl.BlockSpec(memory_space=pltpu.SMEM), pl.BlockSpec(memory_space=pl.ANY)
    count = len(gathered)

    def kernel(at, mine, *refs):
        first, second, rest = refs[:count], refs[count : 2 * count], refs[2 * count :]
        down_kernel(at, mine, first, second, *rest)

    return pl.pallas_call(
        kernel,
        in_specs=[smem] + [any_place] * (2 * count + 4),
        out_specs=pl.BlockSpec(memory_space=pltpu.HBM),
        out_shape=pltpu.HBM(results, BF16),
        scratch_shapes=[
            pltpu.VMEM((mine.shape[0], units), BF16),
            pltpu.VMEM((half, 2, units, width), BF16),
            pltpu.VMEM(results, BF16),
            pltpu.SemaphoreType.DMA((2 * count + 2 + 2 * half,)),
            pltpu.SemaphoreType.DMA((half,)),
        ],
        compiler_params=ROOM,
        cost_estimate=cost(4 * mine.shape[0] * units * width, 4 * half * units * width),
        name="down",
    )(at, mine, *gathered, *crossed, opposite, w_down, w_par)


def local(
    tokens,
    norm_gain,
    ffn_gain,
    w_in,
    decay_rate,
    frequency,
    log_step,
    input_real,
    input_imag,
    readout_real,
    readout_imag,
    skip_gain,
    state_real,
    state_imag,
    w_out,
    shared_gate,
    shared_up,
    shared_down,
    expert_gate,
    expert_up,
    expert_down,
    routing,
    route_weight,
):
    seq_count, model_width = tokens.shape
    ep_count, z_count = lax.axis_size("ep"), lax.axis_size("z")
    z, c = lax.axis_index("z"), lax.axis_index("c")
    slice_width = model_width // (2 * z_count)
    offset = (2 * z + c) * slice_width
    other_offset = (2 * z + 1 - c) * slice_width

    new_real, new_imag, kept, given = front(
        c.reshape(1),
        z.reshape(1),
        log_step,
        tokens,
        norm_gain.reshape(1, -1),
        w_in,
        decay_rate.reshape(1, -1),
        frequency.reshape(1, -1),
        input_real,
        input_imag,
        readout_real,
        readout_imag,
        skip_gain.reshape(1, -1),
        state_real,
        state_imag,
        w_out,
    )
    got = swapped(given)
    own_part, parts = ring_sums(kept, got)

    gate_par, up_par, down_par = (swapped(w) for w in (expert_gate, expert_up, expert_down))

    own_sum = own_part.astype(F32) + sum(part[0].astype(F32) for part in parts)
    other_sum = sum(part[1].astype(F32) for part in parts if part.shape[0] > 1)
    got = swapped(jnp.stack([own_sum, other_sum]).astype(BF16)).astype(F32)
    own_tokens = lax.dynamic_slice_in_dim(tokens, offset, slice_width, 1)
    other_tokens = lax.dynamic_slice_in_dim(tokens, other_offset, slice_width, 1)
    resid_own = (own_tokens.astype(F32) + (own_sum + got[1])).astype(BF16)
    resid_par = (other_tokens.astype(F32) + (other_sum + got[0])).astype(BF16)

    expert_dev = expert_gate.shape[0]
    half = expert_dev // 2
    top_count = routing.shape[1]
    capacity = 2 * seq_count * top_count // (expert_dev * ep_count)
    slot_count = half * ep_count * capacity
    flat_ids = routing.reshape(-1)
    one_hot = (
        flat_ids[:, None] == jnp.arange(expert_dev * ep_count, dtype=jnp.int32)[None, :]
    ).astype(jnp.int32)
    earlier = jnp.cumsum(one_hot, axis=0) - one_hot
    slot_rank = jnp.sum(earlier * one_hot, axis=1)
    home, within = flat_ids // expert_dev, flat_ids % expert_dev
    target = (home * half + within % half) * capacity + slot_rank
    target = jnp.where(within // half == c, target, -1)
    slot_ids = jnp.arange(slot_count, dtype=jnp.int32)
    placed = (target[None, :] == slot_ids[:, None]).reshape(slot_count, seq_count, top_count)
    spread = jnp.sum(placed.astype(F32), axis=2).astype(BF16)
    outgoing = dispatch(spread, resid_own, resid_par, ep_count)
    incoming = lax.all_to_all(outgoing, "ep", split_axis=0, concat_axis=0, tiled=True)

    at = jnp.array([1, 1, -1, 0], jnp.int32) * c + jnp.array([0, 2, 2, 1], jnp.int32) * z
    at = at + jnp.array([0, 0, 1, 0], jnp.int32)
    gain = ffn_gain.reshape(1, -1)
    sent = gate_up(at, incoming, gain, expert_gate, gate_par, expert_up, up_par)
    middle, depth = z_count // 2, sent[0].shape[0]
    chunks = dict(zip([k for k in range(z_count) if k != middle], sent, strict=True))
    parcels = [chunks[0]]
    for steps in range(1, middle):
        if steps == middle - 1:
            chunks[steps] = added(chunks[steps], parcels[1][depth:], 0)
            chunks[z_count - steps] = added(chunks[z_count - steps], parcels[2][depth:], depth // 2)
        parcels.append(moved(chunks[steps], "z", steps))
        parcels.append(moved(chunks[z_count - steps], "z", -steps))
    inner_mine = inner_rows(parcels, model_width, half)
    inner_held = jnp.stack([inner_mine, swapped(inner_mine)])
    gathered, crossed = [], []
    for steps in range(1, middle):
        gathered.append(both_ways(inner_held, steps))
        crossed.append(swapped(gathered[-1][1]))
    opposite = both_ways(gathered[-1][0], 1)
    results = down(
        at,
        inner_mine,
        gathered,
        crossed,
        opposite,
        expert_down,
        down_par,
        ep_count,
        capacity,
    )
    returned = lax.all_to_all(results, "ep", split_axis=0, concat_axis=0, tiled=True)

    held = jnp.stack([resid_own, resid_par])
    mine, theirs = [], []
    for steps in range(1, middle + 1):
        if steps < middle:
            mine.append(both_ways(held, steps))
        else:
            mine.append(both_ways(mine[-1][:1], 1))
        theirs.append(swapped(mine[-1]))
    kept, given = shared_parts(
        at,
        resid_own,
        resid_par,
        mine,
        theirs,
        gain,
        shared_gate.T,
        shared_up.T,
        shared_down,
    )
    got = swapped(given)
    own_part, shared_chip = ring_sums(kept, got)

    weights = route_weight / jnp.sum(route_weight, axis=1, keepdims=True) * ROUTED_SCALE
    chosen = target.reshape(seq_count, top_count)[:, :, None] == slot_ids[None, None, :]
    combine = jnp.sum(jnp.where(chosen, weights[:, :, None], 0.0), axis=1)
    own, given = combined(combine, returned, own_part, shared_chip)
    got = swapped(given)
    mixed = (resid_own.astype(F32) + own + got.astype(F32)).astype(BF16)
    return (mixed, new_real, new_imag)


def solution(mesh):
    ep_count, tp_count = mesh.devices.shape
    cores = Mesh(mesh.devices.reshape(ep_count, tp_count // 2, 2), ("ep", "z", "c"))
    placed = (
        P("ep", None),
        P(),
        P(),
        P(None, TP),
        P(TP),
        P(TP),
        P(TP),
        P(None, TP),
        P(None, TP),
        P(None, TP),
        P(None, TP),
        P(TP),
        P("ep", TP),
        P("ep", TP),
        P(TP, None),
        P(None, TP),
        P(None, TP),
        P(TP, None),
        P("ep", TP, None),
        P("ep", TP, None),
        P("ep", None, TP),
        P("ep", None),
        P("ep", None),
    )

    def step(*arrays):
        return local(*arrays)

    step = jax.shard_map(
        step,
        mesh=cores,
        in_specs=placed,
        out_specs=(P("ep", TP), P("ep", TP), P("ep", TP)),
        check_vma=False,
    )
    return step
```
